32 devices in a mesh: fs: 4 (over z), rep: 4 (over y, x), tp: 2 (over core).
Axes of the slice: x: 2, y: 2, z: 4, core: 2. Of those that a mesh axis runs over, the one named last changes fastest.
Arguments:
- attention_input: bfloat16 [12288, 2048], P(('fs', 'rep')), may hold values from -6 to 6
- query_cotangent: bfloat16 [12288, 1024], P(('fs', 'rep'), 'tp'), may hold values from -15 to 15
- gate_cotangent: float32 [16, 12288], P('tp', ('fs', 'rep')), may hold values from -6 to 6
- gate_totals: float32 [16, 12288], P('tp', ('fs', 'rep')), may hold values from -2304 to 0, as said below
- projector: bfloat16 [2048, 256], P('fs'), may hold values from -1 to 1
- query_master: float32 [2048, 1024], P('fs', 'tp'), may hold values from -0.125 to 0.125
- lowrank_mean: float32 [256, 1024], P('rep', 'tp'), may hold values from -32 to 32
- lowrank_square: float32 [256, 1024], P('rep', 'tp'), may hold values from 0.05 to 2
- gating_mean: float32 [16, 2048], P('tp'), may hold values from -1.8 to 1.8
- gating_square: float32 [16, 2048], P('tp'), may hold values from 0.01 to 1
Outputs:
- query_update: float32 [2048, 1024], P('fs', 'tp')
- query_renewed: float32 [2048, 1024], P('fs', 'tp')
- query_copy: bfloat16 [2048, 1024], P('fs', 'tp')
- mean_after: float32 [256, 1024], P('rep', 'tp')
- square_after: float32 [256, 1024], P('rep', 'tp')
- gating_update: float32 [16, 2048], P('tp')
- gating_average: float32 [16, 2048], P('tp')
- gating_energy: float32 [16, 2048], P('tp')
The draws below stay inside these ranges and needn't reach their ends.
Inputs may be any that keep to these rules, and one draw needn't show every extreme that they name: `gate_totals`: within each sequence of 768 positions, a running sum of negative log gates, so successive differences are negative.
All inputs are finite; a program needn't handle non-finite values.
Results may differ from the reference program's by a relative error of at most 0.0044.
The reference program's roundings to bfloat16 on the way (of `blended` and `gate_signal`) count: a program that leaves them out, or rounds other values in their place, can miss the bound.
Values may be sent and summed in bfloat16 or wider, within the bound.
A program may use at most 64 MiB of HBM per device.

```python
import math
import jax
import jax.numpy as jnp
from jax import lax

D = 2048
HEADS = 16
A = 1024
RANK = 256
DEVICE_TOKENS = 768
TOTAL_TOKENS = 12288


def rising(key, count, spread):
    jitter = jax.random.uniform(key, (count,), jnp.float32)
    steps_up = (jnp.arange(count, dtype=jnp.float32) + jitter) / count
    return jnp.exp(jnp.log(spread) * steps_up)


def draw_query_cotangent(key, part):
    column_key = jax.random.fold_in(key, 11)
    value_key = jax.random.fold_in(key, 12)
    scales = 0.3 * rising(column_key, A, 10.0)
    values = jnp.clip(jax.random.normal(value_key, (TOTAL_TOKENS, A), jnp.float32), -5.0, 5.0)
    return (values * scales[None, :]).astype(jnp.bfloat16)


def draw_projector(key, part):
    column_key = jax.random.fold_in(key, 21)
    value_key = jax.random.fold_in(key, 22)
    scales = rising(column_key, RANK, 3.0)
    values = jnp.clip(jax.random.normal(value_key, (D, RANK), jnp.float32), -5.0, 5.0)
    return (values * scales[None, :] / jnp.sqrt(jnp.float32(D))).astype(jnp.bfloat16)


def draw_lowrank_mean(key, part):
    row_key = jax.random.fold_in(key, 31)
    column_key = jax.random.fold_in(key, 32)
    value_key = jax.random.fold_in(key, 33)
    row_scales = rising(row_key, RANK, 4.0)
    column_scales = rising(column_key, A, 4.0)
    values = jnp.clip(jax.random.normal(value_key, (RANK, A), jnp.float32), -4.0, 4.0)
    return 0.5 * values * row_scales[:, None] * column_scales[None, :]


def draw_gate_totals(key, part):
    order = jax.random.permutation(jax.random.fold_in(key, 41), HEADS)
    fast_count = max(HEADS // 2, 1)
    quick_path = order < fast_count
    sequences = TOTAL_TOKENS // DEVICE_TOKENS
    base = jnp.where(quick_path, jnp.log(40.0), jnp.log(jnp.float32(DEVICE_TOKENS)))
    noise = jnp.clip(jax.random.normal(jax.random.fold_in(key, 42), (HEADS, TOTAL_TOKENS), jnp.float32), -4.0, 4.0)
    gate_logarithm = jax.nn.log_sigmoid(base[:, None] + noise)
    block_factor = jnp.exp(jax.random.uniform(jax.random.fold_in(key, 43), (sequences,), jnp.float32, -0.7, 0.7))
    gate_logarithm = gate_logarithm * jnp.repeat(block_factor, DEVICE_TOKENS)[None, :]
    token_groups = jax.random.uniform(jax.random.fold_in(key, 44), (TOTAL_TOKENS,), jnp.float32) < 3.0 / DEVICE_TOKENS
    layer_level = jnp.log(jax.random.uniform(jax.random.fold_in(key, 45), (HEADS, TOTAL_TOKENS), jnp.float32, 0.5, 0.8))
    gate_logarithm = gate_logarithm + jnp.where(jnp.logical_and(token_groups[None, :], jnp.logical_not(quick_path)[:, None]), layer_level, 0.0)
    totals = jnp.cumsum(gate_logarithm.reshape(HEADS, sequences, DEVICE_TOKENS), axis=2)
    return totals.reshape(HEADS, TOTAL_TOKENS)


def block_levels(rng, dims, shards, least, largest):
    loudness, own = 1.0, jax.random.fold_in(rng, 6)
    for position, parts in shards:
        draws = jnp.exp(jax.random.uniform(jax.random.fold_in(own, position), (parts,), jnp.float32, least / len(shards), largest / len(shards)))
        loudness = loudness * jnp.repeat(draws, dims[position] // parts).reshape([-1 if axis == position else 1 for axis in range(len(dims))])
    return loudness


def scatter_about(key, dims, scale, most, pieces=(), kind=jnp.bfloat16):
    result = jax.random.normal(key, dims, jnp.float32) * scale
    if len(pieces) > 0:
        result = block_levels(key, dims, pieces, -0.22, 0.18) * result
    return jnp.clip(result, min=-most, max=most).astype(kind)


def setup_inputs(seed: int = 0) -> dict:
    key_list = jax.random.split(jax.random.key(seed), 11)
    return {
        "attention_input": scatter_about(key_list[0], (TOTAL_TOKENS, D), 1.0, 6.0, ((0, 16),)),
        "query_cotangent": draw_query_cotangent(jax.random.fold_in(key_list[10], 71), 0),
        "gate_cotangent": scatter_about(key_list[2], (HEADS, TOTAL_TOKENS), 1.0, 6.0, ((0, 2), (1, 16)), jnp.float32),
        "gate_totals": draw_gate_totals(jax.random.fold_in(key_list[10], 71), 0),
        "projector": draw_projector(jax.random.fold_in(key_list[10], 71), 0),
        "query_master": scatter_about(key_list[5], (D, A), D ** -0.5, 0.125, ((0, 4), (1, 2)), jnp.float32),
        "lowrank_mean": draw_lowrank_mean(jax.random.fold_in(key_list[10], 71), 0),
        "lowrank_square": jnp.clip(jnp.exp(math.log(2.0) - 3.6888794 * jax.random.uniform(key_list[7], (RANK, A), jnp.float32) ** block_levels(key_list[7], (RANK, A), ((0, 4), (1, 2)), -0.2, 0.2)), 0.05, 2.0),
        "gating_mean": scatter_about(key_list[8], (HEADS, D), 0.3, 1.8, ((0, 2),), jnp.float32),
        "gating_square": jnp.clip(jnp.exp(math.log(1.0) - 4.6051702 * jax.random.uniform(key_list[9], (HEADS, D), jnp.float32) ** block_levels(key_list[9], (HEADS, D), ((0, 2),), -0.2, 0.2)), 0.01, 1.0),
    }


BETA_ONE = 0.9
BETA_TWO = 0.95
STEP_RATE = 0.01
EPSILON = 1e-08
NORM_FLOOR = 1e-06

def reference(attention_input, query_cotangent, gate_cotangent, gate_totals, projector, query_master, lowrank_mean, lowrank_square, gating_mean, gating_square):
    norming = 1.0 / TOTAL_TOKENS ** 0.5
    contract = (((0,), (0,)), ((), ()))
    gradient = lax.dot_general(attention_input, query_cotangent, contract, preferred_element_type=jnp.float32) * norming
    factor = projector.astype(jnp.float32)
    projected = lax.dot_general(factor, gradient, contract, precision=lax.Precision.HIGHEST, preferred_element_type=jnp.float32)
    mean_after = BETA_ONE * lowrank_mean + (1.0 - BETA_ONE) * projected
    square_after = BETA_TWO * lowrank_square + (1.0 - BETA_TWO) * projected * projected
    direction = mean_after / (jnp.sqrt(square_after) + EPSILON)
    balance = jnp.sqrt(jnp.sum(direction * direction) / (jnp.sum(projected * projected) + NORM_FLOOR))
    blended = (direction - balance * projected).astype(jnp.bfloat16)
    query_update = jnp.dot(projector, blended, preferred_element_type=jnp.float32) + balance * gradient
    query_renewed = query_master - STEP_RATE * query_update
    query_copy = query_renewed.astype(jnp.bfloat16)
    sequences = TOTAL_TOKENS // DEVICE_TOKENS
    totals = gate_totals.reshape(HEADS, sequences, DEVICE_TOKENS)
    earlier = jnp.concatenate([jnp.zeros((HEADS, sequences, 1), jnp.float32), totals[:, :, :-1]], axis=2)
    gate_logarithm = totals - earlier
    trailing = lax.cumsum(gate_cotangent.reshape(HEADS, sequences, DEVICE_TOKENS), axis=2, reverse=True)
    gate_signal = (trailing * -jnp.expm1(gate_logarithm)).astype(jnp.bfloat16).reshape(HEADS, TOTAL_TOKENS)
    forget_gradient = jnp.dot(gate_signal, attention_input, preferred_element_type=jnp.float32) * norming
    gating_average = BETA_ONE * gating_mean + (1.0 - BETA_ONE) * forget_gradient
    gating_energy = BETA_TWO * gating_square + (1.0 - BETA_TWO) * forget_gradient * forget_gradient
    gating_update = gating_average / (jnp.sqrt(gating_energy) + EPSILON)
    return (query_update, query_renewed, query_copy, mean_after, square_after, gating_update, gating_average, gating_energy)
```

```python
import functools

import jax
import jax.numpy as jnp
from jax import lax
from jax.experimental import pallas as pl
from jax.experimental.pallas import tpu as pltpu
from jax.sharding import PartitionSpec as P

BETA_ONE = 0.9
BETA_TWO = 0.95
STEP_RATE = 0.01
EPSILON = 1e-08
NORM_FLOOR = 1e-06


PIECES = 4
VMEM_GRANT = 24 * 1024 * 1024
MESH = pl.DeviceIdType.MESH
CONTRACT = (((0,), (0,)), ((), ()))


def collective_form(
    attention_input,
    query_cotangent,
    gate_cotangent,
    gate_totals,
    projector,
    query_master,
    lowrank_mean,
    lowrank_square,
    gating_mean,
    gating_square,
):
    tokens_all = attention_input.shape[0] * lax.axis_size("fs") * lax.axis_size("rep")
    norming = 1.0 / tokens_all**0.5
    contract = (((0,), (0,)), ((), ()))
    earlier = jnp.concatenate(
        [jnp.zeros((gate_totals.shape[0], 1), jnp.float32), gate_totals[:, :-1]], axis=1
    )
    gate_logarithm = gate_totals - earlier
    trailing = lax.cumsum(gate_cotangent, axis=1, reverse=True)
    gate_signal = (trailing * -jnp.expm1(gate_logarithm)).astype(jnp.bfloat16)
    gate_partial = jnp.dot(gate_signal, attention_input, preferred_element_type=jnp.float32)
    forget_gradient = lax.psum(gate_partial, ("fs", "rep")) * norming
    thin_rows = lax.psum_scatter(
        lax.dot_general(
            attention_input, query_cotangent, contract, preferred_element_type=jnp.float32
        ),
        ("fs", "rep"),
        scatter_dimension=0,
        tiled=True,
    )
    gradient = lax.all_gather(thin_rows, "rep", axis=0, tiled=True) * norming
    rank_rows = lowrank_mean.shape[0]
    own_factor = lax.dynamic_slice_in_dim(
        projector, lax.axis_index("rep") * rank_rows, rank_rows, 1
    ).astype(jnp.float32)
    rank_partial = lax.dot_general(
        own_factor,
        gradient,
        contract,
        precision=lax.Precision.HIGHEST,
        preferred_element_type=jnp.float32,
    )
    projected = lax.psum(rank_partial, "fs")
    mean_after = BETA_ONE * lowrank_mean + (1.0 - BETA_ONE) * projected
    square_after = BETA_TWO * lowrank_square + (1.0 - BETA_TWO) * projected * projected
    direction = mean_after / (jnp.sqrt(square_after) + EPSILON)
    direction_squares, projected_squares = lax.psum(
        (jnp.sum(direction * direction), jnp.sum(projected * projected)), ("rep", "tp")
    )
    balance = jnp.sqrt(direction_squares / (projected_squares + NORM_FLOOR))
    blended = (direction - balance * projected).astype(jnp.bfloat16)
    lifted = jnp.dot(
        projector,
        lax.all_gather(blended, "rep", axis=0, tiled=True),
        preferred_element_type=jnp.float32,
    )
    query_update = lifted + balance * gradient
    query_renewed = query_master - STEP_RATE * query_update
    query_copy = query_renewed.astype(jnp.bfloat16)
    gating_average = BETA_ONE * gating_mean + (1.0 - BETA_ONE) * forget_gradient
    gating_energy = BETA_TWO * gating_square + (1.0 - BETA_TWO) * forget_gradient * forget_gradient
    gating_update = gating_average / (jnp.sqrt(gating_energy) + EPSILON)
    return (
        query_update,
        query_renewed,
        query_copy,
        mean_after,
        square_after,
        gating_update,
        gating_average,
        gating_energy,
    )


def fused_kernel(
    nf, nr, nt,
    x_hbm, c_hbm, gc_ref, gt_ref, pj_ref, lm_ref, ls_ref,
    g_all, h_all, balance_ref, projected_ref, rd_all,
    x_ref, c_ref,
    a_send, a_recv, a_own, b_send, b_recv, g_ref,
    d_part, d_recv, e_part, e_recv, e_own, proj, f_send, f_recv,
    ra_send, ra_recv, rb_part, rb_recv, rc_all,
    send_sem, recv_sem, load_sem,
):
    f, r, t = lax.axis_index("fs"), lax.axis_index("rep"), lax.axis_index("tp")
    tokens, width = x_ref.shape
    cols = c_ref.shape[1]
    piece = cols // PIECES
    thin = width // (nf * nr)
    norming = 1.0 / (tokens * nf * nr) ** 0.5
    started = []

    def columns(owner_r, owner_f):
        return pl.ds(pl.multiple_of((owner_f * nr + owner_r) * thin, thin), thin)

    load_c = pltpu.make_async_copy(c_hbm, c_ref, load_sem.at[nr * nf])
    load_c.start()
    loads = {}
    for k in list(range(1, nr)) + [0]:
        for j in range(nf):
            where = columns(lax.rem(r + k, nr), j)
            loads[k, j] = pltpu.make_async_copy(
                x_hbm.at[:, where], x_ref.at[:, where], load_sem.at[k * nf + j]
            )
            loads[k, j].start()

    def at(df, dr, dt):
        return (lax.rem(f + df, nf), lax.rem(r + dr, nr), lax.rem(t + dt, nt))

    def send(src, dst, where):
        slot = len(started)
        copy = pltpu.make_async_remote_copy(
            src_ref=src, dst_ref=dst, send_sem=send_sem.at[slot], recv_sem=recv_sem.at[slot],
            device_id=where, device_id_type=MESH,
        )
        copy.start()
        started.append(copy)
        return copy

    reps = list(range(1, nr))
    fss = list(range(1, nf))
    rest = [(dr, dt) for dr in range(nr) for dt in range(nt) if dr or dt]
    peers = [at(df, 0, 0) for df in fss] + [at(0, dr, dt) for dr, dt in rest]
    barrier = pltpu.get_barrier_semaphore()
    for peer in peers:
        pl.semaphore_signal(barrier, inc=1, device_id=peer, device_id_type=MESH)

    load_c.wait()

    def block(k, j):
        loads[k, j].wait()
        return lax.dot_general(
            x_ref[:, columns(lax.rem(r + k, nr), j)], c_ref[...], CONTRACT,
            preferred_element_type=jnp.float32,
        )

    a_copies = [[None] * (nr - 1) for _ in range(PIECES)]
    for k in reps:
        for j in range(nf):
            value = block(k, j).astype(jnp.bfloat16)
            for p in range(PIECES):
                a_send[p, k - 1, j] = value[:, p * piece : (p + 1) * piece]
        if k == reps[0]:
            pl.semaphore_wait(barrier, len(peers))
        a_copies[0][k - 1] = send(a_send.at[0, k - 1], a_recv.at[0, k - 1], at(0, k, 0))
    for p in range(1, PIECES):
        for k in reps:
            a_copies[p][k - 1] = send(a_send.at[p, k - 1], a_recv.at[p, k - 1], at(0, k, 0))
    for j in range(nf):
        a_own[j] = block(0, j)

    lanes = 128
    lower = lax.broadcasted_iota(jnp.int32, (lanes, lanes), 0)
    upper = lax.broadcasted_iota(jnp.int32, (lanes, lanes), 1)
    later = (lower >= upper).astype(jnp.float32)
    carry = jnp.zeros((gc_ref.shape[0], 1), jnp.float32)
    signals = []
    totals = gt_ref[...]
    first = lax.broadcasted_iota(jnp.int32, totals.shape, 1) == 0
    gate_logarithm = totals - jnp.where(first, 0.0, pltpu.roll(totals, 1, 1))
    for i in reversed(range(tokens // lanes)):
        window = slice(i * lanes, (i + 1) * lanes)
        own = gc_ref[:, window]
        trailing = carry + jnp.dot(
            own, later, precision=lax.Precision.HIGHEST, preferred_element_type=jnp.float32
        )
        carry = carry + jnp.sum(own, axis=1, keepdims=True)
        signals.append(trailing)
    trailing = jnp.concatenate(signals[::-1], axis=1)
    series = jnp.ones_like(gate_logarithm)
    for i in range(8, 1, -1):
        series = 1.0 + gate_logarithm * series / i
    opening = jnp.where(
        gate_logarithm > -0.25, -gate_logarithm * series, 1.0 - jnp.exp(gate_logarithm)
    )
    gate_signal = (trailing * opening).astype(jnp.bfloat16)
    gate_partial = jnp.dot(gate_signal, x_ref[...], preferred_element_type=jnp.float32)
    for i in range(nr):
        for j in range(nf):
            start = (i * nf + j) * thin
            ra_send[i, j] = gate_partial[:, start : start + thin]
    ra = [send(ra_send.at[lax.rem(r + k, nr)], ra_recv.at[k - 1], at(0, k, 0)) for k in reps]

    b_copies = []
    for p in range(PIECES):
        window = slice(p * piece, (p + 1) * piece)
        for copy in a_copies[p]:
            copy.wait_recv()

        def summed(j):
            total = a_own[j, :, window]
            for k in reps:
                total = total + a_recv[p, k - 1, j].astype(jnp.float32)
            return total

        row = []
        for k in fss:
            b_send[p, k - 1] = summed(lax.rem(f + k, nf)).astype(jnp.bfloat16)
            row.append(send(b_send.at[p, k - 1], b_recv.at[p, k - 1], at(k, 0, 0)))
        g_ref[:, window] = summed(f)
        b_copies.append(row)
    for copy in ra:
        copy.wait_recv()
    gate_rows = ra_send[r]
    for k in reps:
        gate_rows = gate_rows + ra_recv[k - 1]
    rb_part[...] = gate_rows
    rb = [send(rb_part.at[lax.rem(f + k, nf)], rb_recv.at[k - 1], at(k, 0, 0)) for k in fss]

    for p in range(PIECES):
        window = slice(p * piece, (p + 1) * piece)
        for copy in b_copies[p]:
            copy.wait_recv()
        total = g_ref[:, window]
        for k in fss:
            total = total + b_recv[p, k - 1].astype(jnp.float32)
        g_ref[:, window] = total * norming
    gradient = g_ref[...]
    g_all[r] = gradient.astype(jnp.bfloat16)
    factor = pj_ref[pl.ds(pl.multiple_of(r * thin, thin), thin), :].astype(jnp.float32)
    partial = lax.dot_general(
        factor, gradient, CONTRACT, precision=lax.Precision.HIGHEST,
        preferred_element_type=jnp.float32,
    )
    d_part[...] = partial.reshape(d_part.shape)
    d = [send(d_part.at[lax.rem(r + k, nr)], d_recv.at[k - 1], at(0, k, 0)) for k in reps]

    for copy in rb:
        copy.wait_recv()
    gate_block = rb_part[f]
    for k in fss:
        gate_block = gate_block + rb_recv[k - 1]
    rc_all[f] = gate_block * norming
    rc = [send(rc_all.at[f], rc_all.at[f], at(k, 0, 0)) for k in fss]

    for copy in d:
        copy.wait_recv()
    c = [send(g_all.at[r], g_all.at[r], at(0, k, 0)) for k in reps]
    total = d_part[r]
    for k in reps:
        total = total + d_recv[k - 1]
    e_part[...] = total.reshape(e_part.shape)
    e = [send(e_part.at[lax.rem(f + k, nf)], e_recv.at[k - 1], at(k, 0, 0)) for k in fss]
    for copy in e:
        copy.wait_recv()
    total = e_part[f]
    for k in fss:
        total = total + e_recv[k - 1]
    proj[f] = total
    e2 = [send(proj.at[f], proj.at[f], at(k, 0, 0)) for k in fss]

    for copy in rc:
        copy.wait_recv()
    rd_all[r] = rc_all[...]
    rd = [send(rc_all, rd_all.at[r], at(0, k, 0)) for k in reps]

    for copy in e2:
        copy.wait_recv()
    projected = proj[...].reshape(lm_ref.shape)
    mean_after = BETA_ONE * lm_ref[...] + (1.0 - BETA_ONE) * projected
    square_after = BETA_TWO * ls_ref[...] + (1.0 - BETA_TWO) * projected * projected
    direction = mean_after / (jnp.sqrt(square_after) + EPSILON)
    f_send[0] = jnp.full(f_send.shape[1:], jnp.sum(direction * direction))
    f_send[1] = jnp.full(f_send.shape[1:], jnp.sum(projected * projected))
    fc = [send(f_send, f_recv.at[i], at(0, dr, dt)) for i, (dr, dt) in enumerate(rest)]
    projected_ref[...] = projected
    for copy in fc:
        copy.wait_recv()
    sums = f_send[...]
    for i in range(len(rest)):
        sums = sums + f_recv[i]
    ratio = jnp.sqrt(sums[0] / (sums[1] + NORM_FLOOR))
    balance_ref[...] = ratio
    balance = ratio[:1, :1]
    h_all[r] = (direction - balance * projected).astype(jnp.bfloat16)
    h = [send(h_all.at[r], h_all.at[r], at(0, k, 0)) for k in reps]

    for copy in rd + c + h:
        copy.wait_recv()
    for copy in started:
        copy.wait_send()


def closing_kernel(
    g_ref, h_ref, balance_ref, projected_ref, gate_ref, pj_ref, qm_ref, lm_ref, ls_ref, gm_ref, gq_ref,
    qu_ref, qr_ref, qc_ref, ma_ref, sa_ref, gu_ref, ga_ref, ge_ref,
):
    lifted = jnp.dot(
        pj_ref[...], h_ref[...].reshape(pj_ref.shape[1], qm_ref.shape[1]),
        preferred_element_type=jnp.float32,
    )
    query_update = lifted + balance_ref[:1, :1] * g_ref[0].astype(jnp.float32)
    query_renewed = qm_ref[...] - STEP_RATE * query_update
    qu_ref[...] = query_update
    qr_ref[...] = query_renewed
    qc_ref[...] = query_renewed.astype(jnp.bfloat16)

    @pl.when(pl.program_id(0) == 0)
    def _():
        projected = projected_ref[...]
        ma_ref[...] = BETA_ONE * lm_ref[...] + (1.0 - BETA_ONE) * projected
        sa_ref[...] = BETA_TWO * ls_ref[...] + (1.0 - BETA_TWO) * projected * projected
        nr, nf, _, thin = gate_ref.shape
        for i in range(nr):
            for j in range(nf):
                window = slice((i * nf + j) * thin, (i * nf + j + 1) * thin)
                forget_gradient = gate_ref[i, j]
                average = BETA_ONE * gm_ref[:, window] + (1.0 - BETA_ONE) * forget_gradient
                energy = (
                    BETA_TWO * gq_ref[:, window]
                    + (1.0 - BETA_TWO) * forget_gradient * forget_gradient
                )
                ga_ref[:, window] = average
                ge_ref[:, window] = energy
                gu_ref[:, window] = average / (jnp.sqrt(energy) + EPSILON)


def per_device(nf, nr, nt, *args):
    x, c, gc, _, pj, qm, lm, ls, gm, gq = args
    width, cols, rank_rows, heads = x.shape[1], c.shape[1], lm.shape[0], gc.shape[0]
    thin = width // (nf * nr)
    fits = (
        width % (nf * nr * 128) == 0 and rank_rows % (nf * 16) == 0
        and cols % (PIECES * 128) == 0 and heads % 8 == 0 and min(nf, nr) > 1
        and x.shape[0] % 128 == 0
    )
    if not fits:
        return collective_form(*args)
    piece, bf, fl = cols // PIECES, jnp.bfloat16, jnp.float32
    scratch = [
        (x.shape, bf), (c.shape, bf),
        ((PIECES, nr - 1, nf, thin, piece), bf), ((PIECES, nr - 1, nf, thin, piece), bf),
        ((nf, thin, cols), fl), ((PIECES, nf - 1, thin, piece), bf),
        ((PIECES, nf - 1, thin, piece), bf), ((thin, cols), fl),
        ((nr, rank_rows, cols), fl), ((nr - 1, rank_rows, cols), fl),
        ((nf, rank_rows // nf, cols), fl), ((nf - 1, rank_rows // nf, cols), fl),
        ((8, 128), fl), ((nf, rank_rows // nf, cols), fl),
        ((2, 8, 128), fl), ((nr * nt - 1, 2, 8, 128), fl),
        ((nr, nf, heads, thin), fl), ((nr - 1, nf, heads, thin), fl),
        ((nf, heads, thin), fl), ((nf - 1, heads, thin), fl),
        ((nf, heads, thin), fl),
    ]
    copies = (nr - 1) * (PIECES + 5) + (nf - 1) * (PIECES + 4) + nr * nt - 1
    outs = [
        (qm.shape, fl), (qm.shape, fl), (qm.shape, bf), (lm.shape, fl), (lm.shape, fl),
        (gm.shape, fl), (gm.shape, fl), (gm.shape, fl),
    ]
    between = [
        ((nr, thin, cols), bf), ((nr, rank_rows, cols), bf), ((8, 128), fl), (lm.shape, fl),
        ((nr, nf, heads, thin), fl),
    ]
    vmem = pl.BlockSpec(memory_space=pltpu.VMEM)
    hbm = pl.BlockSpec(memory_space=pltpu.HBM)
    passed = pl.pallas_call(
        functools.partial(fused_kernel, nf, nr, nt),
        out_shape=tuple(jax.ShapeDtypeStruct(*o) for o in between),
        in_specs=[hbm] * 2 + [vmem] * 5,
        out_specs=(vmem,) * len(between),
        scratch_shapes=[pltpu.VMEM(*v) for v in scratch]
        + [pltpu.SemaphoreType.DMA((copies,)), pltpu.SemaphoreType.DMA((copies,))]
        + [pltpu.SemaphoreType.DMA((nr * nf + 1,))],
        compiler_params=pltpu.CompilerParams(
            collective_id=0, has_side_effects=True, vmem_limit_bytes=VMEM_GRANT
        ),
    )(x, c, gc, args[3], pj, lm, ls)

    def whole(shape):
        return pl.BlockSpec(shape, lambda i: (0,) * len(shape))

    def rows(width):
        return pl.BlockSpec((thin, width), lambda i: (i, 0))

    return pl.pallas_call(
        closing_kernel,
        grid=(nr,),
        out_shape=tuple(jax.ShapeDtypeStruct(*o) for o in outs),
        in_specs=[pl.BlockSpec((1, thin, cols), lambda i: (i, 0, 0))]
        + [whole(b[0]) for b in between[1:]]
        + [rows(pj.shape[1]), rows(cols), whole(lm.shape), whole(ls.shape)]
        + [whole(gm.shape), whole(gq.shape)],
        out_specs=(rows(cols),) * 3 + tuple(whole(o[0]) for o in outs[3:]),
        compiler_params=pltpu.CompilerParams(vmem_limit_bytes=VMEM_GRANT),
    )(*passed, pj, qm, lm, ls, gm, gq)


def solution(mesh):
    in_specs = (
        P(("fs", "rep"), None),
        P(("fs", "rep"), "tp"),
        P("tp", ("fs", "rep")),
        P("tp", ("fs", "rep")),
        P("fs", None),
        P("fs", "tp"),
        P("rep", "tp"),
        P("rep", "tp"),
        P("tp", None),
        P("tp", None),
    )
    out_specs = (
        P("fs", "tp"),
        P("fs", "tp"),
        P("fs", "tp"),
        P("rep", "tp"),
        P("rep", "tp"),
        P("tp", None),
        P("tp", None),
        P("tp", None),
    )
    return jax.shard_map(
        functools.partial(per_device, mesh.shape["fs"], mesh.shape["rep"], mesh.shape["tp"]),
        mesh=mesh, in_specs=in_specs, out_specs=out_specs, check_vma=False
    )
```

```python
import functools

import jax
import jax.numpy as jnp
from jax import lax
from jax.experimental import pallas as pl
from jax.experimental.pallas import tpu as pltpu
from jax.sharding import PartitionSpec as P

BETA_ONE = 0.9
BETA_TWO = 0.95
STEP_RATE = 0.01
EPSILON = 1e-08
NORM_FLOOR = 1e-06


PIECES = 4
VMEM_GRANT = 24 * 1024 * 1024
MESH = pl.DeviceIdType.MESH
CONTRACT = (((0,), (0,)), ((), ()))


def collective_form(
    attention_input,
    query_cotangent,
    gate_cotangent,
    gate_totals,
    projector,
    query_master,
    lowrank_mean,
    lowrank_square,
    gating_mean,
    gating_square,
):
    tokens_all = attention_input.shape[0] * lax.axis_size("fs") * lax.axis_size("rep")
    norming = 1.0 / tokens_all**0.5
    contract = (((0,), (0,)), ((), ()))
    earlier = jnp.concatenate(
        [jnp.zeros((gate_totals.shape[0], 1), jnp.float32), gate_totals[:, :-1]], axis=1
    )
    gate_logarithm = gate_totals - earlier
    trailing = lax.cumsum(gate_cotangent, axis=1, reverse=True)
    gate_signal = (trailing * -jnp.expm1(gate_logarithm)).astype(jnp.bfloat16)
    gate_partial = jnp.dot(gate_signal, attention_input, preferred_element_type=jnp.float32)
    forget_gradient = lax.psum(gate_partial, ("fs", "rep")) * norming
    thin_rows = lax.psum_scatter(
        lax.dot_general(
            attention_input, query_cotangent, contract, preferred_element_type=jnp.float32
        ),
        ("fs", "rep"),
        scatter_dimension=0,
        tiled=True,
    )
    gradient = lax.all_gather(thin_rows, "rep", axis=0, tiled=True) * norming
    rank_rows = lowrank_mean.shape[0]
    own_factor = lax.dynamic_slice_in_dim(
        projector, lax.axis_index("rep") * rank_rows, rank_rows, 1
    ).astype(jnp.float32)
    rank_partial = lax.dot_general(
        own_factor,
        gradient,
        contract,
        precision=lax.Precision.HIGHEST,
        preferred_element_type=jnp.float32,
    )
    projected = lax.psum(rank_partial, "fs")
    mean_after = BETA_ONE * lowrank_mean + (1.0 - BETA_ONE) * projected
    square_after = BETA_TWO * lowrank_square + (1.0 - BETA_TWO) * projected * projected
    direction = mean_after / (jnp.sqrt(square_after) + EPSILON)
    direction_squares, projected_squares = lax.psum(
        (jnp.sum(direction * direction), jnp.sum(projected * projected)), ("rep", "tp")
    )
    balance = jnp.sqrt(direction_squares / (projected_squares + NORM_FLOOR))
    blended = (direction - balance * projected).astype(jnp.bfloat16)
    lifted = jnp.dot(
        projector,
        lax.all_gather(blended, "rep", axis=0, tiled=True),
        preferred_element_type=jnp.float32,
    )
    query_update = lifted + balance * gradient
    query_renewed = query_master - STEP_RATE * query_update
    query_copy = query_renewed.astype(jnp.bfloat16)
    gating_average = BETA_ONE * gating_mean + (1.0 - BETA_ONE) * forget_gradient
    gating_energy = BETA_TWO * gating_square + (1.0 - BETA_TWO) * forget_gradient * forget_gradient
    gating_update = gating_average / (jnp.sqrt(gating_energy) + EPSILON)
    return (
        query_update,
        query_renewed,
        query_copy,
        mean_after,
        square_after,
        gating_update,
        gating_average,
        gating_energy,
    )


def fused_kernel(
    nf, nr, nt,
    x_hbm, c_hbm, gc_ref, gt_ref, pj_ref, lm_ref, ls_ref,
    g_all, h_all, balance_ref, projected_ref, rd_all,
    x_ref, c_ref,
    a_send, a_recv, a_own, b_send, b_recv, g_ref,
    d_part, d_recv, e_part, e_recv, e_own, proj, f_send, f_recv,
    ra_send, ra_recv, rb_part, rb_recv, rc_all,
    send_sem, recv_sem, load_sem,
):
    f, r, t = lax.axis_index("fs"), lax.axis_index("rep"), lax.axis_index("tp")
    tokens, width = x_ref.shape
    cols = c_ref.shape[1]
    piece = cols // PIECES
    thin = width // (nf * nr)
    norming = 1.0 / (tokens * nf * nr) ** 0.5
    started = []

    def columns(owner_r, owner_f):
        return pl.ds(pl.multiple_of((owner_f * nr + owner_r) * thin, thin), thin)

    load_c = pltpu.make_async_copy(c_hbm, c_ref, load_sem.at[nr * nf])
    load_c.start()
    loads = {}
    for k in list(range(1, nr)) + [0]:
        for j in range(nf):
            where = columns(lax.rem(r + k, nr), j)
            loads[k, j] = pltpu.make_async_copy(
                x_hbm.at[:, where], x_ref.at[:, where], load_sem.at[k * nf + j]
            )
            loads[k, j].start()

    def at(df, dr, dt):
        return (lax.rem(f + df, nf), lax.rem(r + dr, nr), lax.rem(t + dt, nt))

    def send(src, dst, where):
        slot = len(started)
        copy = pltpu.make_async_remote_copy(
            src_ref=src, dst_ref=dst, send_sem=send_sem.at[slot], recv_sem=recv_sem.at[slot],
            device_id=where, device_id_type=MESH,
        )
        copy.start()
        started.append(copy)
        return copy

    reps = list(range(1, nr))
    fss = list(range(1, nf))
    rest = [(dr, dt) for dr in range(nr) for dt in range(nt) if dr or dt]
    peers = [at(df, 0, 0) for df in fss] + [at(0, dr, dt) for dr, dt in rest]
    barrier = pltpu.get_barrier_semaphore()
    for peer in peers:
        pl.semaphore_signal(barrier, inc=1, device_id=peer, device_id_type=MESH)

    load_c.wait()

    def block(k, j):
        loads[k, j].wait()
        return lax.dot_general(
            x_ref[:, columns(lax.rem(r + k, nr), j)], c_ref[...], CONTRACT,
            preferred_element_type=jnp.float32,
        )

    a_copies = [[None] * (nr - 1) for _ in range(PIECES)]
    for k in reps:
        for j in range(nf):
            value = block(k, j).astype(jnp.bfloat16)
            for p in range(PIECES):
                a_send[p, k - 1, j] = value[:, p * piece : (p + 1) * piece]
        if k == reps[0]:
            pl.semaphore_wait(barrier, len(peers))
        a_copies[0][k - 1] = send(a_send.at[0, k - 1], a_recv.at[0, k - 1], at(0, k, 0))
    for p in range(1, PIECES):
        for k in reps:
            a_copies[p][k - 1] = send(a_send.at[p, k - 1], a_recv.at[p, k - 1], at(0, k, 0))
    for j in range(nf):
        a_own[j] = block(0, j)

    lanes = 128
    lower = lax.broadcasted_iota(jnp.int32, (lanes, lanes), 0)
    upper = lax.broadcasted_iota(jnp.int32, (lanes, lanes), 1)
    later = (lower >= upper).astype(jnp.float32)
    carry = jnp.zeros((gc_ref.shape[0], 1), jnp.float32)
    signals = []
    totals = gt_ref[...]
    first = lax.broadcasted_iota(jnp.int32, totals.shape, 1) == 0
    gate_logarithm = totals - jnp.where(first, 0.0, pltpu.roll(totals, 1, 1))
    for i in reversed(range(tokens // lanes)):
        window = slice(i * lanes, (i + 1) * lanes)
        own = gc_ref[:, window]
        trailing = carry + jnp.dot(
            own, later, precision=lax.Precision.HIGHEST, preferred_element_type=jnp.float32
        )
        carry = carry + jnp.sum(own, axis=1, keepdims=True)
        signals.append(trailing)
    trailing = jnp.concatenate(signals[::-1], axis=1)
    series = jnp.ones_like(gate_logarithm)
    for i in range(8, 1, -1):
        series = 1.0 + gate_logarithm * series / i
    opening = jnp.where(
        gate_logarithm > -0.25, -gate_logarithm * series, 1.0 - jnp.exp(gate_logarithm)
    )
    gate_signal = (trailing * opening).astype(jnp.bfloat16)
    gate_partial = jnp.dot(gate_signal, x_ref[...], preferred_element_type=jnp.float32)
    for i in range(nr):
        for j in range(nf):
            start = (i * nf + j) * thin
            ra_send[i, j] = gate_partial[:, start : start + thin]
    ra = [send(ra_send.at[lax.rem(r + k, nr)], ra_recv.at[k - 1], at(0, k, 0)) for k in reps]

    b_copies = []
    for p in range(PIECES):
        window = slice(p * piece, (p + 1) * piece)
        for copy in a_copies[p]:
            copy.wait_recv()

        def summed(j):
            total = a_own[j, :, window]
            for k in reps:
                total = total + a_recv[p, k - 1, j].astype(jnp.float32)
            return total

        row = []
        for k in fss:
            b_send[p, k - 1] = summed(lax.rem(f + k, nf)).astype(jnp.bfloat16)
            row.append(send(b_send.at[p, k - 1], b_recv.at[p, k - 1], at(k, 0, 0)))
        g_ref[:, window] = summed(f)
        b_copies.append(row)
    for copy in ra:
        copy.wait_recv()
    gate_rows = ra_send[r]
    for k in reps:
        gate_rows = gate_rows + ra_recv[k - 1]
    rb_part[...] = gate_rows
    rb = [send(rb_part.at[lax.rem(f + k, nf)], rb_recv.at[k - 1], at(k, 0, 0)) for k in fss]

    for p in range(PIECES):
        window = slice(p * piece, (p + 1) * piece)
        for copy in b_copies[p]:
            copy.wait_recv()
        total = g_ref[:, window]
        for k in fss:
            total = total + b_recv[p, k - 1].astype(jnp.float32)
        g_ref[:, window] = total * norming
    gradient = g_ref[...]
    g_all[r] = gradient.astype(jnp.bfloat16)
    factor = pj_ref[pl.ds(pl.multiple_of(r * thin, thin), thin), :].astype(jnp.float32)
    partial = lax.dot_general(
        factor, gradient, CONTRACT, precision=lax.Precision.HIGHEST,
        preferred_element_type=jnp.float32,
    )
    d_part[...] = partial.reshape(d_part.shape)
    d = [send(d_part.at[lax.rem(r + k, nr)], d_recv.at[k - 1], at(0, k, 0)) for k in reps]

    for copy in rb:
        copy.wait_recv()
    gate_block = rb_part[f]
    for k in fss:
        gate_block = gate_block + rb_recv[k - 1]
    rc_all[f] = gate_block * norming
    rc = [send(rc_all.at[f], rc_all.at[f], at(k, 0, 0)) for k in fss]

    for copy in d:
        copy.wait_recv()
    c = [send(g_all.at[r], g_all.at[r], at(0, k, 0)) for k in reps]
    total = d_part[r]
    for k in reps:
        total = total + d_recv[k - 1]
    e_part[...] = total.reshape(e_part.shape)
    e = [send(e_part.at[lax.rem(f + k, nf)], e_recv.at[k - 1], at(k, 0, 0)) for k in fss]
    for copy in e:
        copy.wait_recv()
    total = e_part[f]
    for k in fss:
        total = total + e_recv[k - 1]
    proj[f] = total
    e2 = [send(proj.at[f], proj.at[f], at(k, 0, 0)) for k in fss]

    for copy in rc:
        copy.wait_recv()
    rd_all[r] = rc_all[...]
    rd = [send(rc_all, rd_all.at[r], at(0, k, 0)) for k in reps]

    for copy in e2:
        copy.wait_recv()
    projected = proj[...].reshape(lm_ref.shape)
    mean_after = BETA_ONE * lm_ref[...] + (1.0 - BETA_ONE) * projected
    square_after = BETA_TWO * ls_ref[...] + (1.0 - BETA_TWO) * projected * projected
    direction = mean_after / (jnp.sqrt(square_after) + EPSILON)
    f_send[0] = jnp.full(f_send.shape[1:], jnp.sum(direction * direction))
    f_send[1] = jnp.full(f_send.shape[1:], jnp.sum(projected * projected))
    fc = [send(f_send, f_recv.at[i], at(0, dr, dt)) for i, (dr, dt) in enumerate(rest)]
    projected_ref[...] = projected
    for copy in fc:
        copy.wait_recv()
    sums = f_send[...]
    for i in range(len(rest)):
        sums = sums + f_recv[i]
    ratio = jnp.sqrt(sums[0] / (sums[1] + NORM_FLOOR))
    balance_ref[...] = ratio
    balance = ratio[:1, :1]
    h_all[r] = (direction - balance * projected).astype(jnp.bfloat16)
    h = [send(h_all.at[r], h_all.at[r], at(0, k, 0)) for k in reps]

    for copy in rd + c + h:
        copy.wait_recv()
    for copy in started:
        copy.wait_send()


def closing_kernel(
    g_ref, h_ref, balance_ref, projected_ref, gate_ref, pj_ref, qm_ref, lm_ref, ls_ref, gm_ref, gq_ref,
    qu_ref, qr_ref, qc_ref, ma_ref, sa_ref, gu_ref, ga_ref, ge_ref,
):
    lifted = jnp.dot(
        pj_ref[...], h_ref[...].reshape(pj_ref.shape[1], qm_ref.shape[1]),
        preferred_element_type=jnp.float32,
    )
    query_update = lifted + balance_ref[:1, :1] * g_ref[0].astype(jnp.float32)
    query_renewed = qm_ref[...] - STEP_RATE * query_update
    qu_ref[...] = query_update
    qr_ref[...] = query_renewed
    qc_ref[...] = query_renewed.astype(jnp.bfloat16)

    @pl.when(pl.program_id(0) == 0)
    def _():
        projected = projected_ref[...]
        ma_ref[...] = BETA_ONE * lm_ref[...] + (1.0 - BETA_ONE) * projected
        sa_ref[...] = BETA_TWO * ls_ref[...] + (1.0 - BETA_TWO) * projected * projected
        nr, nf, _, thin = gate_ref.shape
        for i in range(nr):
            for j in range(nf):
                window = slice((i * nf + j) * thin, (i * nf + j + 1) * thin)
                forget_gradient = gate_ref[i, j]
                average = BETA_ONE * gm_ref[:, window] + (1.0 - BETA_ONE) * forget_gradient
                energy = (
                    BETA_TWO * gq_ref[:, window]
                    + (1.0 - BETA_TWO) * forget_gradient * forget_gradient
                )
                ga_ref[:, window] = average
                ge_ref[:, window] = energy
                gu_ref[:, window] = average / (jnp.sqrt(energy) + EPSILON)


def per_device(nf, nr, nt, *args):
    x, c, gc, _, pj, qm, lm, ls, gm, gq = args
    width, cols, rank_rows, heads = x.shape[1], c.shape[1], lm.shape[0], gc.shape[0]
    thin = width // (nf * nr)
    fits = (
        width % (nf * nr * 128) == 0 and rank_rows % (nf * 16) == 0
        and cols % (PIECES * 128) == 0 and heads % 8 == 0 and min(nf, nr) > 1
        and x.shape[0] % 128 == 0
    )
    if not fits:
        return collective_form(*args)
    piece, bf, fl = cols // PIECES, jnp.bfloat16, jnp.float32
    scratch = [
        (x.shape, bf), (c.shape, bf),
        ((PIECES, nr - 1, nf, thin, piece), bf), ((PIECES, nr - 1, nf, thin, piece), bf),
        ((nf, thin, cols), fl), ((PIECES, nf - 1, thin, piece), bf),
        ((PIECES, nf - 1, thin, piece), bf), ((thin, cols), fl),
        ((nr, rank_rows, cols), fl), ((nr - 1, rank_rows, cols), fl),
        ((nf, rank_rows // nf, cols), fl), ((nf - 1, rank_rows // nf, cols), fl),
        ((8, 128), fl), ((nf, rank_rows // nf, cols), fl),
        ((2, 8, 128), fl), ((nr * nt - 1, 2, 8, 128), fl),
        ((nr, nf, heads, thin), fl), ((nr - 1, nf, heads, thin), fl),
        ((nf, heads, thin), fl), ((nf - 1, heads, thin), fl),
        ((nf, heads, thin), fl),
    ]
    copies = (nr - 1) * (PIECES + 5) + (nf - 1) * (PIECES + 4) + nr * nt - 1
    outs = [
        (qm.shape, fl), (qm.shape, fl), (qm.shape, bf), (lm.shape, fl), (lm.shape, fl),
        (gm.shape, fl), (gm.shape, fl), (gm.shape, fl),
    ]
    between = [
        ((nr, thin, cols), bf), ((nr, rank_rows, cols), bf), ((8, 128), fl), (lm.shape, fl),
        ((nr, nf, heads, thin), fl),
    ]
    vmem = pl.BlockSpec(memory_space=pltpu.VMEM)
    hbm = pl.BlockSpec(memory_space=pltpu.HBM)
    passed = pl.pallas_call(
        functools.partial(fused_kernel, nf, nr, nt),
        out_shape=tuple(jax.ShapeDtypeStruct(*o) for o in between),
        in_specs=[hbm] * 2 + [vmem] * 5,
        out_specs=(vmem,) * len(between),
        scratch_shapes=[pltpu.VMEM(*v) for v in scratch]
        + [pltpu.SemaphoreType.DMA((copies,)), pltpu.SemaphoreType.DMA((copies,))]
        + [pltpu.SemaphoreType.DMA((nr * nf + 1,))],
        compiler_params=pltpu.CompilerParams(
            collective_id=0, has_side_effects=True, vmem_limit_bytes=VMEM_GRANT
        ),
    )(*(pltpu.with_memory_space_constraint(v, pltpu.HBM) for v in (x, c)), gc, args[3], pj, lm, ls)

    def whole(shape):
        return pl.BlockSpec(shape, lambda i: (0,) * len(shape))

    def rows(width):
        return pl.BlockSpec((thin, width), lambda i: (i, 0))

    return pl.pallas_call(
        closing_kernel,
        grid=(nr,),
        out_shape=tuple(jax.ShapeDtypeStruct(*o) for o in outs),
        in_specs=[pl.BlockSpec((1, thin, cols), lambda i: (i, 0, 0))]
        + [whole(b[0]) for b in between[1:]]
        + [rows(pj.shape[1]), rows(cols), whole(lm.shape), whole(ls.shape)]
        + [whole(gm.shape), whole(gq.shape)],
        out_specs=(rows(cols),) * 3 + tuple(whole(o[0]) for o in outs[3:]),
        compiler_params=pltpu.CompilerParams(vmem_limit_bytes=VMEM_GRANT),
    )(*passed, pj, qm, lm, ls, gm, gq)


def solution(mesh):
    in_specs = (
        P(("fs", "rep"), None),
        P(("fs", "rep"), "tp"),
        P("tp", ("fs", "rep")),
        P("tp", ("fs", "rep")),
        P("fs", None),
        P("fs", "tp"),
        P("rep", "tp"),
        P("rep", "tp"),
        P("tp", None),
        P("tp", None),
    )
    out_specs = (
        P("fs", "tp"),
        P("fs", "tp"),
        P("fs", "tp"),
        P("rep", "tp"),
        P("rep", "tp"),
        P("tp", None),
        P("tp", None),
        P("tp", None),
    )
    return jax.shard_map(
        functools.partial(per_device, mesh.shape["fs"], mesh.shape["rep"], mesh.shape["tp"]),
        mesh=mesh, in_specs=in_specs, out_specs=out_specs, check_vma=False
    )
```

```python
import functools

import jax
import jax.numpy as jnp
from jax import lax
from jax.experimental import pallas as pl
from jax.experimental.pallas import tpu as pltpu
from jax.sharding import PartitionSpec as P

BETA_ONE = 0.9
BETA_TWO = 0.95
STEP_RATE = 0.01
EPSILON = 1e-08
NORM_FLOOR = 1e-06


PIECES = 4
VMEM_GRANT = 32 * 1024 * 1024
MESH = pl.DeviceIdType.MESH
CONTRACT = (((0,), (0,)), ((), ()))


def collective_form(
    attention_input,
    query_cotangent,
    gate_cotangent,
    gate_totals,
    projector,
    query_master,
    lowrank_mean,
    lowrank_square,
    gating_mean,
    gating_square,
):
    tokens_all = attention_input.shape[0] * lax.axis_size("fs") * lax.axis_size("rep")
    norming = 1.0 / tokens_all**0.5
    contract = (((0,), (0,)), ((), ()))
    earlier = jnp.concatenate(
        [jnp.zeros((gate_totals.shape[0], 1), jnp.float32), gate_totals[:, :-1]], axis=1
    )
    gate_logarithm = gate_totals - earlier
    trailing = lax.cumsum(gate_cotangent, axis=1, reverse=True)
    gate_signal = (trailing * -jnp.expm1(gate_logarithm)).astype(jnp.bfloat16)
    gate_partial = jnp.dot(gate_signal, attention_input, preferred_element_type=jnp.float32)
    forget_gradient = lax.psum(gate_partial, ("fs", "rep")) * norming
    thin_rows = lax.psum_scatter(
        lax.dot_general(
            attention_input, query_cotangent, contract, preferred_element_type=jnp.float32
        ),
        ("fs", "rep"),
        scatter_dimension=0,
        tiled=True,
    )
    gradient = lax.all_gather(thin_rows, "rep", axis=0, tiled=True) * norming
    rank_rows = lowrank_mean.shape[0]
    own_factor = lax.dynamic_slice_in_dim(
        projector, lax.axis_index("rep") * rank_rows, rank_rows, 1
    ).astype(jnp.float32)
    rank_partial = lax.dot_general(
        own_factor,
        gradient,
        contract,
        precision=lax.Precision.HIGHEST,
        preferred_element_type=jnp.float32,
    )
    projected = lax.psum(rank_partial, "fs")
    mean_after = BETA_ONE * lowrank_mean + (1.0 - BETA_ONE) * projected
    square_after = BETA_TWO * lowrank_square + (1.0 - BETA_TWO) * projected * projected
    direction = mean_after / (jnp.sqrt(square_after) + EPSILON)
    direction_squares, projected_squares = lax.psum(
        (jnp.sum(direction * direction), jnp.sum(projected * projected)), ("rep", "tp")
    )
    balance = jnp.sqrt(direction_squares / (projected_squares + NORM_FLOOR))
    blended = (direction - balance * projected).astype(jnp.bfloat16)
    lifted = jnp.dot(
        projector,
        lax.all_gather(blended, "rep", axis=0, tiled=True),
        preferred_element_type=jnp.float32,
    )
    query_update = lifted + balance * gradient
    query_renewed = query_master - STEP_RATE * query_update
    query_copy = query_renewed.astype(jnp.bfloat16)
    gating_average = BETA_ONE * gating_mean + (1.0 - BETA_ONE) * forget_gradient
    gating_energy = BETA_TWO * gating_square + (1.0 - BETA_TWO) * forget_gradient * forget_gradient
    gating_update = gating_average / (jnp.sqrt(gating_energy) + EPSILON)
    return (
        query_update,
        query_renewed,
        query_copy,
        mean_after,
        square_after,
        gating_update,
        gating_average,
        gating_energy,
    )


def fused_kernel(
    nf, nr, nt,
    x_hbm, c_hbm, gc_hbm, gt_hbm, pj_hbm, lm_hbm, ls_hbm,
    g_all, h_all, balance_ref, projected_ref, rd_all,
    x_ref, c_ref, gc_ref, gt_ref, lm_ref, ls_ref, p_all,
    a_send, a_recv, a_own, a_keep, m_send, m_recv, b_send, b_recv, g_ref,
    xp_ref, d_part, d_send, d_recv, e_all, f_send, f_recv,
    ra_send, ra_recv, rb_part, rb_recv, rc_all,
    send_sem, recv_sem, load_sem,
):
    f, r, t = lax.axis_index("fs"), lax.axis_index("rep"), lax.axis_index("tp")
    tokens, width = x_ref.shape
    cols = c_ref.shape[1]
    piece = cols // PIECES
    thin = width // (nf * nr)
    half = thin // 2
    rank_rows = lm_ref.shape[0]
    rank_half = p_all.shape[2] // nt
    norming = 1.0 / (tokens * nf * nr) ** 0.5
    fl, bf = jnp.float32, jnp.bfloat16
    started = []
    side, line = lax.rem(r, 2), r // 2
    square = [r, line * 2 + (1 - side), (1 - line) * 2 + side, (1 - line) * 2 + (1 - side)]
    fss, squares = list(range(1, nf)), [1, 2, 3]

    loading = []

    def load(src, dst):
        copy = pltpu.make_async_copy(src, dst, load_sem.at[len(loading)])
        copy.start()
        loading.append(copy)
        return copy

    def columns(owner, j):
        return pl.ds(pl.multiple_of((j * nr + owner) * thin, thin), thin)

    load_c = load(c_hbm, c_ref)
    loads = {}
    for k in [3, 1, 2, 0]:
        for j in range(nf):
            where = columns(square[k], j)
            loads[k, j] = load(x_hbm.at[:, where], x_ref.at[:, where])
        if k == 3:
            load_p = load(pj_hbm, p_all.at[f])
    others = [load(*v) for v in ((gc_hbm, gc_ref), (gt_hbm, gt_ref), (lm_hbm, lm_ref), (ls_hbm, ls_ref))]

    def send(src, dst, where):
        slot = len(started)
        copy = pltpu.make_async_remote_copy(
            src_ref=src, dst_ref=dst, send_sem=send_sem.at[slot], recv_sem=recv_sem.at[slot],
            device_id=where, device_id_type=MESH,
        )
        copy.start()
        started.append(copy)
        return copy

    def rep(k):
        return (f, square[k], t)

    def depth(k):
        return (lax.rem(f + k, nf), r, t)

    rest = [(k, dt) for k in range(4) for dt in range(nt) if k or dt]
    spots = [(f, square[k], lax.rem(t + dt, nt)) for k, dt in rest]
    peers = [depth(k) for k in fss] + spots
    barrier = pltpu.get_barrier_semaphore()
    for peer in peers:
        pl.semaphore_signal(barrier, inc=1, device_id=peer, device_id_type=MESH)

    load_c.wait()

    def block(k, j):
        loads[k, j].wait()
        return lax.dot_general(
            x_ref[:, columns(square[k], j)], c_ref[...], CONTRACT, preferred_element_type=fl
        )

    def cut(p):
        return slice(p * piece, (p + 1) * piece)

    def fill(k, j):
        value = block(k, j)
        upper, lower = value[:half], value[half:]
        if k == 0:
            a_own[j] = value
        if k == 1:
            a_keep[1, j] = lower
        if k == 2:
            a_keep[0, j] = upper
        for h, part, slot in ((0, upper, {3: 0, 1: 1}), (1, lower, {3: 0, 2: 1})):
            if k in slot:
                small = part.astype(bf)
                for p in range(PIECES):
                    a_send[p, h, slot[k], j] = small[:, cut(p)]

    first = {}

    def send_first(p, h, o):
        first[p, h, o] = send(a_send.at[p, h, o], a_recv.at[p, h, o], rep(1 + h))

    second = {}

    def send_second(p):
        for h in range(2):
            first[p, h, 0].wait_recv()
            for j in range(nf):
                value = a_keep[h, j, :, cut(p)] + a_recv[p, h, 0, j].astype(fl)
                m_send[p, h, j] = value.astype(bf)
            second[p, h] = send(m_send.at[p, h], m_recv.at[p, h], rep(2 - h))

    third = {}

    def send_third(p):
        for h in range(2):
            first[p, h, 1].wait_recv()
            second[p, h].wait_recv()

        def summed(h, j):
            rows = slice(h * half, (h + 1) * half)
            return (
                a_own[j, rows, cut(p)] + a_recv[p, h, 1, j].astype(fl)
                + m_recv[p, h, j].astype(fl)
            )

        for k in fss:
            for h in range(2):
                b_send[p, k - 1, h] = summed(h, lax.rem(f + k, nf)).astype(bf)
            third[p, k] = send(b_send.at[p, k - 1], b_recv.at[p, k - 1], depth(k))
        for h in range(2):
            g_ref[h, :, cut(p)] = summed(h, f)

    fourth = []

    def send_fourth(p):
        for k in fss:
            third[p, k].wait_recv()
        for h in range(2):
            total = g_ref[h, :, cut(p)]
            for k in fss:
                total = total + b_recv[p, k - 1, h].astype(fl)
            g_all[r, h * half : (h + 1) * half, cut(p)] = (total * norming).astype(bf)
        where = g_all.at[r, :, cut(p)]
        fourth.extend(send(where, where, rep(k)) for k in squares)

    for j in range(nf):
        fill(3, j)
    load_p.wait()
    pl.semaphore_wait(barrier, len(peers))
    mine = pl.ds(pl.multiple_of(t * rank_half, rank_half), rank_half)
    p_far = [send(p_all.at[f, :, mine], p_all.at[f, :, mine], depth(k)) for k in fss]
    send_first(0, 0, 0)
    send_first(0, 1, 0)
    for k in (1, 2):
        for j in range(nf):
            fill(k, j)
        send_first(0, k - 1, 1)
    for h in range(2):
        for o in range(2):
            send_first(1, h, o)
    for j in range(nf):
        fill(0, j)

    for copy in others:
        copy.wait()
    lanes = 128
    lower = lax.broadcasted_iota(jnp.int32, (lanes, lanes), 0)
    upper = lax.broadcasted_iota(jnp.int32, (lanes, lanes), 1)
    later = (lower >= upper).astype(fl)
    carry = jnp.zeros((gc_ref.shape[0], 1), fl)
    signals = []
    totals = gt_ref[...]
    opens = lax.broadcasted_iota(jnp.int32, totals.shape, 1) == 0
    gate_logarithm = totals - jnp.where(opens, 0.0, pltpu.roll(totals, 1, 1))
    for i in reversed(range(tokens // lanes)):
        window = slice(i * lanes, (i + 1) * lanes)
        own = gc_ref[:, window]
        trailing = carry + jnp.dot(
            own, later, precision=lax.Precision.HIGHEST, preferred_element_type=fl
        )
        carry = carry + jnp.sum(own, axis=1, keepdims=True)
        signals.append(trailing)
    trailing = jnp.concatenate(signals[::-1], axis=1)
    series = jnp.ones_like(gate_logarithm)
    for i in range(8, 1, -1):
        series = 1.0 + gate_logarithm * series / i
    opening = jnp.where(
        gate_logarithm > -0.25, -gate_logarithm * series, 1.0 - jnp.exp(gate_logarithm)
    )
    gate_signal = (trailing * opening).astype(bf)
    gate_partial = jnp.dot(gate_signal, x_ref[...], preferred_element_type=fl)
    for i in range(nr):
        for j in range(nf):
            start = (i * nf + j) * thin
            ra_send[i, j] = gate_partial[:, start : start + thin]
    ra = [send(ra_send.at[square[k]], ra_recv.at[k - 1], rep(k)) for k in squares]

    def cast(q):
        place = lax.rem(f + q, nf)
        where = pl.ds(pl.multiple_of(place * nr * thin, nr * thin), nr * thin)
        return jnp.dot(x_ref[:, where], p_all[place], preferred_element_type=fl)

    xp_ref[...] = cast(0)

    send_second(0)
    for h in range(2):
        for o in range(2):
            send_first(2, h, o)
    send_second(1)

    p_near = []
    for k in fss:
        p_far[k - 1].wait_recv()
        place = lax.rem(f + nf - k, nf)
        where = p_all.at[place, :, mine]
        p_near.append(send(where, where, (f, r, 1 - t)))
    for k in fss:
        p_near[k - 1].wait_recv()
        xp_ref[...] += cast(nf - k)
    cast_all = xp_ref[...]
    high = cast_all.astype(bf)
    low = (cast_all - high.astype(fl)).astype(bf)
    partial = lax.dot_general(high, c_ref[...], CONTRACT, preferred_element_type=fl)
    partial += lax.dot_general(low, c_ref[...], CONTRACT, preferred_element_type=fl)
    d_part[...] = (partial * norming).reshape(d_part.shape)
    d = []
    for k in squares:
        d_send[k - 1] = d_part[square[k]].astype(bf)
        d.append(send(d_send.at[k - 1], d_recv.at[k - 1], rep(k)))
    for h in range(2):
        for o in range(2):
            send_first(3, h, o)
    send_third(0)
    send_second(2)
    send_third(1)

    for copy in d:
        copy.wait_recv()
    total = d_part[r]
    for k in squares:
        total = total + d_recv[k - 1].astype(fl)
    e_all[f] = total.astype(bf)
    e = [send(e_all.at[f], e_all.at[f], depth(k)) for k in fss]

    for copy in ra:
        copy.wait_recv()
    gate_rows = ra_send[r]
    for k in squares:
        gate_rows = gate_rows + ra_recv[k - 1]
    rb_part[...] = gate_rows
    rb = [send(rb_part.at[lax.rem(f + k, nf)], rb_recv.at[k - 1], depth(k)) for k in fss]

    send_second(3)
    send_third(2)
    send_fourth(0)
    send_fourth(1)
    for copy in rb:
        copy.wait_recv()
    gate_block = rb_part[f]
    for k in fss:
        gate_block = gate_block + rb_recv[k - 1]
    rc_all[f] = gate_block * norming
    rc = [send(rc_all.at[f], rc_all.at[f], depth(k)) for k in fss]
    send_third(3)

    for copy in e:
        copy.wait_recv()
    projected = e_all[0].astype(fl)
    for j in fss:
        projected = projected + e_all[j].astype(fl)
    mean_after = BETA_ONE * lm_ref[...] + (1.0 - BETA_ONE) * projected
    square_after = BETA_TWO * ls_ref[...] + (1.0 - BETA_TWO) * projected * projected
    direction = mean_after / (jnp.sqrt(square_after) + EPSILON)
    top = lax.broadcasted_iota(jnp.int32, f_send.shape, 0) == 0
    f_send[...] = jnp.where(top, jnp.sum(direction * direction), jnp.sum(projected * projected))
    fc = [send(f_send, f_recv.at[i], spot) for i, spot in enumerate(spots)]
    projected_ref[...] = projected
    send_fourth(2)
    for copy in fc:
        copy.wait_recv()
    sums = f_send[...]
    for i in range(len(rest)):
        sums = sums + f_recv[i]
    balance = jnp.sqrt(sums[:1, :1] / (sums[1:2, :1] + NORM_FLOOR))
    balance_ref[...] = jnp.broadcast_to(balance, balance_ref.shape)
    h_all[r] = (direction - balance * projected).astype(bf)
    hs = [send(h_all.at[r], h_all.at[r], rep(k)) for k in squares]

    for copy in rc:
        copy.wait_recv()
    rd_all[r] = rc_all[...]
    rd = [send(rd_all.at[r], rd_all.at[r], rep(k)) for k in squares]
    send_fourth(3)
    for copy in rd + hs + fourth:
        copy.wait_recv()
    for copy in started:
        copy.wait_send()


def closing_kernel(
    g_ref, h_ref, balance_ref, projected_ref, gate_ref, pj_ref, qm_ref, lm_ref, ls_ref, gm_ref, gq_ref,
    qu_ref, qr_ref, qc_ref, ma_ref, sa_ref, gu_ref, ga_ref, ge_ref,
):
    lifted = jnp.dot(
        pj_ref[...], h_ref[...].reshape(pj_ref.shape[1], qm_ref.shape[1]),
        preferred_element_type=jnp.float32,
    )
    query_update = lifted + balance_ref[:1, :1] * g_ref[0].astype(jnp.float32)
    query_renewed = qm_ref[...] - STEP_RATE * query_update
    qu_ref[...] = query_update
    qr_ref[...] = query_renewed
    qc_ref[...] = query_renewed.astype(jnp.bfloat16)

    @pl.when(pl.program_id(0) == 0)
    def _():
        projected = projected_ref[...]
        ma_ref[...] = BETA_ONE * lm_ref[...] + (1.0 - BETA_ONE) * projected
        sa_ref[...] = BETA_TWO * ls_ref[...] + (1.0 - BETA_TWO) * projected * projected
        nr, nf, _, thin = gate_ref.shape
        for i in range(nr):
            for j in range(nf):
                window = slice((i * nf + j) * thin, (i * nf + j + 1) * thin)
                forget_gradient = gate_ref[i, j]
                average = BETA_ONE * gm_ref[:, window] + (1.0 - BETA_ONE) * forget_gradient
                energy = (
                    BETA_TWO * gq_ref[:, window]
                    + (1.0 - BETA_TWO) * forget_gradient * forget_gradient
                )
                ga_ref[:, window] = average
                ge_ref[:, window] = energy
                gu_ref[:, window] = average / (jnp.sqrt(energy) + EPSILON)


def per_device(nf, nr, nt, *args):
    x, c, gc, gt, pj, qm, lm, ls, gm, gq = args
    width, cols, rank_rows, heads = x.shape[1], c.shape[1], lm.shape[0], gc.shape[0]
    thin = width // (nf * nr)
    fits = (
        width % (nf * nr * 128) == 0 and rank_rows % 16 == 0
        and cols % (PIECES * 128) == 0 and heads % 8 == 0 and nf > 1 and nr == 4 and nt == 2
        and x.shape[0] % 128 == 0 and pj.shape[1] % (nt * 128) == 0
    )
    if not fits:
        return collective_form(*args)
    piece, half, bf, fl = cols // PIECES, thin // 2, jnp.bfloat16, jnp.float32
    rank_all = pj.shape[1]
    scratch = [
        (x.shape, bf), (c.shape, bf), (gc.shape, fl), (gt.shape, fl), (lm.shape, fl),
        (ls.shape, fl), ((nf, nr * thin, rank_all), bf),
        ((PIECES, 2, 2, nf, half, piece), bf), ((PIECES, 2, 2, nf, half, piece), bf),
        ((nf, thin, cols), fl), ((2, nf, half, cols), fl),
        ((PIECES, 2, nf, half, piece), bf), ((PIECES, 2, nf, half, piece), bf),
        ((PIECES, nf - 1, 2, half, piece), bf), ((PIECES, nf - 1, 2, half, piece), bf),
        ((2, half, cols), fl),
        ((x.shape[0], rank_all), fl), ((nr, rank_rows, cols), fl),
        ((nr - 1, rank_rows, cols), bf), ((nr - 1, rank_rows, cols), bf),
        ((nf, rank_rows, cols), bf), ((8, 128), fl), ((nr * nt - 1, 8, 128), fl),
        ((nr, nf, heads, thin), fl), ((nr - 1, nf, heads, thin), fl),
        ((nf, heads, thin), fl), ((nf - 1, heads, thin), fl),
        ((nf, heads, thin), fl),
    ]
    copies = PIECES * 6 + (PIECES + 4) * (nr - 1) + (PIECES + 5) * (nf - 1) + nr * nt - 1
    outs = [
        (qm.shape, fl), (qm.shape, fl), (qm.shape, bf), (lm.shape, fl), (lm.shape, fl),
        (gm.shape, fl), (gm.shape, fl), (gm.shape, fl),
    ]
    between = [
        ((nr, thin, cols), bf), ((nr, rank_rows, cols), bf), ((8, 128), fl), (lm.shape, fl),
        ((nr, nf, heads, thin), fl),
    ]
    vmem = pl.BlockSpec(memory_space=pltpu.VMEM)
    hbm = pl.BlockSpec(memory_space=pltpu.HBM)
    passed = pl.pallas_call(
        functools.partial(fused_kernel, nf, nr, nt),
        out_shape=tuple(jax.ShapeDtypeStruct(*o) for o in between),
        in_specs=[hbm] * 7,
        out_specs=(vmem,) * len(between),
        scratch_shapes=[pltpu.VMEM(*v) for v in scratch]
        + [pltpu.SemaphoreType.DMA((copies,)), pltpu.SemaphoreType.DMA((copies,))]
        + [pltpu.SemaphoreType.DMA((nr * nf + 6,))],
        compiler_params=pltpu.CompilerParams(
            collective_id=0, has_side_effects=True, vmem_limit_bytes=VMEM_GRANT
        ),
    )(*(pltpu.with_memory_space_constraint(v, pltpu.HBM) for v in (x, c, gc, gt, pj, lm, ls)))

    def whole(shape):
        return pl.BlockSpec(shape, lambda i: (0,) * len(shape))

    def rows(width):
        return pl.BlockSpec((thin, width), lambda i: (i, 0))

    return pl.pallas_call(
        closing_kernel,
        grid=(nr,),
        out_shape=tuple(jax.ShapeDtypeStruct(*o) for o in outs),
        in_specs=[pl.BlockSpec((1, thin, cols), lambda i: (i, 0, 0))]
        + [whole(b[0]) for b in between[1:]]
        + [rows(pj.shape[1]), rows(cols), whole(lm.shape), whole(ls.shape)]
        + [whole(gm.shape), whole(gq.shape)],
        out_specs=(rows(cols),) * 3 + tuple(whole(o[0]) for o in outs[3:]),
        compiler_params=pltpu.CompilerParams(vmem_limit_bytes=VMEM_GRANT),
    )(*passed, pj, qm, lm, ls, gm, gq)


def solution(mesh):
    in_specs = (
        P(("fs", "rep"), None),
        P(("fs", "rep"), "tp"),
        P("tp", ("fs", "rep")),
        P("tp", ("fs", "rep")),
        P("fs", None),
        P("fs", "tp"),
        P("rep", "tp"),
        P("rep", "tp"),
        P("tp", None),
        P("tp", None),
    )
    out_specs = (
        P("fs", "tp"),
        P("fs", "tp"),
        P("fs", "tp"),
        P("rep", "tp"),
        P("rep", "tp"),
        P("tp", None),
        P("tp", None),
        P("tp", None),
    )
    return jax.shard_map(
        functools.partial(per_device, mesh.shape["fs"], mesh.shape["rep"], mesh.shape["tp"]),
        mesh=mesh, in_specs=in_specs, out_specs=out_specs, check_vma=False
    )
```

```python
import functools

import jax
import jax.numpy as jnp
from jax import lax
from jax.experimental import pallas as pl
from jax.experimental.pallas import tpu as pltpu
from jax.sharding import PartitionSpec as P

BETA_ONE = 0.9
BETA_TWO = 0.95
STEP_RATE = 0.01
EPSILON = 1e-08
NORM_FLOOR = 1e-06


PIECES = 4
VMEM_GRANT = 32 * 1024 * 1024
MESH = pl.DeviceIdType.MESH
CONTRACT = (((0,), (0,)), ((), ()))


def collective_form(
    attention_input,
    query_cotangent,
    gate_cotangent,
    gate_totals,
    projector,
    query_master,
    lowrank_mean,
    lowrank_square,
    gating_mean,
    gating_square,
):
    tokens_all = attention_input.shape[0] * lax.axis_size("fs") * lax.axis_size("rep")
    norming = 1.0 / tokens_all**0.5
    contract = (((0,), (0,)), ((), ()))
    earlier = jnp.concatenate(
        [jnp.zeros((gate_totals.shape[0], 1), jnp.float32), gate_totals[:, :-1]], axis=1
    )
    gate_logarithm = gate_totals - earlier
    trailing = lax.cumsum(gate_cotangent, axis=1, reverse=True)
    gate_signal = (trailing * -jnp.expm1(gate_logarithm)).astype(jnp.bfloat16)
    gate_partial = jnp.dot(gate_signal, attention_input, preferred_element_type=jnp.float32)
    forget_gradient = lax.psum(gate_partial, ("fs", "rep")) * norming
    thin_rows = lax.psum_scatter(
        lax.dot_general(
            attention_input, query_cotangent, contract, preferred_element_type=jnp.float32
        ),
        ("fs", "rep"),
        scatter_dimension=0,
        tiled=True,
    )
    gradient = lax.all_gather(thin_rows, "rep", axis=0, tiled=True) * norming
    rank_rows = lowrank_mean.shape[0]
    own_factor = lax.dynamic_slice_in_dim(
        projector, lax.axis_index("rep") * rank_rows, rank_rows, 1
    ).astype(jnp.float32)
    rank_partial = lax.dot_general(
        own_factor,
        gradient,
        contract,
        precision=lax.Precision.HIGHEST,
        preferred_element_type=jnp.float32,
    )
    projected = lax.psum(rank_partial, "fs")
    mean_after = BETA_ONE * lowrank_mean + (1.0 - BETA_ONE) * projected
    square_after = BETA_TWO * lowrank_square + (1.0 - BETA_TWO) * projected * projected
    direction = mean_after / (jnp.sqrt(square_after) + EPSILON)
    direction_squares, projected_squares = lax.psum(
        (jnp.sum(direction * direction), jnp.sum(projected * projected)), ("rep", "tp")
    )
    balance = jnp.sqrt(direction_squares / (projected_squares + NORM_FLOOR))
    blended = (direction - balance * projected).astype(jnp.bfloat16)
    lifted = jnp.dot(
        projector,
        lax.all_gather(blended, "rep", axis=0, tiled=True),
        preferred_element_type=jnp.float32,
    )
    query_update = lifted + balance * gradient
    query_renewed = query_master - STEP_RATE * query_update
    query_copy = query_renewed.astype(jnp.bfloat16)
    gating_average = BETA_ONE * gating_mean + (1.0 - BETA_ONE) * forget_gradient
    gating_energy = BETA_TWO * gating_square + (1.0 - BETA_TWO) * forget_gradient * forget_gradient
    gating_update = gating_average / (jnp.sqrt(gating_energy) + EPSILON)
    return (
        query_update,
        query_renewed,
        query_copy,
        mean_after,
        square_after,
        gating_update,
        gating_average,
        gating_energy,
    )


def fused_kernel(
    nf, nr, nt,
    x_hbm, c_hbm, gc_hbm, gt_hbm, pj_hbm, lm_hbm, ls_hbm,
    g_all, h_all, balance_ref, projected_ref, rd_all,
    x_ref, c_ref, c_twin, gc_ref, gt_ref, lm_ref, ls_ref, p_all,
    a_send, a_recv, a_own, a_keep, m_send, m_recv, b_send, b_recv, g_ref,
    xp_ref, d_send, d_recv, e_all, f_send, f_recv,
    ra_send, ra_recv, rb_part, rb_recv, rc_all,
    send_sem, recv_sem, load_sem,
):
    f, r, t = lax.axis_index("fs"), lax.axis_index("rep"), lax.axis_index("tp")
    tokens, width = x_ref.shape
    cols = c_ref.shape[1]
    piece = cols // PIECES
    thin = width // (nf * nr)
    half = thin // 2
    rank_rows = lm_ref.shape[0]
    rank_half = p_all.shape[2]
    norming = 1.0 / (tokens * nf * nr) ** 0.5
    fl, bf = jnp.float32, jnp.bfloat16
    side, line = lax.rem(r, 2), r // 2
    square = [r, line * 2 + (1 - side), (1 - line) * 2 + side, (1 - line) * 2 + (1 - side)]
    fss, squares = list(range(1, nf)), [1, 2, 3]

    def columns(owner, j):
        return pl.ds(pl.multiple_of((j * nr + owner) * thin, thin), thin)

    def load(slot, src, dst):
        pltpu.make_async_copy(src, dst, load_sem.at[slot]).start()

    def settle(sem, ref):
        pltpu.make_async_copy(ref, ref, sem).wait()

    mine = pl.ds(pl.multiple_of(t * rank_half, rank_half), rank_half)
    load(nr, c_hbm, c_ref)
    load(nr + 1, pj_hbm.at[:, mine], p_all.at[f])
    for k in [3, 1, 2, 0]:
        for j in range(nf):
            where = columns(square[k], j)
            load(k, x_hbm.at[:, where], x_ref.at[:, where])
    for i, v in enumerate(((gc_hbm, gc_ref), (gt_hbm, gt_ref), (lm_hbm, lm_ref), (ls_hbm, ls_ref))):
        load(nr + 2 + i, *v)

    groups, arrivals, totals_sent = {}, {}, {}

    def send(group, key, src, dst, where):
        copy = pltpu.make_async_remote_copy(
            src_ref=src, dst_ref=dst,
            send_sem=send_sem.at[groups.setdefault(group, len(groups))],
            recv_sem=recv_sem.at[arrivals.setdefault(key, len(arrivals))],
            device_id=where, device_id_type=MESH,
        )
        copy.start()

    def arrive(key, ref):
        settle(recv_sem.at[arrivals[key]], ref)

    def rep(k):
        return (f, square[k], t)

    def depth(k):
        return (lax.rem(f + k, nf), r, t)

    spots = [(f, square[k], lax.rem(t + dt, nt)) for k in range(4) for dt in range(nt) if k or dt]
    peers = [depth(k) for k in fss] + spots
    barrier = pltpu.get_barrier_semaphore()
    for peer in peers:
        pl.semaphore_signal(barrier, inc=1, device_id=peer, device_id_type=MESH)

    settle(load_sem.at[nr], c_ref)

    def cut(p):
        return slice(p * piece, (p + 1) * piece)

    def fill(k, j):
        value = lax.dot_general(
            x_ref[:, columns(square[k], j)], c_ref[...], CONTRACT, preferred_element_type=fl
        )
        upper, lower = value[:half], value[half:]
        if k == 0:
            a_own[j] = value
        if k == 1:
            a_keep[1, j] = lower
        if k == 2:
            a_keep[0, j] = upper
        for h, part, slot in ((0, upper, {3: 0, 1: 1}), (1, lower, {3: 0, 2: 1})):
            if k in slot:
                small = part.astype(bf)
                for p in range(PIECES):
                    a_send[p, h, slot[k], j] = small[:, cut(p)]

    def ready(k):
        settle(load_sem.at[k], x_ref.at[:, : nf * thin])

    def send_open(h, o):
        send("first", ("open", o), a_send.at[0, h, o], a_recv.at[0, h, o], rep(1 + h))

    def send_first(p):
        for h in range(2):
            send("first", ("first", p), a_send.at[p, h], a_recv.at[p, h], rep(1 + h))

    def send_second(p):
        if p == 0:
            arrive(("open", 0), a_recv.at[0, :, 0])
        else:
            arrive(("first", p), a_recv.at[p])
        for h in range(2):
            for j in range(nf):
                value = a_keep[h, j, :, cut(p)] + a_recv[p, h, 0, j].astype(fl)
                m_send[p, h, j] = value.astype(bf)
            send("second", ("second", p), m_send.at[p, h], m_recv.at[p, h], rep(2 - h))

    def send_third(p):
        if p == 0:
            arrive(("open", 1), a_recv.at[0, :, 1])
        arrive(("second", p), m_recv.at[p])

        def summed(h, j):
            rows = slice(h * half, (h + 1) * half)
            return (
                a_own[j, rows, cut(p)] + a_recv[p, h, 1, j].astype(fl)
                + m_recv[p, h, j].astype(fl)
            )

        for k in fss:
            for h in range(2):
                b_send[p, k - 1, h] = summed(h, lax.rem(f + k, nf)).astype(bf)
            send("third", ("third", p), b_send.at[p, k - 1], b_recv.at[p, k - 1], depth(k))
        for h in range(2):
            g_ref[h, :, cut(p)] = summed(h, f)

    def send_fourth(p):
        arrive(("third", p), b_recv.at[p])
        for h in range(2):
            total = g_ref[h, :, cut(p)]
            for k in fss:
                total = total + b_recv[p, k - 1, h].astype(fl)
            g_all[r, h * half : (h + 1) * half, cut(p)] = (total * norming).astype(bf)
        where = g_all.at[r, :, cut(p)]
        for k in squares:
            send("fourth", "fourth", where, where, rep(k))

    ready(3)
    fill(3, 0)
    fill(3, 1)
    settle(load_sem.at[nr + 1], p_all.at[0])
    pl.semaphore_wait(barrier, len(peers))
    for k in fss:
        send("cast", ("cast", k), p_all.at[f], p_all.at[f], depth(k))
    send("twin", "twin", c_ref, c_twin, (f, r, 1 - t))
    for j in range(2, nf):
        fill(3, j)
    send_open(0, 0)
    send_open(1, 0)
    for k in (1, 2):
        ready(k)
        for j in range(nf):
            fill(k, j)
        send_open(k - 1, 1)
    send_first(1)
    ready(0)
    for j in range(nf):
        fill(0, j)
    send_second(0)
    send_first(2)

    def cast(q):
        place = lax.rem(f + q, nf)
        where = pl.ds(pl.multiple_of(place * nr * thin, nr * thin), nr * thin)
        return jnp.dot(x_ref[:, where], p_all[place], preferred_element_type=fl)

    xp_ref[...] = cast(0)

    for i, ref in enumerate((gc_ref, gt_ref, lm_ref, ls_ref)):
        settle(load_sem.at[nr + 2 + i], ref)
    lanes = 128
    lower = lax.broadcasted_iota(jnp.int32, (lanes, lanes), 0)
    upper = lax.broadcasted_iota(jnp.int32, (lanes, lanes), 1)
    later = (lower >= upper).astype(fl)
    carry = jnp.zeros((gc_ref.shape[0], 1), fl)
    signals = []
    totals = gt_ref[...]
    opens = lax.broadcasted_iota(jnp.int32, totals.shape, 1) == 0
    gate_logarithm = totals - jnp.where(opens, 0.0, pltpu.roll(totals, 1, 1))
    for i in reversed(range(tokens // lanes)):
        window = slice(i * lanes, (i + 1) * lanes)
        own = gc_ref[:, window]
        trailing = carry + jnp.dot(
            own, later, precision=lax.Precision.HIGHEST, preferred_element_type=fl
        )
        carry = carry + jnp.sum(own, axis=1, keepdims=True)
        signals.append(trailing)
    trailing = jnp.concatenate(signals[::-1], axis=1)
    series = jnp.ones_like(gate_logarithm)
    for i in range(8, 1, -1):
        series = 1.0 + gate_logarithm * series / i
    opening = jnp.where(
        gate_logarithm > -0.25, -gate_logarithm * series, 1.0 - jnp.exp(gate_logarithm)
    )
    gate_signal = (trailing * opening).astype(bf)
    gate_partial = jnp.dot(gate_signal, x_ref[...], preferred_element_type=fl)
    for i in range(nr):
        for j in range(nf):
            start = (i * nf + j) * thin
            ra_send[i, j] = gate_partial[:, start : start + thin]
    for k in squares:
        send("ra", "ra", ra_send.at[square[k]], ra_recv.at[k - 1], rep(k))

    for k in fss[:-1]:
        arrive(("cast", k), p_all.at[0])
        xp_ref[...] += cast(nf - k)
    send_second(1)
    arrive(("cast", nf - 1), p_all.at[0])
    cast_all = xp_ref[...] + cast(1)
    high = cast_all.astype(bf)
    low = (cast_all - high.astype(fl)).astype(bf)
    arrive("twin", c_twin)
    crossed = lax.rem(line + t, 2)
    for u, ref in ((1, c_twin), (0, c_ref)):
        partial = lax.dot_general(high, ref[...], CONTRACT, preferred_element_type=fl)
        partial += lax.dot_general(low, ref[...], CONTRACT, preferred_element_type=fl)
        partial = (partial * norming).astype(bf)
        straight, across = partial[:rank_rows], partial[rank_rows:]
        d_send[0, u] = jnp.where(side == 0, straight, across)
        d_send[1, u] = jnp.where(side == 0, across, straight)
        core = lax.rem(t + u, nt)
        near = (f, (1 - crossed) * square[0] + crossed * square[2], core)
        far = (f, (1 - crossed) * square[1] + crossed * square[3], core)
        send("d", "d", d_send.at[1, u], d_recv.at[1 + 2 * crossed], far)
        if u == 1:
            send("d", "d", d_send.at[0, u], d_recv.at[2 * crossed], near)
        else:
            @pl.when(crossed == 0)
            def _():
                d_recv[0] = d_send[0, 0]

            @pl.when(crossed == 1)
            def _():
                send("d1", "d", d_send.at[0, 0], d_recv.at[2], rep(2))

    send_second(2)
    send_first(3)
    send_third(0)
    send_third(1)

    @pl.when(crossed == 0)
    def _():
        arrive("d", d_recv.at[: nr - 1])

    @pl.when(crossed == 1)
    def _():
        arrive("d", d_recv)

    total = d_recv[0].astype(fl)
    for k in squares:
        total = total + d_recv[k].astype(fl)
    e_all[f] = total.astype(bf)
    for k in fss:
        send("e", "e", e_all.at[f], e_all.at[f], depth(k))

    arrive("ra", ra_recv)
    gate_rows = ra_send[r]
    for k in squares:
        gate_rows = gate_rows + ra_recv[k - 1]
    rb_part[...] = gate_rows
    for k in fss:
        send("rb", "rb", rb_part.at[lax.rem(f + k, nf)], rb_recv.at[k - 1], depth(k))

    send_fourth(0)
    send_third(2)
    send_second(3)
    send_fourth(1)
    arrive("rb", rb_recv)
    gate_block = rb_part[f]
    for k in fss:
        gate_block = gate_block + rb_recv[k - 1]
    rc_all[f] = gate_block * norming
    for k in fss:
        send("rc", "rc", rc_all.at[f], rc_all.at[f], depth(k))

    arrive("e", e_all.at[: nf - 1])
    projected = e_all[0].astype(fl)
    for j in fss:
        projected = projected + e_all[j].astype(fl)
    mean_after = BETA_ONE * lm_ref[...] + (1.0 - BETA_ONE) * projected
    square_after = BETA_TWO * ls_ref[...] + (1.0 - BETA_TWO) * projected * projected
    direction = mean_after / (jnp.sqrt(square_after) + EPSILON)
    top = lax.broadcasted_iota(jnp.int32, f_send.shape, 0) == 0
    f_send[...] = jnp.where(top, jnp.sum(direction * direction), jnp.sum(projected * projected))
    for i, spot in enumerate(spots):
        send("f", "f", f_send, f_recv.at[i], spot)
    projected_ref[...] = projected
    send_third(3)
    arrive("f", f_recv)
    sums = f_send[...]
    for i in range(len(spots)):
        sums = sums + f_recv[i]
    balance = jnp.sqrt(sums[:1, :1] / (sums[1:2, :1] + NORM_FLOOR))
    balance_ref[...] = jnp.broadcast_to(balance, balance_ref.shape)
    h_all[r] = (direction - balance * projected).astype(bf)
    for k in squares:
        send("h", "h", h_all.at[r], h_all.at[r], rep(k))

    send_fourth(2)
    arrive("rc", rc_all.at[: nf - 1])
    rd_all[r] = rc_all[...]
    for k in squares:
        send("rd", "rd", rd_all.at[r], rd_all.at[r], rep(k))
    send_fourth(3)
    arrive("rd", rd_all.at[: nr - 1])
    arrive("h", h_all.at[: nr - 1])
    arrive("fourth", g_all.at[: nr - 1])
    sent = {
        "first": a_send, "cast": p_all.at[: nf - 1], "twin": c_ref, "second": m_send,
        "third": b_send, "fourth": g_all.at[: nr - 1], "d": d_recv.at[: nr - 1],
        "e": e_all.at[: nf - 1], "f": f_recv, "h": h_all.at[: nr - 1], "ra": ra_recv,
        "rb": rb_recv, "rc": rc_all.at[: nf - 1], "rd": rd_all.at[: nr - 1],
    }
    for group, ref in sent.items():
        settle(send_sem.at[groups[group]], ref)

    @pl.when(crossed == 1)
    def _():
        settle(send_sem.at[groups["d1"]], d_send.at[0, 0])


def closing_kernel(
    g_ref, h_ref, balance_ref, projected_ref, gate_ref, pj_ref, qm_ref, lm_ref, ls_ref, gm_ref, gq_ref,
    qu_ref, qr_ref, qc_ref, ma_ref, sa_ref, gu_ref, ga_ref, ge_ref,
):
    lifted = jnp.dot(
        pj_ref[...], h_ref[...].reshape(pj_ref.shape[1], qm_ref.shape[1]),
        preferred_element_type=jnp.float32,
    )
    query_update = lifted + balance_ref[:1, :1] * g_ref[0].astype(jnp.float32)
    query_renewed = qm_ref[...] - STEP_RATE * query_update
    qu_ref[...] = query_update
    qr_ref[...] = query_renewed
    qc_ref[...] = query_renewed.astype(jnp.bfloat16)

    @pl.when(pl.program_id(0) == 0)
    def _():
        projected = projected_ref[...]
        ma_ref[...] = BETA_ONE * lm_ref[...] + (1.0 - BETA_ONE) * projected
        sa_ref[...] = BETA_TWO * ls_ref[...] + (1.0 - BETA_TWO) * projected * projected
        nr, nf, _, thin = gate_ref.shape
        for i in range(nr):
            for j in range(nf):
                window = slice((i * nf + j) * thin, (i * nf + j + 1) * thin)
                forget_gradient = gate_ref[i, j]
                average = BETA_ONE * gm_ref[:, window] + (1.0 - BETA_ONE) * forget_gradient
                energy = (
                    BETA_TWO * gq_ref[:, window]
                    + (1.0 - BETA_TWO) * forget_gradient * forget_gradient
                )
                ga_ref[:, window] = average
                ge_ref[:, window] = energy
                gu_ref[:, window] = average / (jnp.sqrt(energy) + EPSILON)


def per_device(nf, nr, nt, *args):
    x, c, gc, gt, pj, qm, lm, ls, gm, gq = args
    width, cols, rank_rows, heads = x.shape[1], c.shape[1], lm.shape[0], gc.shape[0]
    rank_all = pj.shape[1]
    thin = width // (nf * nr)
    fits = (
        width % (nf * nr * 128) == 0 and rank_rows % 16 == 0
        and cols % (PIECES * 128) == 0 and heads % 8 == 0 and nf > 1 and nr == 4 and nt == 2
        and x.shape[0] % 128 == 0 and rank_all % (nt * 128) == 0
    )
    if not fits:
        return collective_form(*args)
    piece, half, bf, fl = cols // PIECES, thin // 2, jnp.bfloat16, jnp.float32
    scratch = [
        (x.shape, bf), (c.shape, bf), (c.shape, bf), (gc.shape, fl), (gt.shape, fl),
        (lm.shape, fl), (ls.shape, fl), ((nf, nr * thin, rank_all // nt), bf),
        ((PIECES, 2, 2, nf, half, piece), bf), ((PIECES, 2, 2, nf, half, piece), bf),
        ((nf, thin, cols), fl), ((2, nf, half, cols), fl),
        ((PIECES, 2, nf, half, piece), bf), ((PIECES, 2, nf, half, piece), bf),
        ((PIECES, nf - 1, 2, half, piece), bf), ((PIECES, nf - 1, 2, half, piece), bf),
        ((2, half, cols), fl),
        ((x.shape[0], rank_all // nt), fl),
        ((2, nt, rank_rows, cols), bf), ((nr, rank_rows, cols), bf),
        ((nf, rank_rows, cols), bf), ((8, 128), fl), ((nr * nt - 1, 8, 128), fl),
        ((nr, nf, heads, thin), fl), ((nr - 1, nf, heads, thin), fl),
        ((nf, heads, thin), fl), ((nf - 1, heads, thin), fl),
        ((nf, heads, thin), fl),
    ]
    outs = [
        (qm.shape, fl), (qm.shape, fl), (qm.shape, bf), (lm.shape, fl), (lm.shape, fl),
        (gm.shape, fl), (gm.shape, fl), (gm.shape, fl),
    ]
    between = [
        ((nr, thin, cols), bf), ((nr, rank_rows, cols), bf), ((8, 128), fl), (lm.shape, fl),
        ((nr, nf, heads, thin), fl),
    ]
    vmem = pl.BlockSpec(memory_space=pltpu.VMEM)
    hbm = pl.BlockSpec(memory_space=pltpu.HBM)
    semaphores = (15, 3 * PIECES + nf + 10, nr + 6)
    passed = pl.pallas_call(
        functools.partial(fused_kernel, nf, nr, nt),
        out_shape=tuple(jax.ShapeDtypeStruct(*o) for o in between),
        in_specs=[hbm] * 7,
        out_specs=(vmem,) * len(between),
        scratch_shapes=[pltpu.VMEM(*v) for v in scratch]
        + [pltpu.SemaphoreType.DMA((n,)) for n in semaphores],
        compiler_params=pltpu.CompilerParams(
            collective_id=0, has_side_effects=True, vmem_limit_bytes=VMEM_GRANT
        ),
    )(*(pltpu.with_memory_space_constraint(v, pltpu.HBM) for v in (x, c, gc, gt, pj, lm, ls)))

    def whole(shape):
        return pl.BlockSpec(shape, lambda i: (0,) * len(shape))

    def rows(width):
        return pl.BlockSpec((thin, width), lambda i: (i, 0))

    return pl.pallas_call(
        closing_kernel,
        grid=(nr,),
        out_shape=tuple(jax.ShapeDtypeStruct(*o) for o in outs),
        in_specs=[pl.BlockSpec((1, thin, cols), lambda i: (i, 0, 0))]
        + [whole(b[0]) for b in between[1:]]
        + [rows(pj.shape[1]), rows(cols), whole(lm.shape), whole(ls.shape)]
        + [whole(gm.shape), whole(gq.shape)],
        out_specs=(rows(cols),) * 3 + tuple(whole(o[0]) for o in outs[3:]),
        compiler_params=pltpu.CompilerParams(vmem_limit_bytes=VMEM_GRANT),
    )(*passed, pj, qm, lm, ls, gm, gq)


def solution(mesh):
    in_specs = (
        P(("fs", "rep"), None),
        P(("fs", "rep"), "tp"),
        P("tp", ("fs", "rep")),
        P("tp", ("fs", "rep")),
        P("fs", None),
        P("fs", "tp"),
        P("rep", "tp"),
        P("rep", "tp"),
        P("tp", None),
        P("tp", None),
    )
    out_specs = (
        P("fs", "tp"),
        P("fs", "tp"),
        P("fs", "tp"),
        P("rep", "tp"),
        P("rep", "tp"),
        P("tp", None),
        P("tp", None),
        P("tp", None),
    )
    return jax.shard_map(
        functools.partial(per_device, mesh.shape["fs"], mesh.shape["rep"], mesh.shape["tp"]),
        mesh=mesh, in_specs=in_specs, out_specs=out_specs, check_vma=False
    )
```

```python
import functools

import jax
import jax.numpy as jnp
from jax import lax
from jax.experimental import pallas as pl
from jax.experimental.pallas import tpu as pltpu
from jax.sharding import PartitionSpec as P

BETA_ONE = 0.9
BETA_TWO = 0.95
STEP_RATE = 0.01
EPSILON = 1e-08
NORM_FLOOR = 1e-06


PIECES = 4
VMEM_GRANT = 32 * 1024 * 1024
MESH = pl.DeviceIdType.MESH
CONTRACT = (((0,), (0,)), ((), ()))


def collective_form(
    attention_input,
    query_cotangent,
    gate_cotangent,
    gate_totals,
    projector,
    query_master,
    lowrank_mean,
    lowrank_square,
    gating_mean,
    gating_square,
):
    tokens_all = attention_input.shape[0] * lax.axis_size("fs") * lax.axis_size("rep")
    norming = 1.0 / tokens_all**0.5
    contract = (((0,), (0,)), ((), ()))
    earlier = jnp.concatenate(
        [jnp.zeros((gate_totals.shape[0], 1), jnp.float32), gate_totals[:, :-1]], axis=1
    )
    gate_logarithm = gate_totals - earlier
    trailing = lax.cumsum(gate_cotangent, axis=1, reverse=True)
    gate_signal = (trailing * -jnp.expm1(gate_logarithm)).astype(jnp.bfloat16)
    gate_partial = jnp.dot(gate_signal, attention_input, preferred_element_type=jnp.float32)
    forget_gradient = lax.psum(gate_partial, ("fs", "rep")) * norming
    thin_rows = lax.psum_scatter(
        lax.dot_general(
            attention_input, query_cotangent, contract, preferred_element_type=jnp.float32
        ),
        ("fs", "rep"),
        scatter_dimension=0,
        tiled=True,
    )
    gradient = lax.all_gather(thin_rows, "rep", axis=0, tiled=True) * norming
    rank_rows = lowrank_mean.shape[0]
    own_factor = lax.dynamic_slice_in_dim(
        projector, lax.axis_index("rep") * rank_rows, rank_rows, 1
    ).astype(jnp.float32)
    rank_partial = lax.dot_general(
        own_factor,
        gradient,
        contract,
        precision=lax.Precision.HIGHEST,
        preferred_element_type=jnp.float32,
    )
    projected = lax.psum(rank_partial, "fs")
    mean_after = BETA_ONE * lowrank_mean + (1.0 - BETA_ONE) * projected
    square_after = BETA_TWO * lowrank_square + (1.0 - BETA_TWO) * projected * projected
    direction = mean_after / (jnp.sqrt(square_after) + EPSILON)
    direction_squares, projected_squares = lax.psum(
        (jnp.sum(direction * direction), jnp.sum(projected * projected)), ("rep", "tp")
    )
    balance = jnp.sqrt(direction_squares / (projected_squares + NORM_FLOOR))
    blended = (direction - balance * projected).astype(jnp.bfloat16)
    lifted = jnp.dot(
        projector,
        lax.all_gather(blended, "rep", axis=0, tiled=True),
        preferred_element_type=jnp.float32,
    )
    query_update = lifted + balance * gradient
    query_renewed = query_master - STEP_RATE * query_update
    query_copy = query_renewed.astype(jnp.bfloat16)
    gating_average = BETA_ONE * gating_mean + (1.0 - BETA_ONE) * forget_gradient
    gating_energy = BETA_TWO * gating_square + (1.0 - BETA_TWO) * forget_gradient * forget_gradient
    gating_update = gating_average / (jnp.sqrt(gating_energy) + EPSILON)
    return (
        query_update,
        query_renewed,
        query_copy,
        mean_after,
        square_after,
        gating_update,
        gating_average,
        gating_energy,
    )


def fused_kernel(
    nf, nr, nt,
    x_hbm, c_hbm, gc_hbm, gt_hbm, pj_hbm, lm_hbm, ls_hbm,
    g_all, h_all, balance_ref, projected_ref, rd_all,
    x_ref, c_ref, c_twin, gc_ref, gt_ref, lm_ref, ls_ref, p_all,
    a_send, a_recv, a_own, a_keep, m_send, m_recv, b_send, b_recv, g_ref,
    xp_ref, d_send, d_recv, e_all, f_send, f_recv,
    ra_send, ra_recv, rb_all,
    send_sem, recv_sem, load_sem,
):
    f, r, t = lax.axis_index("fs"), lax.axis_index("rep"), lax.axis_index("tp")
    tokens, width = x_ref.shape
    cols = c_ref.shape[1]
    piece = cols // PIECES
    thin = width // (nf * nr)
    half = thin // 2
    rank_rows = lm_ref.shape[0]
    rank_half = p_all.shape[2]
    norming = 1.0 / (tokens * nf * nr) ** 0.5
    fl, bf = jnp.float32, jnp.bfloat16
    side, line = lax.rem(r, 2), r // 2
    square = [r, line * 2 + (1 - side), (1 - line) * 2 + side, (1 - line) * 2 + (1 - side)]
    fss, squares = list(range(1, nf)), [1, 2, 3]

    def columns(owner, j):
        return pl.ds(pl.multiple_of((j * nr + owner) * thin, thin), thin)

    def load(slot, src, dst):
        pltpu.make_async_copy(src, dst, load_sem.at[slot]).start()

    def settle(sem, ref):
        pltpu.make_async_copy(ref, ref, sem).wait()

    mine = pl.ds(pl.multiple_of(t * rank_half, rank_half), rank_half)
    load(nr, c_hbm, c_ref)
    load(nr + 1, pj_hbm.at[:, mine], p_all.at[f])
    for k in [3, 1, 2, 0]:
        for j in range(nf):
            where = columns(square[k], j)
            load(k, x_hbm.at[:, where], x_ref.at[:, where])
    for i, v in enumerate(((gc_hbm, gc_ref), (gt_hbm, gt_ref), (lm_hbm, lm_ref), (ls_hbm, ls_ref))):
        load(nr + 2 + i, *v)

    groups, arrivals, totals_sent = {}, {}, {}

    def send(group, key, src, dst, where):
        copy = pltpu.make_async_remote_copy(
            src_ref=src, dst_ref=dst,
            send_sem=send_sem.at[groups.setdefault(group, len(groups))],
            recv_sem=recv_sem.at[arrivals.setdefault(key, len(arrivals))],
            device_id=where, device_id_type=MESH,
        )
        copy.start()

    def arrive(key, ref):
        settle(recv_sem.at[arrivals[key]], ref)

    def rep(k):
        return (f, square[k], t)

    def place(n):
        up = jnp.where(f <= n, n + 1, n)
        down = jnp.where(f <= nf - 2 - n, nf - 1 - n, nf - 2 - n)
        return jnp.where(2 * f < nf, up, down)

    def spread(group, key, src, dst):
        for n in reversed(range(nf - 1)):
            send(group, key, src, dst, (place(n), r, t))

    spots = [(f, square[k], lax.rem(t + dt, nt)) for k in range(4) for dt in range(nt) if k or dt]
    peers = [(place(n), r, t) for n in range(nf - 1)] + spots
    barrier = pltpu.get_barrier_semaphore()
    for peer in peers:
        pl.semaphore_signal(barrier, inc=1, device_id=peer, device_id_type=MESH)

    settle(load_sem.at[nr], c_ref)

    def cut(p):
        return slice(p * piece, (p + 1) * piece)

    def fill(k, j):
        value = lax.dot_general(
            x_ref[:, columns(square[k], j)], c_ref[...], CONTRACT, preferred_element_type=fl
        )
        upper, lower = value[:half], value[half:]
        if k == 0:
            a_own[j] = value
        if k == 1:
            a_keep[1, j] = lower
        if k == 2:
            a_keep[0, j] = upper
        for h, part, slot in ((0, upper, {3: 0, 1: 1}), (1, lower, {3: 0, 2: 1})):
            if k in slot:
                small = part.astype(bf)
                for p in range(PIECES):
                    a_send[p, h, slot[k], j] = small[:, cut(p)]

    def ready(k):
        settle(load_sem.at[k], x_ref.at[:, : nf * thin])

    def send_open(h, o):
        send("first", ("open", o), a_send.at[0, h, o], a_recv.at[0, h, o], rep(1 + h))

    def send_first(p):
        for h in range(2):
            send("first", ("first", p), a_send.at[p, h], a_recv.at[p, h], rep(1 + h))

    def send_second(p):
        if p == 0:
            arrive(("open", 0), a_recv.at[0, :, 0])
        else:
            arrive(("first", p), a_recv.at[p])
        for h in range(2):
            for j in range(nf):
                value = a_keep[h, j, :, cut(p)] + a_recv[p, h, 0, j].astype(fl)
                m_send[p, h, j] = value.astype(bf)
            send("second", ("second", p), m_send.at[p, h], m_recv.at[p, h], rep(2 - h))

    def send_third(p):
        if p == 0:
            arrive(("open", 1), a_recv.at[0, :, 1])
        arrive(("second", p), m_recv.at[p])

        def summed(h, j):
            rows = slice(h * half, (h + 1) * half)
            return (
                a_own[j, rows, cut(p)] + a_recv[p, h, 1, j].astype(fl)
                + m_recv[p, h, j].astype(fl)
            )

        for n in reversed(range(nf - 1)):
            for h in range(2):
                b_send[p, n, h] = summed(h, place(n)).astype(bf)
            send("third", ("third", p), b_send.at[p, n], b_recv.at[p, f], (place(n), r, t))
        for h in range(2):
            g_ref[h, :, cut(p)] = summed(h, f)

    def send_fourth(p):
        arrive(("third", p), b_recv.at[p, : nf - 1])
        for h in range(2):
            total = g_ref[h, :, cut(p)]
            for n in range(nf - 1):
                total = total + b_recv[p, place(n), h].astype(fl)
            g_all[r, h * half : (h + 1) * half, cut(p)] = (total * norming).astype(bf)
        where = g_all.at[r, :, cut(p)]
        for k in squares:
            send("fourth", "fourth", where, where, rep(k))

    ready(3)
    fill(3, 0)
    fill(3, 1)
    settle(load_sem.at[nr + 1], p_all.at[0])
    pl.semaphore_wait(barrier, len(peers))
    cast_sem = 3 * PIECES + 10
    for n in reversed(range(nf - 1)):
        pltpu.make_async_remote_copy(
            src_ref=p_all.at[f], dst_ref=p_all.at[f],
            send_sem=send_sem.at[groups.setdefault("cast", len(groups))],
            recv_sem=recv_sem.at[cast_sem + f],
            device_id=(place(n), r, t), device_id_type=MESH,
        ).start()
    send("twin", "twin", c_ref, c_twin, (f, r, 1 - t))
    for j in range(2, nf):
        fill(3, j)
    send_open(0, 0)
    send_open(1, 0)
    for k in (1, 2):
        ready(k)
        for j in range(nf):
            fill(k, j)
        send_open(k - 1, 1)
    send_first(1)
    ready(0)
    for j in range(nf):
        fill(0, j)
    send_second(0)
    send_first(2)

    def cast(q):
        where = pl.ds(pl.multiple_of(q * nr * thin, nr * thin), nr * thin)
        return jnp.dot(x_ref[:, where], p_all[q], preferred_element_type=fl)

    xp_ref[...] = cast(f)

    for i, ref in enumerate((gc_ref, gt_ref, lm_ref, ls_ref)):
        settle(load_sem.at[nr + 2 + i], ref)
    lanes = 128
    lower = lax.broadcasted_iota(jnp.int32, (lanes, lanes), 0)
    upper = lax.broadcasted_iota(jnp.int32, (lanes, lanes), 1)
    later = (lower >= upper).astype(fl)
    carry = jnp.zeros((gc_ref.shape[0], 1), fl)
    signals = []
    totals = gt_ref[...]
    opens = lax.broadcasted_iota(jnp.int32, totals.shape, 1) == 0
    gate_logarithm = totals - jnp.where(opens, 0.0, pltpu.roll(totals, 1, 1))
    for i in reversed(range(tokens // lanes)):
        window = slice(i * lanes, (i + 1) * lanes)
        own = gc_ref[:, window]
        trailing = carry + jnp.dot(
            own, later, precision=lax.Precision.HIGHEST, preferred_element_type=fl
        )
        carry = carry + jnp.sum(own, axis=1, keepdims=True)
        signals.append(trailing)
    trailing = jnp.concatenate(signals[::-1], axis=1)
    series = jnp.ones_like(gate_logarithm)
    for i in range(8, 1, -1):
        series = 1.0 + gate_logarithm * series / i
    opening = jnp.where(
        gate_logarithm > -0.25, -gate_logarithm * series, 1.0 - jnp.exp(gate_logarithm)
    )
    gate_signal = (trailing * opening).astype(bf)
    gate_partial = jnp.dot(gate_signal, x_ref[...], preferred_element_type=fl)
    for i in range(nr):
        for j in range(nf):
            start = (i * nf + j) * thin
            ra_send[i, j] = gate_partial[:, start : start + thin]
    for k in squares:
        send("ra", "ra", ra_send.at[square[k]], ra_recv.at[k - 1], rep(k))

    def arrive_cast(n):
        settle(recv_sem.at[cast_sem + place(n)], p_all.at[0])
        return cast(place(n))

    xp_ref[...] += arrive_cast(0)
    send_second(1)
    send_first(3)
    for n in range(1, nf - 2):
        xp_ref[...] += arrive_cast(n)
    send_third(0)
    cast_all = xp_ref[...] + arrive_cast(nf - 2)
    high = cast_all.astype(bf)
    low = (cast_all - high.astype(fl)).astype(bf)
    arrive("twin", c_twin)
    crossed = lax.rem(line + t, 2)
    for u, ref in ((1, c_twin), (0, c_ref)):
        partial = lax.dot_general(high, ref[...], CONTRACT, preferred_element_type=fl)
        partial += lax.dot_general(low, ref[...], CONTRACT, preferred_element_type=fl)
        partial = (partial * norming).astype(bf)
        straight, across = partial[:rank_rows], partial[rank_rows:]
        d_send[0, u] = jnp.where(side == 0, straight, across)
        d_send[1, u] = jnp.where(side == 0, across, straight)
        core = lax.rem(t + u, nt)
        near = (f, (1 - crossed) * square[0] + crossed * square[2], core)
        far = (f, (1 - crossed) * square[1] + crossed * square[3], core)
        send("d", "d", d_send.at[1, u], d_recv.at[1 + 2 * crossed], far)
        if u == 1:
            send("d", "d", d_send.at[0, u], d_recv.at[2 * crossed], near)
        else:
            @pl.when(crossed == 0)
            def _():
                d_recv[0] = d_send[0, 0]

            @pl.when(crossed == 1)
            def _():
                send("d1", "d", d_send.at[0, 0], d_recv.at[2], rep(2))

    send_second(2)
    arrive("ra", ra_recv)
    gate_rows = ra_send[r]
    for k in squares:
        gate_rows = gate_rows + ra_recv[k - 1]
    rb_all[f] = gate_rows
    spread("rb", "rb", rb_all.at[f], rb_all.at[f])
    send_third(1)

    @pl.when(crossed == 0)
    def _():
        arrive("d", d_recv.at[: nr - 1])

    @pl.when(crossed == 1)
    def _():
        arrive("d", d_recv)

    total = d_recv[0].astype(fl)
    for k in squares:
        total = total + d_recv[k].astype(fl)
    e_all[f] = total.astype(bf)
    spread("e", "e", e_all.at[f], e_all.at[f])
    send_fourth(0)
    send_second(3)
    send_third(2)
    send_fourth(1)
    send_third(3)

    arrive("e", e_all.at[: nf - 1])
    projected = e_all[0].astype(fl)
    for j in fss:
        projected = projected + e_all[j].astype(fl)
    mean_after = BETA_ONE * lm_ref[...] + (1.0 - BETA_ONE) * projected
    square_after = BETA_TWO * ls_ref[...] + (1.0 - BETA_TWO) * projected * projected
    direction = mean_after / (jnp.sqrt(square_after) + EPSILON)
    top = lax.broadcasted_iota(jnp.int32, f_send.shape, 0) == 0
    f_send[...] = jnp.where(top, jnp.sum(direction * direction), jnp.sum(projected * projected))
    for i, spot in enumerate(spots):
        send("f", "f", f_send, f_recv.at[i], spot)
    projected_ref[...] = projected
    arrive("f", f_recv)
    sums = f_send[...]
    for i in range(len(spots)):
        sums = sums + f_recv[i]
    balance = jnp.sqrt(sums[:1, :1] / (sums[1:2, :1] + NORM_FLOOR))
    balance_ref[...] = jnp.broadcast_to(balance, balance_ref.shape)
    h_all[r] = (direction - balance * projected).astype(bf)
    for k in squares:
        send("h", "h", h_all.at[r], h_all.at[r], rep(k))

    send_fourth(2)
    arrive("rb", rb_all.at[: nf - 1])
    gate_block = rb_all[0]
    for j in fss:
        gate_block = gate_block + rb_all[j]
    rd_all[r] = gate_block * norming
    for k in squares:
        send("rd", "rd", rd_all.at[r], rd_all.at[r], rep(k))
    send_fourth(3)
    arrive("rd", rd_all.at[: nr - 1])
    arrive("h", h_all.at[: nr - 1])
    arrive("fourth", g_all.at[: nr - 1])
    sent = {
        "first": a_send, "cast": p_all.at[: nf - 1], "twin": c_ref, "second": m_send,
        "third": b_send, "fourth": g_all.at[: nr - 1], "d": d_recv.at[: nr - 1],
        "e": e_all.at[: nf - 1], "f": f_recv, "h": h_all.at[: nr - 1], "ra": ra_recv,
        "rb": rb_all.at[: nf - 1], "rd": rd_all.at[: nr - 1],
    }
    for group, ref in sent.items():
        settle(send_sem.at[groups[group]], ref)

    @pl.when(crossed == 1)
    def _():
        settle(send_sem.at[groups["d1"]], d_send.at[0, 0])


def closing_kernel(
    g_ref, h_ref, balance_ref, projected_ref, gate_ref, pj_ref, qm_ref, lm_ref, ls_ref, gm_ref, gq_ref,
    qu_ref, qr_ref, qc_ref, ma_ref, sa_ref, gu_ref, ga_ref, ge_ref,
):
    lifted = jnp.dot(
        pj_ref[...], h_ref[...].reshape(pj_ref.shape[1], qm_ref.shape[1]),
        preferred_element_type=jnp.float32,
    )
    query_update = lifted + balance_ref[:1, :1] * g_ref[0].astype(jnp.float32)
    query_renewed = qm_ref[...] - STEP_RATE * query_update
    qu_ref[...] = query_update
    qr_ref[...] = query_renewed
    qc_ref[...] = query_renewed.astype(jnp.bfloat16)

    @pl.when(pl.program_id(0) == 0)
    def _():
        projected = projected_ref[...]
        ma_ref[...] = BETA_ONE * lm_ref[...] + (1.0 - BETA_ONE) * projected
        sa_ref[...] = BETA_TWO * ls_ref[...] + (1.0 - BETA_TWO) * projected * projected
        nr, nf, _, thin = gate_ref.shape
        for i in range(nr):
            for j in range(nf):
                window = slice((i * nf + j) * thin, (i * nf + j + 1) * thin)
                forget_gradient = gate_ref[i, j]
                average = BETA_ONE * gm_ref[:, window] + (1.0 - BETA_ONE) * forget_gradient
                energy = (
                    BETA_TWO * gq_ref[:, window]
                    + (1.0 - BETA_TWO) * forget_gradient * forget_gradient
                )
                ga_ref[:, window] = average
                ge_ref[:, window] = energy
                gu_ref[:, window] = average / (jnp.sqrt(energy) + EPSILON)


def per_device(nf, nr, nt, *args):
    x, c, gc, gt, pj, qm, lm, ls, gm, gq = args
    width, cols, rank_rows, heads = x.shape[1], c.shape[1], lm.shape[0], gc.shape[0]
    rank_all = pj.shape[1]
    thin = width // (nf * nr)
    fits = (
        width % (nf * nr * 128) == 0 and rank_rows % 16 == 0
        and cols % (PIECES * 128) == 0 and heads % 8 == 0 and nf > 2 and nr == 4 and nt == 2
        and x.shape[0] % 128 == 0 and rank_all % (nt * 128) == 0
    )
    if not fits:
        return collective_form(*args)
    piece, half, bf, fl = cols // PIECES, thin // 2, jnp.bfloat16, jnp.float32
    scratch = [
        (x.shape, bf), (c.shape, bf), (c.shape, bf), (gc.shape, fl), (gt.shape, fl),
        (lm.shape, fl), (ls.shape, fl), ((nf, nr * thin, rank_all // nt), bf),
        ((PIECES, 2, 2, nf, half, piece), bf), ((PIECES, 2, 2, nf, half, piece), bf),
        ((nf, thin, cols), fl), ((2, nf, half, cols), fl),
        ((PIECES, 2, nf, half, piece), bf), ((PIECES, 2, nf, half, piece), bf),
        ((PIECES, nf - 1, 2, half, piece), bf), ((PIECES, nf, 2, half, piece), bf),
        ((2, half, cols), fl),
        ((x.shape[0], rank_all // nt), fl),
        ((2, nt, rank_rows, cols), bf), ((nr, rank_rows, cols), bf),
        ((nf, rank_rows, cols), bf), ((8, 128), fl), ((nr * nt - 1, 8, 128), fl),
        ((nr, nf, heads, thin), fl), ((nr - 1, nf, heads, thin), fl),
        ((nf, nf, heads, thin), fl),
    ]
    outs = [
        (qm.shape, fl), (qm.shape, fl), (qm.shape, bf), (lm.shape, fl), (lm.shape, fl),
        (gm.shape, fl), (gm.shape, fl), (gm.shape, fl),
    ]
    between = [
        ((nr, thin, cols), bf), ((nr, rank_rows, cols), bf), ((8, 128), fl), (lm.shape, fl),
        ((nr, nf, heads, thin), fl),
    ]
    vmem = pl.BlockSpec(memory_space=pltpu.VMEM)
    hbm = pl.BlockSpec(memory_space=pltpu.HBM)
    semaphores = (14, 3 * PIECES + 10 + nf, nr + 6)
    passed = pl.pallas_call(
        functools.partial(fused_kernel, nf, nr, nt),
        out_shape=tuple(jax.ShapeDtypeStruct(*o) for o in between),
        in_specs=[hbm] * 7,
        out_specs=(vmem,) * len(between),
        scratch_shapes=[pltpu.VMEM(*v) for v in scratch]
        + [pltpu.SemaphoreType.DMA((n,)) for n in semaphores],
        compiler_params=pltpu.CompilerParams(
            collective_id=0, has_side_effects=True, vmem_limit_bytes=VMEM_GRANT
        ),
    )(*(pltpu.with_memory_space_constraint(v, pltpu.HBM) for v in (x, c, gc, gt, pj, lm, ls)))

    def whole(shape):
        return pl.BlockSpec(shape, lambda i: (0,) * len(shape))

    def rows(width):
        return pl.BlockSpec((thin, width), lambda i: (i, 0))

    return pl.pallas_call(
        closing_kernel,
        grid=(nr,),
        out_shape=tuple(jax.ShapeDtypeStruct(*o) for o in outs),
        in_specs=[pl.BlockSpec((1, thin, cols), lambda i: (i, 0, 0))]
        + [whole(b[0]) for b in between[1:]]
        + [rows(pj.shape[1]), rows(cols), whole(lm.shape), whole(ls.shape)]
        + [whole(gm.shape), whole(gq.shape)],
        out_specs=(rows(cols),) * 3 + tuple(whole(o[0]) for o in outs[3:]),
        compiler_params=pltpu.CompilerParams(vmem_limit_bytes=VMEM_GRANT),
    )(*passed, pj, qm, lm, ls, gm, gq)


def solution(mesh):
    in_specs = (
        P(("fs", "rep"), None),
        P(("fs", "rep"), "tp"),
        P("tp", ("fs", "rep")),
        P("tp", ("fs", "rep")),
        P("fs", None),
        P("fs", "tp"),
        P("rep", "tp"),
        P("rep", "tp"),
        P("tp", None),
        P("tp", None),
    )
    out_specs = (
        P("fs", "tp"),
        P("fs", "tp"),
        P("fs", "tp"),
        P("rep", "tp"),
        P("rep", "tp"),
        P("tp", None),
        P("tp", None),
        P("tp", None),
    )
    return jax.shard_map(
        functools.partial(per_device, mesh.shape["fs"], mesh.shape["rep"], mesh.shape["tp"]),
        mesh=mesh, in_specs=in_specs, out_specs=out_specs, check_vma=False
    )
```

```python
import functools

import jax
import jax.numpy as jnp
from jax import lax
from jax.experimental import pallas as pl
from jax.experimental.pallas import tpu as pltpu
from jax.sharding import PartitionSpec as P

BETA_ONE = 0.9
BETA_TWO = 0.95
STEP_RATE = 0.01
EPSILON = 1e-08
NORM_FLOOR = 1e-06


PIECES = 4
VMEM_GRANT = 32 * 1024 * 1024
MESH = pl.DeviceIdType.MESH
CONTRACT = (((0,), (0,)), ((), ()))


def collective_form(
    attention_input,
    query_cotangent,
    gate_cotangent,
    gate_totals,
    projector,
    query_master,
    lowrank_mean,
    lowrank_square,
    gating_mean,
    gating_square,
):
    tokens_all = attention_input.shape[0] * lax.axis_size("fs") * lax.axis_size("rep")
    norming = 1.0 / tokens_all**0.5
    contract = (((0,), (0,)), ((), ()))
    earlier = jnp.concatenate(
        [jnp.zeros((gate_totals.shape[0], 1), jnp.float32), gate_totals[:, :-1]], axis=1
    )
    gate_logarithm = gate_totals - earlier
    trailing = lax.cumsum(gate_cotangent, axis=1, reverse=True)
    gate_signal = (trailing * -jnp.expm1(gate_logarithm)).astype(jnp.bfloat16)
    gate_partial = jnp.dot(gate_signal, attention_input, preferred_element_type=jnp.float32)
    forget_gradient = lax.psum(gate_partial, ("fs", "rep")) * norming
    thin_rows = lax.psum_scatter(
        lax.dot_general(
            attention_input, query_cotangent, contract, preferred_element_type=jnp.float32
        ),
        ("fs", "rep"),
        scatter_dimension=0,
        tiled=True,
    )
    gradient = lax.all_gather(thin_rows, "rep", axis=0, tiled=True) * norming
    rank_rows = lowrank_mean.shape[0]
    own_factor = lax.dynamic_slice_in_dim(
        projector, lax.axis_index("rep") * rank_rows, rank_rows, 1
    ).astype(jnp.float32)
    rank_partial = lax.dot_general(
        own_factor,
        gradient,
        contract,
        precision=lax.Precision.HIGHEST,
        preferred_element_type=jnp.float32,
    )
    projected = lax.psum(rank_partial, "fs")
    mean_after = BETA_ONE * lowrank_mean + (1.0 - BETA_ONE) * projected
    square_after = BETA_TWO * lowrank_square + (1.0 - BETA_TWO) * projected * projected
    direction = mean_after / (jnp.sqrt(square_after) + EPSILON)
    direction_squares, projected_squares = lax.psum(
        (jnp.sum(direction * direction), jnp.sum(projected * projected)), ("rep", "tp")
    )
    balance = jnp.sqrt(direction_squares / (projected_squares + NORM_FLOOR))
    blended = (direction - balance * projected).astype(jnp.bfloat16)
    lifted = jnp.dot(
        projector,
        lax.all_gather(blended, "rep", axis=0, tiled=True),
        preferred_element_type=jnp.float32,
    )
    query_update = lifted + balance * gradient
    query_renewed = query_master - STEP_RATE * query_update
    query_copy = query_renewed.astype(jnp.bfloat16)
    gating_average = BETA_ONE * gating_mean + (1.0 - BETA_ONE) * forget_gradient
    gating_energy = BETA_TWO * gating_square + (1.0 - BETA_TWO) * forget_gradient * forget_gradient
    gating_update = gating_average / (jnp.sqrt(gating_energy) + EPSILON)
    return (
        query_update,
        query_renewed,
        query_copy,
        mean_after,
        square_after,
        gating_update,
        gating_average,
        gating_energy,
    )


def fused_kernel(
    nf, nr, nt,
    x_hbm, c_hbm, gc_hbm, gt_hbm, pj_hbm, lm_hbm, ls_hbm,
    g_all, h_all, balance_ref, projected_ref, rd_all,
    x_ref, c_ref, c_twin, gc_ref, gt_ref, lm_ref, ls_ref, p_all,
    a_send, a_recv, a_own, a_keep, m_send, m_recv, b_send, b_recv, v_send, v_recv,
    xp_ref, d_send, d_recv, e_all, f_send, f_recv,
    ra_send, ra_recv, rb_all,
    send_sem, recv_sem, load_sem,
):
    f, r, t = lax.axis_index("fs"), lax.axis_index("rep"), lax.axis_index("tp")
    tokens, width = x_ref.shape
    cols = c_ref.shape[1]
    piece = cols // PIECES
    thin = width // (nf * nr)
    half = thin // 2
    rank_rows = lm_ref.shape[0]
    rank_half = p_all.shape[2]
    norming = 1.0 / (tokens * nf * nr) ** 0.5
    fl, bf = jnp.float32, jnp.bfloat16
    side, line = lax.rem(r, 2), r // 2
    square = [r, line * 2 + (1 - side), (1 - line) * 2 + side, (1 - line) * 2 + (1 - side)]
    fss, squares = list(range(1, nf)), [1, 2, 3]

    def columns(owner, j):
        return pl.ds(pl.multiple_of((j * nr + owner) * thin, thin), thin)

    def load(slot, src, dst):
        pltpu.make_async_copy(src, dst, load_sem.at[slot]).start()

    def settle(sem, ref):
        pltpu.make_async_copy(ref, ref, sem).wait()

    mine = pl.ds(pl.multiple_of(t * rank_half, rank_half), rank_half)
    load(nr, c_hbm, c_ref)
    load(nr + 1, pj_hbm.at[:, mine], p_all.at[f])
    for k in [3, 1, 2, 0]:
        for j in range(nf):
            where = columns(square[k], j)
            load(k, x_hbm.at[:, where], x_ref.at[:, where])
    for i, v in enumerate(((gc_hbm, gc_ref), (gt_hbm, gt_ref), (lm_hbm, lm_ref), (ls_hbm, ls_ref))):
        load(nr + 2 + i, *v)

    groups, arrivals, totals_sent = {}, {}, {}

    def send(group, key, src, dst, where):
        copy = pltpu.make_async_remote_copy(
            src_ref=src, dst_ref=dst,
            send_sem=send_sem.at[groups.setdefault(group, len(groups))],
            recv_sem=recv_sem.at[arrivals.setdefault(key, len(arrivals))],
            device_id=where, device_id_type=MESH,
        )
        copy.start()

    def arrive(key, ref):
        settle(recv_sem.at[arrivals[key]], ref)

    def rep(k):
        return (f, square[k], t)

    def place(n):
        up = jnp.where(f <= n, n + 1, n)
        down = jnp.where(f <= nf - 2 - n, nf - 1 - n, nf - 2 - n)
        return jnp.where(2 * f < nf, up, down)

    def spread(group, key, src, dst):
        for n in reversed(range(nf - 1)):
            send(group, key, src, dst, (place(n), r, t))

    spots = [(f, square[k], lax.rem(t + dt, nt)) for k in range(4) for dt in range(nt) if k or dt]
    peers = [(place(n), r, t) for n in range(nf - 1)] + spots
    barrier = pltpu.get_barrier_semaphore()
    for peer in peers:
        pl.semaphore_signal(barrier, inc=1, device_id=peer, device_id_type=MESH)

    settle(load_sem.at[nr], c_ref)

    def cut(p):
        return slice(p * piece, (p + 1) * piece)

    def fill(k, j):
        value = lax.dot_general(
            x_ref[:, columns(square[k], j)], c_ref[...], CONTRACT, preferred_element_type=fl
        )
        upper, lower = value[:half], value[half:]
        if k == 0:
            a_own[j] = value
        if k == 1:
            a_keep[1, j] = lower
        if k == 2:
            a_keep[0, j] = upper
        for h, part, slot in ((0, upper, {3: 0, 1: 1}), (1, lower, {3: 0, 2: 1})):
            if k in slot:
                small = part.astype(bf)
                for p in range(PIECES):
                    a_send[p, h, slot[k], j] = small[:, cut(p)]

    def ready(k):
        settle(load_sem.at[k], x_ref.at[:, : nf * thin])

    def send_open(h, o):
        send("first", ("open", o), a_send.at[0, h, o], a_recv.at[0, h, o], rep(1 + h))

    def send_first(p):
        for h in range(2):
            send("first", ("first", p), a_send.at[p, h], a_recv.at[p, h], rep(1 + h))

    def send_second(p):
        if p == 0:
            arrive(("open", 0), a_recv.at[0, :, 0])
        else:
            arrive(("first", p), a_recv.at[p])
        for h in range(2):
            for j in range(nf):
                value = a_keep[h, j, :, cut(p)] + a_recv[p, h, 0, j].astype(fl)
                m_send[p, h, j] = value.astype(bf)
            send("second", ("second", p), m_send.at[p, h], m_recv.at[p, h], rep(2 - h))

    mate = f + 1 - 2 * lax.rem(f, 2)
    over = lax.rem(f + nf // 2, nf)
    mate_over = lax.rem(mate + nf // 2, nf)

    def summed(p, h, j):
        rows = slice(h * half, (h + 1) * half)
        return (
            a_own[j, rows, cut(p)] + a_recv[p, h, 1, j].astype(fl) + m_recv[p, h, j].astype(fl)
        )

    def send_third(p):
        if p == 0:
            arrive(("open", 1), a_recv.at[0, :, 1])
        arrive(("second", p), m_recv.at[p])
        for o, j in enumerate((mate_over, mate)):
            for h in range(2):
                b_send[p, o, h] = summed(p, h, j).astype(bf)
        send("third", ("third", p), b_send.at[p], b_recv.at[p], (mate, r, t))

    def send_cross(p):
        arrive(("third", p), b_recv.at[p])
        for h in range(2):
            v_send[p, h] = (summed(p, h, over) + b_recv[p, 0, h].astype(fl)).astype(bf)
        send("cross", ("cross", p), v_send.at[p], v_recv.at[p], (over, r, t))

    def send_fourth(p):
        arrive(("cross", p), v_recv.at[p])
        for h in range(2):
            total = summed(p, h, f) + b_recv[p, 1, h].astype(fl) + v_recv[p, h].astype(fl)
            g_all[r, h * half : (h + 1) * half, cut(p)] = (total * norming).astype(bf)
        where = g_all.at[r, :, cut(p)]
        for k in squares:
            send("fourth", "fourth", where, where, rep(k))

    ready(3)
    fill(3, 0)
    fill(3, 1)
    settle(load_sem.at[nr + 1], p_all.at[0])
    pl.semaphore_wait(barrier, len(peers))
    inner = f * (nf - 1 - f) > 0
    cast_sem = 4 * PIECES + 10
    deep = p_all.shape[1] // 2

    def leaf(q, i):
        return p_all.at[q, i * deep : (i + 1) * deep]

    def cast_arrive(q, i):
        settle(recv_sem.at[cast_sem + 2 * q + i], leaf(0, i))

    def cast_send(group, q, i, where):
        pltpu.make_async_remote_copy(
            src_ref=leaf(q, i), dst_ref=leaf(q, i),
            send_sem=send_sem.at[groups.setdefault(group, len(groups))],
            recv_sem=recv_sem.at[cast_sem + 2 * q + i],
            device_id=(where, r, t), device_id_type=MESH,
        ).start()

    def relay(hop, i):
        @pl.when(inner)
        def _():
            if hop == 1:
                cast_arrive(f - 1, i)
                cast_send("cast", f - 1, i, f + 1)
                cast_arrive(f + 1, i)
                cast_send("cast", f + 1, i, f - 1)
            else:
                cast_arrive(over, i)
                cast_send("cast2", over, i, (nf - 1) * (f - 1))

    @pl.when(inner)
    def _():
        for i in range(2):
            cast_send("cast", f, i, f - 1)
            cast_send("cast", f, i, f + 1)

    @pl.when(jnp.logical_not(inner))
    def _():
        for i in range(2):
            cast_send("cast", f, i, place(0))

    send("twin", "twin", c_ref, c_twin, (f, r, 1 - t))
    for j in range(2, nf):
        fill(3, j)
    send_open(0, 0)
    send_open(1, 0)
    for k in (1, 2):
        ready(k)
        for j in range(nf):
            fill(k, j)
        send_open(k - 1, 1)
    send_first(1)
    ready(0)
    for j in range(nf):
        fill(0, j)
    relay(1, 0)
    send_second(0)
    send_first(2)

    def cast(q):
        where = pl.ds(pl.multiple_of(q * nr * thin, nr * thin), nr * thin)
        return jnp.dot(x_ref[:, where], p_all[q], preferred_element_type=fl)

    xp_ref[...] = cast(f)
    relay(1, 1)

    for i, ref in enumerate((gc_ref, gt_ref, lm_ref, ls_ref)):
        settle(load_sem.at[nr + 2 + i], ref)
    lanes = 128
    lower = lax.broadcasted_iota(jnp.int32, (lanes, lanes), 0)
    upper = lax.broadcasted_iota(jnp.int32, (lanes, lanes), 1)
    later = (lower >= upper).astype(fl)
    carry = jnp.zeros((gc_ref.shape[0], 1), fl)
    signals = []
    totals = gt_ref[...]
    opens = lax.broadcasted_iota(jnp.int32, totals.shape, 1) == 0
    gate_logarithm = totals - jnp.where(opens, 0.0, pltpu.roll(totals, 1, 1))
    for i in reversed(range(tokens // lanes)):
        window = slice(i * lanes, (i + 1) * lanes)
        own = gc_ref[:, window]
        trailing = carry + jnp.dot(
            own, later, precision=lax.Precision.HIGHEST, preferred_element_type=fl
        )
        carry = carry + jnp.sum(own, axis=1, keepdims=True)
        signals.append(trailing)
    trailing = jnp.concatenate(signals[::-1], axis=1)
    series = jnp.ones_like(gate_logarithm)
    for i in range(8, 1, -1):
        series = 1.0 + gate_logarithm * series / i
    opening = jnp.where(
        gate_logarithm > -0.25, -gate_logarithm * series, 1.0 - jnp.exp(gate_logarithm)
    )
    gate_signal = (trailing * opening).astype(bf)
    gate_partial = jnp.dot(gate_signal, x_ref[...], preferred_element_type=fl)
    for i in range(nr):
        for j in range(nf):
            start = (i * nf + j) * thin
            ra_send[i, j] = gate_partial[:, start : start + thin]
    for k in squares:
        send("ra", "ra", ra_send.at[square[k]], ra_recv.at[k - 1], rep(k))

    relay(2, 0)
    send_second(1)
    relay(2, 1)
    send_third(0)

    def arrive_cast(n):
        @pl.when(jnp.logical_not(inner))
        def _():
            for i in range(2):
                cast_arrive(place(n), i)
        return cast(place(n))

    xp_ref[...] += arrive_cast(0)
    xp_ref[...] += arrive_cast(1)
    cast_all = xp_ref[...] + arrive_cast(2)
    high = cast_all.astype(bf)
    low = (cast_all - high.astype(fl)).astype(bf)
    arrive("twin", c_twin)
    crossed = lax.rem(line + t, 2)
    for u, ref in ((1, c_twin), (0, c_ref)):
        partial = lax.dot_general(high, ref[...], CONTRACT, preferred_element_type=fl)
        partial += lax.dot_general(low, ref[...], CONTRACT, preferred_element_type=fl)
        partial = (partial * norming).astype(bf)
        straight, across = partial[:rank_rows], partial[rank_rows:]
        d_send[0, u] = jnp.where(side == 0, straight, across)
        d_send[1, u] = jnp.where(side == 0, across, straight)
        core = lax.rem(t + u, nt)
        near = (f, (1 - crossed) * square[0] + crossed * square[2], core)
        far = (f, (1 - crossed) * square[1] + crossed * square[3], core)
        send("d", "d", d_send.at[1, u], d_recv.at[1 + 2 * crossed], far)
        if u == 1:
            send("d", "d", d_send.at[0, u], d_recv.at[2 * crossed], near)
        else:
            @pl.when(crossed == 0)
            def _():
                d_recv[0] = d_send[0, 0]

            @pl.when(crossed == 1)
            def _():
                send("d1", "d", d_send.at[0, 0], d_recv.at[2], rep(2))

    send_second(2)
    send_first(3)
    send_cross(0)
    send_third(1)
    arrive("ra", ra_recv)
    gate_rows = ra_send[r]
    for k in squares:
        gate_rows = gate_rows + ra_recv[k - 1]
    rb_all[f] = gate_rows
    spread("rb", "rb", rb_all.at[f], rb_all.at[f])

    @pl.when(crossed == 0)
    def _():
        arrive("d", d_recv.at[: nr - 1])

    @pl.when(crossed == 1)
    def _():
        arrive("d", d_recv)

    total = d_recv[0].astype(fl)
    for k in squares:
        total = total + d_recv[k].astype(fl)
    e_all[f] = total.astype(bf)
    spread("e", "e", e_all.at[f], e_all.at[f])
    send_cross(1)
    send_fourth(0)
    send_third(2)
    send_second(3)
    send_cross(2)

    arrive("e", e_all.at[: nf - 1])
    projected = e_all[0].astype(fl)
    for j in fss:
        projected = projected + e_all[j].astype(fl)
    mean_after = BETA_ONE * lm_ref[...] + (1.0 - BETA_ONE) * projected
    square_after = BETA_TWO * ls_ref[...] + (1.0 - BETA_TWO) * projected * projected
    direction = mean_after / (jnp.sqrt(square_after) + EPSILON)
    top = lax.broadcasted_iota(jnp.int32, f_send.shape, 0) == 0
    f_send[...] = jnp.where(top, jnp.sum(direction * direction), jnp.sum(projected * projected))
    for i, spot in enumerate(spots):
        send("f", "f", f_send, f_recv.at[i], spot)
    projected_ref[...] = projected
    send_fourth(1)
    send_third(3)
    arrive("f", f_recv)
    sums = f_send[...]
    for i in range(len(spots)):
        sums = sums + f_recv[i]
    balance = jnp.sqrt(sums[:1, :1] / (sums[1:2, :1] + NORM_FLOOR))
    balance_ref[...] = jnp.broadcast_to(balance, balance_ref.shape)
    h_all[r] = (direction - balance * projected).astype(bf)
    for k in squares:
        send("h", "h", h_all.at[r], h_all.at[r], rep(k))

    send_fourth(2)
    arrive("rb", rb_all.at[: nf - 1])
    gate_block = rb_all[0]
    for j in fss:
        gate_block = gate_block + rb_all[j]
    rd_all[r] = gate_block * norming
    for k in squares:
        send("rd", "rd", rd_all.at[r], rd_all.at[r], rep(k))
    send_cross(3)
    send_fourth(3)
    arrive("rd", rd_all.at[: nr - 1])
    arrive("h", h_all.at[: nr - 1])
    arrive("fourth", g_all.at[: nr - 1])
    sent = {
        "first": a_send, "twin": c_ref, "second": m_send,
        "third": b_send, "cross": v_send, "fourth": g_all.at[: nr - 1], "d": d_recv.at[: nr - 1],
        "e": e_all.at[: nf - 1], "f": f_recv, "h": h_all.at[: nr - 1], "ra": ra_recv,
        "rb": rb_all.at[: nf - 1], "rd": rd_all.at[: nr - 1],
    }
    for group, ref in sent.items():
        settle(send_sem.at[groups[group]], ref)

    @pl.when(inner)
    def _():
        settle(send_sem.at[groups["cast"]], p_all)
        settle(send_sem.at[groups["cast2"]], p_all.at[0])

    @pl.when(jnp.logical_not(inner))
    def _():
        settle(send_sem.at[groups["cast"]], p_all.at[0])

    @pl.when(crossed == 1)
    def _():
        settle(send_sem.at[groups["d1"]], d_send.at[0, 0])


def closing_kernel(
    g_ref, h_ref, balance_ref, projected_ref, gate_ref, pj_ref, qm_ref, lm_ref, ls_ref, gm_ref, gq_ref,
    qu_ref, qr_ref, qc_ref, ma_ref, sa_ref, gu_ref, ga_ref, ge_ref,
):
    lifted = jnp.dot(
        pj_ref[...], h_ref[...].reshape(pj_ref.shape[1], qm_ref.shape[1]),
        preferred_element_type=jnp.float32,
    )
    query_update = lifted + balance_ref[:1, :1] * g_ref[0].astype(jnp.float32)
    query_renewed = qm_ref[...] - STEP_RATE * query_update
    qu_ref[...] = query_update
    qr_ref[...] = query_renewed
    qc_ref[...] = query_renewed.astype(jnp.bfloat16)

    @pl.when(pl.program_id(0) == 0)
    def _():
        projected = projected_ref[...]
        ma_ref[...] = BETA_ONE * lm_ref[...] + (1.0 - BETA_ONE) * projected
        sa_ref[...] = BETA_TWO * ls_ref[...] + (1.0 - BETA_TWO) * projected * projected
        nr, nf, _, thin = gate_ref.shape
        for i in range(nr):
            for j in range(nf):
                window = slice((i * nf + j) * thin, (i * nf + j + 1) * thin)
                forget_gradient = gate_ref[i, j]
                average = BETA_ONE * gm_ref[:, window] + (1.0 - BETA_ONE) * forget_gradient
                energy = (
                    BETA_TWO * gq_ref[:, window]
                    + (1.0 - BETA_TWO) * forget_gradient * forget_gradient
                )
                ga_ref[:, window] = average
                ge_ref[:, window] = energy
                gu_ref[:, window] = average / (jnp.sqrt(energy) + EPSILON)


def per_device(nf, nr, nt, *args):
    x, c, gc, gt, pj, qm, lm, ls, gm, gq = args
    width, cols, rank_rows, heads = x.shape[1], c.shape[1], lm.shape[0], gc.shape[0]
    rank_all = pj.shape[1]
    thin = width // (nf * nr)
    fits = (
        width % (nf * nr * 128) == 0 and rank_rows % 16 == 0
        and cols % (PIECES * 128) == 0 and heads % 8 == 0 and nf == 4 and nr == 4 and nt == 2
        and x.shape[0] % 128 == 0 and rank_all % (nt * 128) == 0
    )
    if not fits:
        return collective_form(*args)
    piece, half, bf, fl = cols // PIECES, thin // 2, jnp.bfloat16, jnp.float32
    scratch = [
        (x.shape, bf), (c.shape, bf), (c.shape, bf), (gc.shape, fl), (gt.shape, fl),
        (lm.shape, fl), (ls.shape, fl), ((nf, nr * thin, rank_all // nt), bf),
        ((PIECES, 2, 2, nf, half, piece), bf), ((PIECES, 2, 2, nf, half, piece), bf),
        ((nf, thin, cols), fl), ((2, nf, half, cols), fl),
        ((PIECES, 2, nf, half, piece), bf), ((PIECES, 2, nf, half, piece), bf),
        ((PIECES, 2, 2, half, piece), bf), ((PIECES, 2, 2, half, piece), bf),
        ((PIECES, 2, half, piece), bf), ((PIECES, 2, half, piece), bf),
        ((x.shape[0], rank_all // nt), fl),
        ((2, nt, rank_rows, cols), bf), ((nr, rank_rows, cols), bf),
        ((nf, rank_rows, cols), bf), ((8, 128), fl), ((nr * nt - 1, 8, 128), fl),
        ((nr, nf, heads, thin), fl), ((nr - 1, nf, heads, thin), fl),
        ((nf, nf, heads, thin), fl),
    ]
    outs = [
        (qm.shape, fl), (qm.shape, fl), (qm.shape, bf), (lm.shape, fl), (lm.shape, fl),
        (gm.shape, fl), (gm.shape, fl), (gm.shape, fl),
    ]
    between = [
        ((nr, thin, cols), bf), ((nr, rank_rows, cols), bf), ((8, 128), fl), (lm.shape, fl),
        ((nr, nf, heads, thin), fl),
    ]
    vmem = pl.BlockSpec(memory_space=pltpu.VMEM)
    hbm = pl.BlockSpec(memory_space=pltpu.HBM)
    semaphores = (16, 4 * PIECES + 10 + 2 * nf, nr + 6)
    passed = pl.pallas_call(
        functools.partial(fused_kernel, nf, nr, nt),
        out_shape=tuple(jax.ShapeDtypeStruct(*o) for o in between),
        in_specs=[hbm] * 7,
        out_specs=(vmem,) * len(between),
        scratch_shapes=[pltpu.VMEM(*v) for v in scratch]
        + [pltpu.SemaphoreType.DMA((n,)) for n in semaphores],
        compiler_params=pltpu.CompilerParams(
            collective_id=0, has_side_effects=True, vmem_limit_bytes=VMEM_GRANT
        ),
    )(*(pltpu.with_memory_space_constraint(v, pltpu.HBM) for v in (x, c, gc, gt, pj, lm, ls)))

    def whole(shape):
        return pl.BlockSpec(shape, lambda i: (0,) * len(shape))

    def rows(width):
        return pl.BlockSpec((thin, width), lambda i: (i, 0))

    return pl.pallas_call(
        closing_kernel,
        grid=(nr,),
        out_shape=tuple(jax.ShapeDtypeStruct(*o) for o in outs),
        in_specs=[pl.BlockSpec((1, thin, cols), lambda i: (i, 0, 0))]
        + [whole(b[0]) for b in between[1:]]
        + [rows(pj.shape[1]), rows(cols), whole(lm.shape), whole(ls.shape)]
        + [whole(gm.shape), whole(gq.shape)],
        out_specs=(rows(cols),) * 3 + tuple(whole(o[0]) for o in outs[3:]),
        compiler_params=pltpu.CompilerParams(vmem_limit_bytes=VMEM_GRANT),
    )(*passed, pj, qm, lm, ls, gm, gq)


def solution(mesh):
    in_specs = (
        P(("fs", "rep"), None),
        P(("fs", "rep"), "tp"),
        P("tp", ("fs", "rep")),
        P("tp", ("fs", "rep")),
        P("fs", None),
        P("fs", "tp"),
        P("rep", "tp"),
        P("rep", "tp"),
        P("tp", None),
        P("tp", None),
    )
    out_specs = (
        P("fs", "tp"),
        P("fs", "tp"),
        P("fs", "tp"),
        P("rep", "tp"),
        P("rep", "tp"),
        P("tp", None),
        P("tp", None),
        P("tp", None),
    )
    return jax.shard_map(
        functools.partial(per_device, mesh.shape["fs"], mesh.shape["rep"], mesh.shape["tp"]),
        mesh=mesh, in_specs=in_specs, out_specs=out_specs, check_vma=False
    )
```

```python
import functools

import jax
import jax.numpy as jnp
from jax import lax
from jax.experimental import pallas as pl
from jax.experimental.pallas import tpu as pltpu
from jax.sharding import PartitionSpec as P

BETA_ONE = 0.9
BETA_TWO = 0.95
STEP_RATE = 0.01
EPSILON = 1e-08
NORM_FLOOR = 1e-06


PIECES = 4
LEAVES = 4
VMEM_GRANT = 32 * 1024 * 1024
MESH = pl.DeviceIdType.MESH
CONTRACT = (((0,), (0,)), ((), ()))


def collective_form(
    attention_input,
    query_cotangent,
    gate_cotangent,
    gate_totals,
    projector,
    query_master,
    lowrank_mean,
    lowrank_square,
    gating_mean,
    gating_square,
):
    tokens_all = attention_input.shape[0] * lax.axis_size("fs") * lax.axis_size("rep")
    norming = 1.0 / tokens_all**0.5
    contract = (((0,), (0,)), ((), ()))
    earlier = jnp.concatenate(
        [jnp.zeros((gate_totals.shape[0], 1), jnp.float32), gate_totals[:, :-1]], axis=1
    )
    gate_logarithm = gate_totals - earlier
    trailing = lax.cumsum(gate_cotangent, axis=1, reverse=True)
    gate_signal = (trailing * -jnp.expm1(gate_logarithm)).astype(jnp.bfloat16)
    gate_partial = jnp.dot(gate_signal, attention_input, preferred_element_type=jnp.float32)
    forget_gradient = lax.psum(gate_partial, ("fs", "rep")) * norming
    thin_rows = lax.psum_scatter(
        lax.dot_general(
            attention_input, query_cotangent, contract, preferred_element_type=jnp.float32
        ),
        ("fs", "rep"),
        scatter_dimension=0,
        tiled=True,
    )
    gradient = lax.all_gather(thin_rows, "rep", axis=0, tiled=True) * norming
    rank_rows = lowrank_mean.shape[0]
    own_factor = lax.dynamic_slice_in_dim(
        projector, lax.axis_index("rep") * rank_rows, rank_rows, 1
    ).astype(jnp.float32)
    rank_partial = lax.dot_general(
        own_factor,
        gradient,
        contract,
        precision=lax.Precision.HIGHEST,
        preferred_element_type=jnp.float32,
    )
    projected = lax.psum(rank_partial, "fs")
    mean_after = BETA_ONE * lowrank_mean + (1.0 - BETA_ONE) * projected
    square_after = BETA_TWO * lowrank_square + (1.0 - BETA_TWO) * projected * projected
    direction = mean_after / (jnp.sqrt(square_after) + EPSILON)
    direction_squares, projected_squares = lax.psum(
        (jnp.sum(direction * direction), jnp.sum(projected * projected)), ("rep", "tp")
    )
    balance = jnp.sqrt(direction_squares / (projected_squares + NORM_FLOOR))
    blended = (direction - balance * projected).astype(jnp.bfloat16)
    lifted = jnp.dot(
        projector,
        lax.all_gather(blended, "rep", axis=0, tiled=True),
        preferred_element_type=jnp.float32,
    )
    query_update = lifted + balance * gradient
    query_renewed = query_master - STEP_RATE * query_update
    query_copy = query_renewed.astype(jnp.bfloat16)
    gating_average = BETA_ONE * gating_mean + (1.0 - BETA_ONE) * forget_gradient
    gating_energy = BETA_TWO * gating_square + (1.0 - BETA_TWO) * forget_gradient * forget_gradient
    gating_update = gating_average / (jnp.sqrt(gating_energy) + EPSILON)
    return (
        query_update,
        query_renewed,
        query_copy,
        mean_after,
        square_after,
        gating_update,
        gating_average,
        gating_energy,
    )


def fused_kernel(
    nf, nr, nt,
    x_hbm, c_hbm, gc_hbm, gt_hbm, pj_hbm, lm_hbm, ls_hbm,
    g_all, h_all, balance_ref, projected_ref, rd_all,
    x_ref, c_ref, c_twin, gc_ref, gt_ref, lm_ref, ls_ref, p_all,
    a_send, a_recv, a_own, a_keep, m_send, m_recv, b_send, b_recv, v_send, v_recv,
    xp_ref, d_send, d_recv, e_all, f_send, f_recv,
    ra_send, ra_recv, rb_all,
    send_sem, recv_sem, load_sem,
):
    f, r, t = lax.axis_index("fs"), lax.axis_index("rep"), lax.axis_index("tp")
    tokens, width = x_ref.shape
    cols = c_ref.shape[1]
    piece = cols // PIECES
    thin = width // (nf * nr)
    half = thin // 2
    rank_rows = lm_ref.shape[0]
    rank_half = p_all.shape[2]
    norming = 1.0 / (tokens * nf * nr) ** 0.5
    fl, bf = jnp.float32, jnp.bfloat16
    side, line = lax.rem(r, 2), r // 2
    square = [r, line * 2 + (1 - side), (1 - line) * 2 + side, (1 - line) * 2 + (1 - side)]
    fss, squares = list(range(1, nf)), [1, 2, 3]

    def columns(owner, j):
        return pl.ds(pl.multiple_of((j * nr + owner) * thin, thin), thin)

    def load(slot, src, dst):
        pltpu.make_async_copy(src, dst, load_sem.at[slot]).start()

    def settle(sem, ref):
        pltpu.make_async_copy(ref, ref, sem).wait()

    mine = pl.ds(pl.multiple_of(t * rank_half, rank_half), rank_half)
    load(nr + 1, pj_hbm.at[:, mine], p_all.at[f])
    load(nr, c_hbm, c_ref)
    for k in [3, 1, 2, 0]:
        for j in range(nf):
            where = columns(square[k], j)
            load(k, x_hbm.at[:, where], x_ref.at[:, where])
    for i, v in enumerate(((gc_hbm, gc_ref), (gt_hbm, gt_ref), (lm_hbm, lm_ref), (ls_hbm, ls_ref))):
        load(nr + 2 + i, *v)

    groups, arrivals, totals_sent = {}, {}, {}

    def send(group, key, src, dst, where):
        copy = pltpu.make_async_remote_copy(
            src_ref=src, dst_ref=dst,
            send_sem=send_sem.at[groups.setdefault(group, len(groups))],
            recv_sem=recv_sem.at[arrivals.setdefault(key, len(arrivals))],
            device_id=where, device_id_type=MESH,
        )
        copy.start()

    def arrive(key, ref):
        settle(recv_sem.at[arrivals[key]], ref)

    def rep(k):
        return (f, square[k], t)

    def place(n):
        up = jnp.where(f <= n, n + 1, n)
        down = jnp.where(f <= nf - 2 - n, nf - 1 - n, nf - 2 - n)
        return jnp.where(2 * f < nf, up, down)

    def spread(group, key, src, dst):
        for n in reversed(range(nf - 1)):
            send(group, key, src, dst, (place(n), r, t))

    spots = [(f, square[k], lax.rem(t + dt, nt)) for k in range(4) for dt in range(nt) if k or dt]
    peers = [(place(n), r, t) for n in range(nf - 1)] + spots
    barrier = pltpu.get_barrier_semaphore()
    for peer in peers:
        pl.semaphore_signal(barrier, inc=1, device_id=peer, device_id_type=MESH)

    def cut(p):
        return slice(p * piece, (p + 1) * piece)

    def fill(k, j):
        value = lax.dot_general(
            x_ref[:, columns(square[k], j)], c_ref[...], CONTRACT, preferred_element_type=fl
        )
        upper, lower = value[:half], value[half:]
        if k == 0:
            a_own[j] = value
        if k == 1:
            a_keep[1, j] = lower
        if k == 2:
            a_keep[0, j] = upper
        for h, part, slot in ((0, upper, {3: 0, 1: 1}), (1, lower, {3: 0, 2: 1})):
            if k in slot:
                small = part.astype(bf)
                for p in range(PIECES):
                    a_send[p, h, slot[k], j] = small[:, cut(p)]

    def ready(k):
        settle(load_sem.at[k], x_ref.at[:, : nf * thin])

    def send_open(h, o):
        send("first", ("open", o), a_send.at[0, h, o], a_recv.at[0, h, o], rep(1 + h))

    def send_first(p):
        for h in range(2):
            send("first", ("first", p), a_send.at[p, h], a_recv.at[p, h], rep(1 + h))

    def send_second(p):
        if p == 0:
            arrive(("open", 0), a_recv.at[0, :, 0])
        else:
            arrive(("first", p), a_recv.at[p])
        for h in range(2):
            for j in range(nf):
                value = a_keep[h, j, :, cut(p)] + a_recv[p, h, 0, j].astype(fl)
                m_send[p, h, j] = value.astype(bf)
            send("second", ("second", p), m_send.at[p, h], m_recv.at[p, h], rep(2 - h))

    mate = f + 1 - 2 * lax.rem(f, 2)
    over = lax.rem(f + nf // 2, nf)
    mate_over = lax.rem(mate + nf // 2, nf)

    def summed(p, h, j):
        rows = slice(h * half, (h + 1) * half)
        return (
            a_own[j, rows, cut(p)] + a_recv[p, h, 1, j].astype(fl) + m_recv[p, h, j].astype(fl)
        )

    def send_third(p):
        if p == 0:
            arrive(("open", 1), a_recv.at[0, :, 1])
        arrive(("second", p), m_recv.at[p])
        for o, j in enumerate((mate_over, mate)):
            for h in range(2):
                b_send[p, o, h] = summed(p, h, j).astype(bf)
        send("third", ("third", p), b_send.at[p], b_recv.at[p], (mate, r, t))

    def send_cross(p):
        arrive(("third", p), b_recv.at[p])
        for h in range(2):
            v_send[p, h] = (summed(p, h, over) + b_recv[p, 0, h].astype(fl)).astype(bf)
        send("cross", ("cross", p), v_send.at[p], v_recv.at[p], (over, r, t))

    def send_fourth(p):
        arrive(("cross", p), v_recv.at[p])
        for h in range(2):
            total = summed(p, h, f) + b_recv[p, 1, h].astype(fl) + v_recv[p, h].astype(fl)
            g_all[r, h * half : (h + 1) * half, cut(p)] = (total * norming).astype(bf)
        where = g_all.at[r, :, cut(p)]
        for k in squares:
            send("fourth", "fourth", where, where, rep(k))

    settle(load_sem.at[nr + 1], p_all.at[0])
    pl.semaphore_wait(barrier, len(peers))
    inner = f * (nf - 1 - f) > 0
    cast_sem = 4 * PIECES + 10
    deep = p_all.shape[1] // LEAVES

    def leaf(q, i):
        return p_all.at[q, i * deep : (i + 1) * deep]

    def cast_arrive(q, i):
        settle(recv_sem.at[cast_sem + LEAVES * q + i], leaf(0, i))

    def cast_send(group, q, i, where):
        pltpu.make_async_remote_copy(
            src_ref=leaf(q, i), dst_ref=leaf(q, i),
            send_sem=send_sem.at[groups.setdefault(group, len(groups))],
            recv_sem=recv_sem.at[cast_sem + LEAVES * q + i],
            device_id=(where, r, t), device_id_type=MESH,
        ).start()

    def relay(hop, leaves):
        @pl.when(inner)
        def _():
            for i in leaves:
                relay_leaf(hop, i)

    def relay_leaf(hop, i):
        if hop == 1:
            cast_arrive(f - 1, i)
            cast_send("cast", f - 1, i, f + 1)
            cast_arrive(f + 1, i)
            cast_send("cast", f + 1, i, f - 1)
        else:
            cast_arrive(over, i)
            cast_send("cast2", over, i, (nf - 1) * (f - 1))

    @pl.when(inner)
    def _():
        for i in range(LEAVES):
            cast_send("cast", f, i, f - 1)
            cast_send("cast", f, i, f + 1)

    @pl.when(jnp.logical_not(inner))
    def _():
        for i in range(LEAVES):
            cast_send("cast", f, i, place(0))

    settle(load_sem.at[nr], c_ref)
    send("twin", "twin", c_ref, c_twin, (f, r, 1 - t))
    ready(3)
    for j in range(nf):
        fill(3, j)
    send_open(0, 0)
    send_open(1, 0)
    for k in (1, 2):
        ready(k)
        for j in range(nf):
            fill(k, j)
        send_open(k - 1, 1)
    send_first(1)
    ready(0)
    for j in range(nf):
        fill(0, j)
    relay(1, range(LEAVES))
    send_second(0)

    def cast(q):
        where = pl.ds(pl.multiple_of(q * nr * thin, nr * thin), nr * thin)
        return jnp.dot(x_ref[:, where], p_all[q], preferred_element_type=fl)

    xp_ref[...] = cast(f)
    relay(2, range(LEAVES))

    for i, ref in enumerate((gc_ref, gt_ref, lm_ref, ls_ref)):
        settle(load_sem.at[nr + 2 + i], ref)
    lanes = 128
    lower = lax.broadcasted_iota(jnp.int32, (lanes, lanes), 0)
    upper = lax.broadcasted_iota(jnp.int32, (lanes, lanes), 1)
    later = (lower >= upper).astype(fl)
    carry = jnp.zeros((gc_ref.shape[0], 1), fl)
    signals = []
    totals = gt_ref[...]
    opens = lax.broadcasted_iota(jnp.int32, totals.shape, 1) == 0
    gate_logarithm = totals - jnp.where(opens, 0.0, pltpu.roll(totals, 1, 1))
    for i in reversed(range(tokens // lanes)):
        window = slice(i * lanes, (i + 1) * lanes)
        own = gc_ref[:, window]
        trailing = carry + jnp.dot(
            own, later, precision=lax.Precision.HIGHEST, preferred_element_type=fl
        )
        carry = carry + jnp.sum(own, axis=1, keepdims=True)
        signals.append(trailing)
    trailing = jnp.concatenate(signals[::-1], axis=1)
    series = jnp.ones_like(gate_logarithm)
    for i in range(8, 1, -1):
        series = 1.0 + gate_logarithm * series / i
    opening = jnp.where(
        gate_logarithm > -0.25, -gate_logarithm * series, 1.0 - jnp.exp(gate_logarithm)
    )
    gate_signal = (trailing * opening).astype(bf)
    gate_partial = jnp.dot(gate_signal, x_ref[...], preferred_element_type=fl)
    for i in range(nr):
        for j in range(nf):
            start = (i * nf + j) * thin
            ra_send[i, j] = gate_partial[:, start : start + thin]

    def arrive_cast(n):
        @pl.when(jnp.logical_not(inner))
        def _():
            for i in range(LEAVES):
                cast_arrive(place(n), i)
        return cast(place(n))

    xp_ref[...] += arrive_cast(0)
    xp_ref[...] += arrive_cast(1)
    send_second(1)
    send_first(2)
    cast_all = xp_ref[...] + arrive_cast(2)
    high = cast_all.astype(bf)
    low = (cast_all - high.astype(fl)).astype(bf)
    terms = jnp.concatenate([high, low], axis=1)
    arrive("twin", c_twin)
    crossed = lax.rem(line + t, 2)
    for u, ref in ((1, c_twin), (0, c_ref)):
        partial = lax.dot_general(terms, ref[...], CONTRACT, preferred_element_type=fl)
        partial = ((partial[:rank_half] + partial[rank_half:]) * norming).astype(bf)
        straight, across = partial[:rank_rows], partial[rank_rows:]
        d_send[0, u] = jnp.where(side == 0, straight, across)
        d_send[1, u] = jnp.where(side == 0, across, straight)
        core = lax.rem(t + u, nt)
        near = (f, (1 - crossed) * square[0] + crossed * square[2], core)
        far = (f, (1 - crossed) * square[1] + crossed * square[3], core)
        send("d", "d", d_send.at[1, u], d_recv.at[1 + 2 * crossed], far)
        if u == 1:
            send("d", "d", d_send.at[0, u], d_recv.at[2 * crossed], near)
        else:
            @pl.when(crossed == 0)
            def _():
                d_recv[0] = d_send[0, 0]

            @pl.when(crossed == 1)
            def _():
                send("d1", "d", d_send.at[0, 0], d_recv.at[2], rep(2))

    send_third(0)
    send_third(1)
    send_first(3)
    send_second(2)
    for k in squares:
        send("ra", "ra", ra_send.at[square[k]], ra_recv.at[k - 1], rep(k))
    send_cross(0)
    send_cross(1)

    @pl.when(crossed == 0)
    def _():
        arrive("d", d_recv.at[: nr - 1])

    @pl.when(crossed == 1)
    def _():
        arrive("d", d_recv)

    total = d_recv[0].astype(fl)
    for k in squares:
        total = total + d_recv[k].astype(fl)
    e_all[f] = total.astype(bf)
    spread("e", "e", e_all.at[f], e_all.at[f])
    send_second(3)
    send_fourth(0)
    send_third(2)
    send_fourth(1)
    arrive("ra", ra_recv)
    gate_rows = ra_send[r]
    for k in squares:
        gate_rows = gate_rows + ra_recv[k - 1]
    rb_all[f] = gate_rows
    spread("rb", "rb", rb_all.at[f], rb_all.at[f])
    send_third(3)

    arrive("e", e_all.at[: nf - 1])
    projected = e_all[0].astype(fl)
    for j in fss:
        projected = projected + e_all[j].astype(fl)
    mean_after = BETA_ONE * lm_ref[...] + (1.0 - BETA_ONE) * projected
    square_after = BETA_TWO * ls_ref[...] + (1.0 - BETA_TWO) * projected * projected
    direction = mean_after / (jnp.sqrt(square_after) + EPSILON)
    top = lax.broadcasted_iota(jnp.int32, f_send.shape, 0) == 0
    f_send[...] = jnp.where(top, jnp.sum(direction * direction), jnp.sum(projected * projected))
    for i, spot in enumerate(spots):
        send("f", "f", f_send, f_recv.at[i], spot)
    projected_ref[...] = projected
    send_cross(2)
    send_cross(3)
    arrive("rb", rb_all.at[: nf - 1])
    gate_block = rb_all[0]
    for j in fss:
        gate_block = gate_block + rb_all[j]
    rd_all[r] = gate_block * norming
    for k in squares:
        send("rd", "rd", rd_all.at[r], rd_all.at[r], rep(k))
    send_fourth(2)
    arrive("f", f_recv)
    sums = f_send[...]
    for i in range(len(spots)):
        sums = sums + f_recv[i]
    balance = jnp.sqrt(sums[:1, :1] / (sums[1:2, :1] + NORM_FLOOR))
    balance_ref[...] = jnp.broadcast_to(balance, balance_ref.shape)
    h_all[r] = (direction - balance * projected).astype(bf)
    for k in squares:
        send("h", "h", h_all.at[r], h_all.at[r], rep(k))

    send_fourth(3)
    arrive("rd", rd_all.at[: nr - 1])
    arrive("h", h_all.at[: nr - 1])
    arrive("fourth", g_all.at[: nr - 1])
    sent = {
        "first": a_send, "twin": c_ref, "second": m_send,
        "third": b_send, "cross": v_send, "fourth": g_all.at[: nr - 1], "d": d_recv.at[: nr - 1],
        "e": e_all.at[: nf - 1], "f": f_recv, "h": h_all.at[: nr - 1], "ra": ra_recv,
        "rb": rb_all.at[: nf - 1], "rd": rd_all.at[: nr - 1],
    }
    for group, ref in sent.items():
        settle(send_sem.at[groups[group]], ref)

    @pl.when(inner)
    def _():
        settle(send_sem.at[groups["cast"]], p_all)
        settle(send_sem.at[groups["cast2"]], p_all.at[0])

    @pl.when(jnp.logical_not(inner))
    def _():
        settle(send_sem.at[groups["cast"]], p_all.at[0])

    @pl.when(crossed == 1)
    def _():
        settle(send_sem.at[groups["d1"]], d_send.at[0, 0])


def closing_kernel(
    g_ref, h_ref, balance_ref, projected_ref, gate_ref, pj_ref, qm_ref, lm_ref, ls_ref, gm_ref, gq_ref,
    *rest,
):
    outs, staged, out_sem = rest[:8], rest[8:16], rest[16]
    qu_ref, qr_ref, qc_ref, ma_ref, sa_ref, gu_ref, ga_ref, ge_ref = staged
    copies = []

    def flush(i, where=slice(None)):
        copy = pltpu.make_async_copy(
            staged[i].at[where], outs[i].at[where], out_sem.at[len(copies)]
        )
        copy.start()
        copies.append(copy)

    factor = h_ref[...].reshape(pj_ref.shape[1], qm_ref.shape[1])
    balance = balance_ref[:1, :1]
    thin = g_ref.shape[1]
    for i in range(g_ref.shape[0]):
        rows = slice(i * thin, (i + 1) * thin)
        lifted = jnp.dot(pj_ref[rows], factor, preferred_element_type=jnp.float32)
        query_update = lifted + balance * g_ref[i].astype(jnp.float32)
        query_renewed = qm_ref[rows] - STEP_RATE * query_update
        qu_ref[rows] = query_update
        flush(0, rows)
        qr_ref[rows] = query_renewed
        flush(1, rows)
        qc_ref[rows] = query_renewed.astype(jnp.bfloat16)
        flush(2, rows)
    projected = projected_ref[...]
    ma_ref[...] = BETA_ONE * lm_ref[...] + (1.0 - BETA_ONE) * projected
    flush(3)
    sa_ref[...] = BETA_TWO * ls_ref[...] + (1.0 - BETA_TWO) * projected * projected
    flush(4)
    nr, nf, _, thin = gate_ref.shape
    for i in range(nr):
        for j in range(nf):
            window = slice((i * nf + j) * thin, (i * nf + j + 1) * thin)
            forget_gradient = gate_ref[i, j]
            average = BETA_ONE * gm_ref[:, window] + (1.0 - BETA_ONE) * forget_gradient
            energy = (
                BETA_TWO * gq_ref[:, window]
                + (1.0 - BETA_TWO) * forget_gradient * forget_gradient
            )
            ga_ref[:, window] = average
            ge_ref[:, window] = energy
            gu_ref[:, window] = average / (jnp.sqrt(energy) + EPSILON)
    for i in (5, 6, 7):
        flush(i)
    for copy in copies:
        copy.wait()


def per_device(nf, nr, nt, *args):
    x, c, gc, gt, pj, qm, lm, ls, gm, gq = args
    width, cols, rank_rows, heads = x.shape[1], c.shape[1], lm.shape[0], gc.shape[0]
    rank_all = pj.shape[1]
    thin = width // (nf * nr)
    fits = (
        width % (nf * nr * 128) == 0 and rank_rows % 16 == 0
        and cols % (PIECES * 128) == 0 and heads % 8 == 0 and nf == 4 and nr == 4 and nr * thin % (LEAVES * 16) == 0 and nt == 2
        and x.shape[0] % 128 == 0 and rank_all % (nt * 128) == 0
    )
    if not fits:
        return collective_form(*args)
    piece, half, bf, fl = cols // PIECES, thin // 2, jnp.bfloat16, jnp.float32
    scratch = [
        (x.shape, bf), (c.shape, bf), (c.shape, bf), (gc.shape, fl), (gt.shape, fl),
        (lm.shape, fl), (ls.shape, fl), ((nf, nr * thin, rank_all // nt), bf),
        ((PIECES, 2, 2, nf, half, piece), bf), ((PIECES, 2, 2, nf, half, piece), bf),
        ((nf, thin, cols), fl), ((2, nf, half, cols), fl),
        ((PIECES, 2, nf, half, piece), bf), ((PIECES, 2, nf, half, piece), bf),
        ((PIECES, 2, 2, half, piece), bf), ((PIECES, 2, 2, half, piece), bf),
        ((PIECES, 2, half, piece), bf), ((PIECES, 2, half, piece), bf),
        ((x.shape[0], rank_all // nt), fl),
        ((2, nt, rank_rows, cols), bf), ((nr, rank_rows, cols), bf),
        ((nf, rank_rows, cols), bf), ((8, 128), fl), ((nr * nt - 1, 8, 128), fl),
        ((nr, nf, heads, thin), fl), ((nr - 1, nf, heads, thin), fl),
        ((nf, nf, heads, thin), fl),
    ]
    outs = [
        (qm.shape, fl), (qm.shape, fl), (qm.shape, bf), (lm.shape, fl), (lm.shape, fl),
        (gm.shape, fl), (gm.shape, fl), (gm.shape, fl),
    ]
    between = [
        ((nr, thin, cols), bf), ((nr, rank_rows, cols), bf), ((8, 128), fl), (lm.shape, fl),
        ((nr, nf, heads, thin), fl),
    ]
    vmem = pl.BlockSpec(memory_space=pltpu.VMEM)
    hbm = pl.BlockSpec(memory_space=pltpu.HBM)
    semaphores = (16, 4 * PIECES + 10 + LEAVES * nf, nr + 6)
    passed = pl.pallas_call(
        functools.partial(fused_kernel, nf, nr, nt),
        out_shape=tuple(jax.ShapeDtypeStruct(*o) for o in between),
        in_specs=[hbm] * 7,
        out_specs=(vmem,) * len(between),
        scratch_shapes=[pltpu.VMEM(*v) for v in scratch]
        + [pltpu.SemaphoreType.DMA((n,)) for n in semaphores],
        compiler_params=pltpu.CompilerParams(
            collective_id=0, has_side_effects=True, vmem_limit_bytes=VMEM_GRANT
        ),
    )(*(pltpu.with_memory_space_constraint(v, pltpu.HBM) for v in (x, c, gc, gt, pj, lm, ls)))

    return pl.pallas_call(
        closing_kernel,
        out_shape=tuple(jax.ShapeDtypeStruct(*o) for o in outs),
        in_specs=[vmem] * (len(between) + 6),
        out_specs=(hbm,) * len(outs),
        scratch_shapes=[pltpu.VMEM(*o) for o in outs]
        + [pltpu.SemaphoreType.DMA((3 * nr + 5,))],
        compiler_params=pltpu.CompilerParams(vmem_limit_bytes=VMEM_GRANT // 2),
    )(*passed, pj, qm, lm, ls, gm, gq)


def solution(mesh):
    in_specs = (
        P(("fs", "rep"), None),
        P(("fs", "rep"), "tp"),
        P("tp", ("fs", "rep")),
        P("tp", ("fs", "rep")),
        P("fs", None),
        P("fs", "tp"),
        P("rep", "tp"),
        P("rep", "tp"),
        P("tp", None),
        P("tp", None),
    )
    out_specs = (
        P("fs", "tp"),
        P("fs", "tp"),
        P("fs", "tp"),
        P("rep", "tp"),
        P("rep", "tp"),
        P("tp", None),
        P("tp", None),
        P("tp", None),
    )
    return jax.shard_map(
        functools.partial(per_device, mesh.shape["fs"], mesh.shape["rep"], mesh.shape["tp"]),
        mesh=mesh, in_specs=in_specs, out_specs=out_specs, check_vma=False
    )
```

```python
import functools

import jax
import jax.numpy as jnp
from jax import lax
from jax.experimental import pallas as pl
from jax.experimental.pallas import tpu as pltpu
from jax.sharding import PartitionSpec as P

BETA_ONE = 0.9
BETA_TWO = 0.95
STEP_RATE = 0.01
EPSILON = 1e-08
NORM_FLOOR = 1e-06


PIECES = 4
LEAVES = 4
VMEM_GRANT = 32 * 1024 * 1024
MESH = pl.DeviceIdType.MESH
CONTRACT = (((0,), (0,)), ((), ()))


def collective_form(
    attention_input,
    query_cotangent,
    gate_cotangent,
    gate_totals,
    projector,
    query_master,
    lowrank_mean,
    lowrank_square,
    gating_mean,
    gating_square,
):
    tokens_all = attention_input.shape[0] * lax.axis_size("fs") * lax.axis_size("rep")
    norming = 1.0 / tokens_all**0.5
    contract = (((0,), (0,)), ((), ()))
    earlier = jnp.concatenate(
        [jnp.zeros((gate_totals.shape[0], 1), jnp.float32), gate_totals[:, :-1]], axis=1
    )
    gate_logarithm = gate_totals - earlier
    trailing = lax.cumsum(gate_cotangent, axis=1, reverse=True)
    gate_signal = (trailing * -jnp.expm1(gate_logarithm)).astype(jnp.bfloat16)
    gate_partial = jnp.dot(gate_signal, attention_input, preferred_element_type=jnp.float32)
    forget_gradient = lax.psum(gate_partial, ("fs", "rep")) * norming
    thin_rows = lax.psum_scatter(
        lax.dot_general(
            attention_input, query_cotangent, contract, preferred_element_type=jnp.float32
        ),
        ("fs", "rep"),
        scatter_dimension=0,
        tiled=True,
    )
    gradient = lax.all_gather(thin_rows, "rep", axis=0, tiled=True) * norming
    rank_rows = lowrank_mean.shape[0]
    own_factor = lax.dynamic_slice_in_dim(
        projector, lax.axis_index("rep") * rank_rows, rank_rows, 1
    ).astype(jnp.float32)
    rank_partial = lax.dot_general(
        own_factor,
        gradient,
        contract,
        precision=lax.Precision.HIGHEST,
        preferred_element_type=jnp.float32,
    )
    projected = lax.psum(rank_partial, "fs")
    mean_after = BETA_ONE * lowrank_mean + (1.0 - BETA_ONE) * projected
    square_after = BETA_TWO * lowrank_square + (1.0 - BETA_TWO) * projected * projected
    direction = mean_after / (jnp.sqrt(square_after) + EPSILON)
    direction_squares, projected_squares = lax.psum(
        (jnp.sum(direction * direction), jnp.sum(projected * projected)), ("rep", "tp")
    )
    balance = jnp.sqrt(direction_squares / (projected_squares + NORM_FLOOR))
    blended = (direction - balance * projected).astype(jnp.bfloat16)
    lifted = jnp.dot(
        projector,
        lax.all_gather(blended, "rep", axis=0, tiled=True),
        preferred_element_type=jnp.float32,
    )
    query_update = lifted + balance * gradient
    query_renewed = query_master - STEP_RATE * query_update
    query_copy = query_renewed.astype(jnp.bfloat16)
    gating_average = BETA_ONE * gating_mean + (1.0 - BETA_ONE) * forget_gradient
    gating_energy = BETA_TWO * gating_square + (1.0 - BETA_TWO) * forget_gradient * forget_gradient
    gating_update = gating_average / (jnp.sqrt(gating_energy) + EPSILON)
    return (
        query_update,
        query_renewed,
        query_copy,
        mean_after,
        square_after,
        gating_update,
        gating_average,
        gating_energy,
    )


def fused_kernel(
    nf, nr, nt,
    x_hbm, c_hbm, gc_hbm, gt_hbm, pj_hbm, lm_hbm, ls_hbm,
    g_all, h_all, balance_ref, projected_ref, rd_all,
    x_ref, c_ref, c_twin, gc_ref, gt_ref, lm_ref, ls_ref, p_all,
    a_send, a_recv, a_own, a_keep, m_send, m_recv, b_send, b_recv, v_send, v_recv,
    xp_ref, d_send, d_recv, e_all, f_send, f_recv,
    ra_send, ra_recv, rb_all,
    send_sem, recv_sem, load_sem,
):
    f, r, t = lax.axis_index("fs"), lax.axis_index("rep"), lax.axis_index("tp")
    tokens, width = x_ref.shape
    cols = c_ref.shape[1]
    piece = cols // PIECES
    thin = width // (nf * nr)
    half = thin // 2
    rank_rows = lm_ref.shape[0]
    rank_half = p_all.shape[2]
    norming = 1.0 / (tokens * nf * nr) ** 0.5
    fl, bf = jnp.float32, jnp.bfloat16
    side, line = lax.rem(r, 2), r // 2
    square = [r, line * 2 + (1 - side), (1 - line) * 2 + side, (1 - line) * 2 + (1 - side)]
    fss, squares = list(range(1, nf)), [1, 2, 3]

    def columns(owner, j):
        return pl.ds(pl.multiple_of((j * nr + owner) * thin, thin), thin)

    def load(slot, src, dst):
        pltpu.make_async_copy(src, dst, load_sem.at[slot]).start()

    def settle(sem, ref):
        pltpu.make_async_copy(ref, ref, sem).wait()

    mine = pl.ds(pl.multiple_of(t * rank_half, rank_half), rank_half)
    load(nr + 1, pj_hbm.at[:, mine], p_all.at[f])
    load(nr, c_hbm, c_ref)
    for k in [3, 1, 2, 0]:
        for j in range(nf):
            where = columns(square[k], j)
            load(k, x_hbm.at[:, where], x_ref.at[:, where])
    for i, v in enumerate(((gc_hbm, gc_ref), (gt_hbm, gt_ref), (lm_hbm, lm_ref), (ls_hbm, ls_ref))):
        load(nr + 2 + i, *v)

    groups, arrivals, totals_sent = {}, {}, {}

    def send(group, key, src, dst, where):
        copy = pltpu.make_async_remote_copy(
            src_ref=src, dst_ref=dst,
            send_sem=send_sem.at[groups.setdefault(group, len(groups))],
            recv_sem=recv_sem.at[arrivals.setdefault(key, len(arrivals))],
            device_id=where, device_id_type=MESH,
        )
        copy.start()

    def arrive(key, ref):
        settle(recv_sem.at[arrivals[key]], ref)

    def rep(k):
        return (f, square[k], t)

    def place(n):
        up = jnp.where(f <= n, n + 1, n)
        down = jnp.where(f <= nf - 2 - n, nf - 1 - n, nf - 2 - n)
        return jnp.where(2 * f < nf, up, down)

    def spread(group, key, src, dst):
        for n in reversed(range(nf - 1)):
            send(group, key, src, dst, (place(n), r, t))

    spots = [(f, square[k], lax.rem(t + dt, nt)) for k in range(4) for dt in range(nt) if k or dt]
    peers = [(place(n), r, t) for n in range(nf - 1)] + spots
    barrier = pltpu.get_barrier_semaphore()
    for peer in peers:
        pl.semaphore_signal(barrier, inc=1, device_id=peer, device_id_type=MESH)

    def cut(p):
        return slice(p * piece, (p + 1) * piece)

    def fill(k, j):
        value = lax.dot_general(
            x_ref[:, columns(square[k], j)], c_ref[...], CONTRACT, preferred_element_type=fl
        )
        upper, lower = value[:half], value[half:]
        if k == 0:
            a_own[j] = value
        if k == 1:
            a_keep[1, j] = lower
        if k == 2:
            a_keep[0, j] = upper
        for h, part, slot in ((0, upper, {3: 0, 1: 1}), (1, lower, {3: 0, 2: 1})):
            if k in slot:
                small = part.astype(bf)
                for p in range(PIECES):
                    a_send[p, h, slot[k], j] = small[:, cut(p)]

    def ready(k):
        settle(load_sem.at[k], x_ref.at[:, : nf * thin])

    def send_open(h, o):
        send("first", ("open", o), a_send.at[0, h, o], a_recv.at[0, h, o], rep(1 + h))

    def send_first(p):
        for h in range(2):
            send("first", ("first", p), a_send.at[p, h], a_recv.at[p, h], rep(1 + h))

    def send_second(p):
        if p == 0:
            arrive(("open", 0), a_recv.at[0, :, 0])
        else:
            arrive(("first", p), a_recv.at[p])
        for h in range(2):
            for j in range(nf):
                value = a_keep[h, j, :, cut(p)] + a_recv[p, h, 0, j].astype(fl)
                m_send[p, h, j] = value.astype(bf)
            send("second", ("second", p), m_send.at[p, h], m_recv.at[p, h], rep(2 - h))

    mate = f + 1 - 2 * lax.rem(f, 2)
    over = lax.rem(f + nf // 2, nf)
    mate_over = lax.rem(mate + nf // 2, nf)

    def summed(p, h, j):
        rows = slice(h * half, (h + 1) * half)
        return (
            a_own[j, rows, cut(p)] + a_recv[p, h, 1, j].astype(fl) + m_recv[p, h, j].astype(fl)
        )

    def send_third(p):
        if p == 0:
            arrive(("open", 1), a_recv.at[0, :, 1])
        arrive(("second", p), m_recv.at[p])
        for o, j in enumerate((mate_over, mate)):
            for h in range(2):
                b_send[p, o, h] = summed(p, h, j).astype(bf)
        if p < PIECES - 1:
            send("third", ("third", p), b_send.at[p], b_recv.at[p], (mate, r, t))
            return
        for h in range(2):
            v_send[p, h] = summed(p, h, over).astype(bf)
        send("third", ("third", p), b_send.at[p, 0], b_recv.at[p, 0], (mate_over, r, t))
        send("cross", ("cross", p), v_send.at[p], v_recv.at[p], (over, r, t))
        send("third", ("third", p), b_send.at[p, 1], b_recv.at[p, 1], (mate, r, t))

    def send_cross(p):
        arrive(("third", p), b_recv.at[p])
        for h in range(2):
            v_send[p, h] = (summed(p, h, over) + b_recv[p, 0, h].astype(fl)).astype(bf)
        send("cross", ("cross", p), v_send.at[p], v_recv.at[p], (over, r, t))

    def send_fourth(p):
        arrive(("cross", p), v_recv.at[p])
        if p == PIECES - 1:
            arrive(("third", p), b_recv.at[p])
        for h in range(2):
            total = summed(p, h, f) + b_recv[p, 1, h].astype(fl) + v_recv[p, h].astype(fl)
            if p == PIECES - 1:
                total = total + b_recv[p, 0, h].astype(fl)
            g_all[r, h * half : (h + 1) * half, cut(p)] = (total * norming).astype(bf)
        where = g_all.at[r, :, cut(p)]
        for k in (3, 1, 2):
            send("fourth", "fourth", where, where, rep(k))

    settle(load_sem.at[nr + 1], p_all.at[0])
    pl.semaphore_wait(barrier, len(peers))
    inner = f * (nf - 1 - f) > 0
    cast_sem = 4 * PIECES + 10
    deep = p_all.shape[1] // LEAVES

    def leaf(q, i):
        return p_all.at[q, i * deep : (i + 1) * deep]

    def cast_arrive(q, i):
        settle(recv_sem.at[cast_sem + LEAVES * q + i], leaf(0, i))

    def cast_send(group, q, i, where):
        pltpu.make_async_remote_copy(
            src_ref=leaf(q, i), dst_ref=leaf(q, i),
            send_sem=send_sem.at[groups.setdefault(group, len(groups))],
            recv_sem=recv_sem.at[cast_sem + LEAVES * q + i],
            device_id=(where, r, t), device_id_type=MESH,
        ).start()

    def relay(hop, leaves):
        @pl.when(inner)
        def _():
            for i in leaves:
                relay_leaf(hop, i)

    def relay_leaf(hop, i):
        if hop == 1:
            cast_arrive(f - 1, i)
            cast_send("cast", f - 1, i, f + 1)
            cast_arrive(f + 1, i)
            cast_send("cast", f + 1, i, f - 1)
        else:
            cast_arrive(over, i)
            cast_send("cast2", over, i, (nf - 1) * (f - 1))

    @pl.when(inner)
    def _():
        for i in range(LEAVES):
            cast_send("cast", f, i, f - 1)
            cast_send("cast", f, i, f + 1)

    @pl.when(jnp.logical_not(inner))
    def _():
        for i in range(LEAVES):
            cast_send("cast", f, i, place(0))

    settle(load_sem.at[nr], c_ref)
    send("twin", "twin", c_ref, c_twin, (f, r, 1 - t))
    ready(3)
    for j in range(nf):
        fill(3, j)
    send_open(0, 0)
    send_open(1, 0)
    for k in (1, 2):
        ready(k)
        for j in range(nf):
            fill(k, j)
        send_open(k - 1, 1)
    send_first(1)
    ready(0)
    for j in range(nf):
        fill(0, j)
    relay(1, range(LEAVES))
    send_second(0)

    def cast(q):
        where = pl.ds(pl.multiple_of(q * nr * thin, nr * thin), nr * thin)
        return jnp.dot(x_ref[:, where], p_all[q], preferred_element_type=fl)

    xp_ref[...] = cast(f)
    relay(2, range(LEAVES))

    for i, ref in enumerate((gc_ref, gt_ref, lm_ref, ls_ref)):
        settle(load_sem.at[nr + 2 + i], ref)
    lanes = 128
    lower = lax.broadcasted_iota(jnp.int32, (lanes, lanes), 0)
    upper = lax.broadcasted_iota(jnp.int32, (lanes, lanes), 1)
    later = (lower >= upper).astype(fl)
    carry = jnp.zeros((gc_ref.shape[0], 1), fl)
    signals = []
    totals = gt_ref[...]
    opens = lax.broadcasted_iota(jnp.int32, totals.shape, 1) == 0
    gate_logarithm = totals - jnp.where(opens, 0.0, pltpu.roll(totals, 1, 1))
    for i in reversed(range(tokens // lanes)):
        window = slice(i * lanes, (i + 1) * lanes)
        own = gc_ref[:, window]
        trailing = carry + jnp.dot(
            own, later, precision=lax.Precision.HIGHEST, preferred_element_type=fl
        )
        carry = carry + jnp.sum(own, axis=1, keepdims=True)
        signals.append(trailing)
    trailing = jnp.concatenate(signals[::-1], axis=1)
    series = jnp.ones_like(gate_logarithm)
    for i in range(8, 1, -1):
        series = 1.0 + gate_logarithm * series / i
    opening = jnp.where(
        gate_logarithm > -0.25, -gate_logarithm * series, 1.0 - jnp.exp(gate_logarithm)
    )
    gate_signal = (trailing * opening).astype(bf)
    gate_partial = jnp.dot(gate_signal, x_ref[...], preferred_element_type=fl)
    for i in range(nr):
        for j in range(nf):
            start = (i * nf + j) * thin
            ra_send[i, j] = gate_partial[:, start : start + thin]

    def arrive_cast(n):
        @pl.when(jnp.logical_not(inner))
        def _():
            for i in range(LEAVES):
                cast_arrive(place(n), i)
        return cast(place(n))

    for k in (3, 1, 2):
        send("ra", "ra", ra_send.at[square[k]], ra_recv.at[k - 1], rep(k))
    xp_ref[...] += arrive_cast(0)
    xp_ref[...] += arrive_cast(1)
    send_second(1)
    send_first(2)
    cast_all = xp_ref[...] + arrive_cast(2)
    high = cast_all.astype(bf)
    low = (cast_all - high.astype(fl)).astype(bf)
    terms = jnp.concatenate([high, low], axis=1)
    arrive("twin", c_twin)
    crossed = lax.rem(line + t, 2)
    for u, ref in ((1, c_twin), (0, c_ref)):
        partial = lax.dot_general(terms, ref[...], CONTRACT, preferred_element_type=fl)
        partial = ((partial[:rank_half] + partial[rank_half:]) * norming).astype(bf)
        straight, across = partial[:rank_rows], partial[rank_rows:]
        d_send[0, u] = jnp.where(side == 0, straight, across)
        d_send[1, u] = jnp.where(side == 0, across, straight)
        core = lax.rem(t + u, nt)
        near = (f, (1 - crossed) * square[0] + crossed * square[2], core)
        far = (f, (1 - crossed) * square[1] + crossed * square[3], core)
        send("d", "d", d_send.at[1, u], d_recv.at[1 + 2 * crossed], far)
        if u == 1:
            send("d", "d", d_send.at[0, u], d_recv.at[2 * crossed], near)
        else:
            @pl.when(crossed == 0)
            def _():
                d_recv[0] = d_send[0, 0]

            @pl.when(crossed == 1)
            def _():
                send("d1", "d", d_send.at[0, 0], d_recv.at[2], rep(2))

    send_third(0)
    arrive("ra", ra_recv)
    gate_rows = ra_send[r]
    for k in squares:
        gate_rows = gate_rows + ra_recv[k - 1]
    rb_all[f] = gate_rows
    spread("rb", "rb", rb_all.at[f], rb_all.at[f])
    send_third(1)
    send_second(2)
    send_first(3)
    send_cross(0)
    send_cross(1)

    @pl.when(crossed == 0)
    def _():
        arrive("d", d_recv.at[: nr - 1])

    @pl.when(crossed == 1)
    def _():
        arrive("d", d_recv)

    total = d_recv[0].astype(fl)
    for k in squares:
        total = total + d_recv[k].astype(fl)
    e_all[f] = total.astype(bf)
    spread("e", "e", e_all.at[f], e_all.at[f])
    send_fourth(0)
    send_third(2)
    send_second(3)
    send_fourth(1)
    send_cross(2)

    arrive("e", e_all.at[: nf - 1])
    projected = e_all[0].astype(fl)
    for j in fss:
        projected = projected + e_all[j].astype(fl)
    mean_after = BETA_ONE * lm_ref[...] + (1.0 - BETA_ONE) * projected
    square_after = BETA_TWO * ls_ref[...] + (1.0 - BETA_TWO) * projected * projected
    direction = mean_after / (jnp.sqrt(square_after) + EPSILON)
    top = lax.broadcasted_iota(jnp.int32, f_send.shape, 0) == 0
    f_send[...] = jnp.where(top, jnp.sum(direction * direction), jnp.sum(projected * projected))
    for i, spot in enumerate(spots):
        send("f", "f", f_send, f_recv.at[i], spot)
    projected_ref[...] = projected
    send_third(3)
    arrive("rb", rb_all.at[: nf - 1])
    gate_block = rb_all[0]
    for j in fss:
        gate_block = gate_block + rb_all[j]
    rd_all[r] = gate_block * norming
    for k in (3, 1, 2):
        send("rd", "rd", rd_all.at[r], rd_all.at[r], rep(k))
    send_fourth(2)
    arrive("f", f_recv)
    sums = f_send[...]
    for i in range(len(spots)):
        sums = sums + f_recv[i]
    balance = jnp.sqrt(sums[:1, :1] / (sums[1:2, :1] + NORM_FLOOR))
    balance_ref[...] = jnp.broadcast_to(balance, balance_ref.shape)
    h_all[r] = (direction - balance * projected).astype(bf)
    for k in (3, 1, 2):
        send("h", "h", h_all.at[r], h_all.at[r], rep(k))

    send_fourth(3)
    arrive("rd", rd_all.at[: nr - 1])
    arrive("h", h_all.at[: nr - 1])
    arrive("fourth", g_all.at[: nr - 1])
    sent = {
        "first": a_send, "twin": c_ref, "second": m_send,
        "third": b_send, "cross": v_send, "fourth": g_all.at[: nr - 1], "d": d_recv.at[: nr - 1],
        "e": e_all.at[: nf - 1], "f": f_recv, "h": h_all.at[: nr - 1], "ra": ra_recv,
        "rb": rb_all.at[: nf - 1], "rd": rd_all.at[: nr - 1],
    }
    for group, ref in sent.items():
        settle(send_sem.at[groups[group]], ref)

    @pl.when(inner)
    def _():
        settle(send_sem.at[groups["cast"]], p_all)
        settle(send_sem.at[groups["cast2"]], p_all.at[0])

    @pl.when(jnp.logical_not(inner))
    def _():
        settle(send_sem.at[groups["cast"]], p_all.at[0])

    @pl.when(crossed == 1)
    def _():
        settle(send_sem.at[groups["d1"]], d_send.at[0, 0])


def closing_kernel(
    g_ref, h_ref, balance_ref, projected_ref, gate_ref, pj_ref, qm_ref, lm_ref, ls_ref, gm_ref, gq_ref,
    *rest,
):
    outs, staged, out_sem = rest[:8], rest[8:16], rest[16]
    qu_ref, qr_ref, qc_ref, ma_ref, sa_ref, gu_ref, ga_ref, ge_ref = staged
    copies = []

    def flush(i, where=slice(None)):
        copy = pltpu.make_async_copy(
            staged[i].at[where], outs[i].at[where], out_sem.at[len(copies)]
        )
        copy.start()
        copies.append(copy)

    factor = h_ref[...].reshape(pj_ref.shape[1], qm_ref.shape[1])
    balance = balance_ref[:1, :1]
    thin = g_ref.shape[1]
    for i in range(g_ref.shape[0]):
        rows = slice(i * thin, (i + 1) * thin)
        lifted = jnp.dot(pj_ref[rows], factor, preferred_element_type=jnp.float32)
        query_update = lifted + balance * g_ref[i].astype(jnp.float32)
        query_renewed = qm_ref[rows] - STEP_RATE * query_update
        qu_ref[rows] = query_update
        flush(0, rows)
        qr_ref[rows] = query_renewed
        flush(1, rows)
        qc_ref[rows] = query_renewed.astype(jnp.bfloat16)
        flush(2, rows)
    projected = projected_ref[...]
    ma_ref[...] = BETA_ONE * lm_ref[...] + (1.0 - BETA_ONE) * projected
    flush(3)
    sa_ref[...] = BETA_TWO * ls_ref[...] + (1.0 - BETA_TWO) * projected * projected
    flush(4)
    nr, nf, _, thin = gate_ref.shape
    for i in range(nr):
        for j in range(nf):
            window = slice((i * nf + j) * thin, (i * nf + j + 1) * thin)
            forget_gradient = gate_ref[i, j]
            average = BETA_ONE * gm_ref[:, window] + (1.0 - BETA_ONE) * forget_gradient
            energy = (
                BETA_TWO * gq_ref[:, window]
                + (1.0 - BETA_TWO) * forget_gradient * forget_gradient
            )
            ga_ref[:, window] = average
            ge_ref[:, window] = energy
            gu_ref[:, window] = average / (jnp.sqrt(energy) + EPSILON)
    for i in (5, 6, 7):
        flush(i)
    for copy in copies:
        copy.wait()


def per_device(nf, nr, nt, *args):
    x, c, gc, gt, pj, qm, lm, ls, gm, gq = args
    width, cols, rank_rows, heads = x.shape[1], c.shape[1], lm.shape[0], gc.shape[0]
    rank_all = pj.shape[1]
    thin = width // (nf * nr)
    fits = (
        width % (nf * nr * 128) == 0 and rank_rows % 16 == 0
        and cols % (PIECES * 128) == 0 and heads % 8 == 0 and nf == 4 and nr == 4 and nr * thin % (LEAVES * 16) == 0 and nt == 2
        and x.shape[0] % 128 == 0 and rank_all % (nt * 128) == 0
    )
    if not fits:
        return collective_form(*args)
    piece, half, bf, fl = cols // PIECES, thin // 2, jnp.bfloat16, jnp.float32
    scratch = [
        (x.shape, bf), (c.shape, bf), (c.shape, bf), (gc.shape, fl), (gt.shape, fl),
        (lm.shape, fl), (ls.shape, fl), ((nf, nr * thin, rank_all // nt), bf),
        ((PIECES, 2, 2, nf, half, piece), bf), ((PIECES, 2, 2, nf, half, piece), bf),
        ((nf, thin, cols), fl), ((2, nf, half, cols), fl),
        ((PIECES, 2, nf, half, piece), bf), ((PIECES, 2, nf, half, piece), bf),
        ((PIECES, 2, 2, half, piece), bf), ((PIECES, 2, 2, half, piece), bf),
        ((PIECES, 2, half, piece), bf), ((PIECES, 2, half, piece), bf),
        ((x.shape[0], rank_all // nt), fl),
        ((2, nt, rank_rows, cols), bf), ((nr, rank_rows, cols), bf),
        ((nf, rank_rows, cols), bf), ((8, 128), fl), ((nr * nt - 1, 8, 128), fl),
        ((nr, nf, heads, thin), fl), ((nr - 1, nf, heads, thin), fl),
        ((nf, nf, heads, thin), fl),
    ]
    outs = [
        (qm.shape, fl), (qm.shape, fl), (qm.shape, bf), (lm.shape, fl), (lm.shape, fl),
        (gm.shape, fl), (gm.shape, fl), (gm.shape, fl),
    ]
    between = [
        ((nr, thin, cols), bf), ((nr, rank_rows, cols), bf), ((8, 128), fl), (lm.shape, fl),
        ((nr, nf, heads, thin), fl),
    ]
    vmem = pl.BlockSpec(memory_space=pltpu.VMEM)
    hbm = pl.BlockSpec(memory_space=pltpu.HBM)
    semaphores = (16, 4 * PIECES + 10 + LEAVES * nf, nr + 6)
    passed = pl.pallas_call(
        functools.partial(fused_kernel, nf, nr, nt),
        out_shape=tuple(jax.ShapeDtypeStruct(*o) for o in between),
        in_specs=[hbm] * 7,
        out_specs=(vmem,) * len(between),
        scratch_shapes=[pltpu.VMEM(*v) for v in scratch]
        + [pltpu.SemaphoreType.DMA((n,)) for n in semaphores],
        compiler_params=pltpu.CompilerParams(
            collective_id=0, has_side_effects=True, vmem_limit_bytes=VMEM_GRANT
        ),
    )(*(pltpu.with_memory_space_constraint(v, pltpu.HBM) for v in (x, c, gc, gt, pj, lm, ls)))

    return pl.pallas_call(
        closing_kernel,
        out_shape=tuple(jax.ShapeDtypeStruct(*o) for o in outs),
        in_specs=[vmem] * (len(between) + 6),
        out_specs=(hbm,) * len(outs),
        scratch_shapes=[pltpu.VMEM(*o) for o in outs]
        + [pltpu.SemaphoreType.DMA((3 * nr + 5,))],
        compiler_params=pltpu.CompilerParams(vmem_limit_bytes=VMEM_GRANT // 2),
    )(*passed, pj, qm, lm, ls, gm, gq)


def solution(mesh):
    in_specs = (
        P(("fs", "rep"), None),
        P(("fs", "rep"), "tp"),
        P("tp", ("fs", "rep")),
        P("tp", ("fs", "rep")),
        P("fs", None),
        P("fs", "tp"),
        P("rep", "tp"),
        P("rep", "tp"),
        P("tp", None),
        P("tp", None),
    )
    out_specs = (
        P("fs", "tp"),
        P("fs", "tp"),
        P("fs", "tp"),
        P("rep", "tp"),
        P("rep", "tp"),
        P("tp", None),
        P("tp", None),
        P("tp", None),
    )
    return jax.shard_map(
        functools.partial(per_device, mesh.shape["fs"], mesh.shape["rep"], mesh.shape["tp"]),
        mesh=mesh, in_specs=in_specs, out_specs=out_specs, check_vma=False
    )
```

```python
import functools

import jax
import jax.numpy as jnp
from jax import lax
from jax.experimental import pallas as pl
from jax.experimental.pallas import tpu as pltpu
from jax.sharding import PartitionSpec as P

BETA_ONE = 0.9
BETA_TWO = 0.95
STEP_RATE = 0.01
EPSILON = 1e-08
NORM_FLOOR = 1e-06


PIECES = 4
LEAVES = 4
VMEM_GRANT = 32 * 1024 * 1024
MESH = pl.DeviceIdType.MESH
CONTRACT = (((0,), (0,)), ((), ()))


def collective_form(
    attention_input,
    query_cotangent,
    gate_cotangent,
    gate_totals,
    projector,
    query_master,
    lowrank_mean,
    lowrank_square,
    gating_mean,
    gating_square,
):
    tokens_all = attention_input.shape[0] * lax.axis_size("fs") * lax.axis_size("rep")
    norming = 1.0 / tokens_all**0.5
    contract = (((0,), (0,)), ((), ()))
    earlier = jnp.concatenate(
        [jnp.zeros((gate_totals.shape[0], 1), jnp.float32), gate_totals[:, :-1]], axis=1
    )
    gate_logarithm = gate_totals - earlier
    trailing = lax.cumsum(gate_cotangent, axis=1, reverse=True)
    gate_signal = (trailing * -jnp.expm1(gate_logarithm)).astype(jnp.bfloat16)
    gate_partial = jnp.dot(gate_signal, attention_input, preferred_element_type=jnp.float32)
    forget_gradient = lax.psum(gate_partial, ("fs", "rep")) * norming
    thin_rows = lax.psum_scatter(
        lax.dot_general(
            attention_input, query_cotangent, contract, preferred_element_type=jnp.float32
        ),
        ("fs", "rep"),
        scatter_dimension=0,
        tiled=True,
    )
    gradient = lax.all_gather(thin_rows, "rep", axis=0, tiled=True) * norming
    rank_rows = lowrank_mean.shape[0]
    own_factor = lax.dynamic_slice_in_dim(
        projector, lax.axis_index("rep") * rank_rows, rank_rows, 1
    ).astype(jnp.float32)
    rank_partial = lax.dot_general(
        own_factor,
        gradient,
        contract,
        precision=lax.Precision.HIGHEST,
        preferred_element_type=jnp.float32,
    )
    projected = lax.psum(rank_partial, "fs")
    mean_after = BETA_ONE * lowrank_mean + (1.0 - BETA_ONE) * projected
    square_after = BETA_TWO * lowrank_square + (1.0 - BETA_TWO) * projected * projected
    direction = mean_after / (jnp.sqrt(square_after) + EPSILON)
    direction_squares, projected_squares = lax.psum(
        (jnp.sum(direction * direction), jnp.sum(projected * projected)), ("rep", "tp")
    )
    balance = jnp.sqrt(direction_squares / (projected_squares + NORM_FLOOR))
    blended = (direction - balance * projected).astype(jnp.bfloat16)
    lifted = jnp.dot(
        projector,
        lax.all_gather(blended, "rep", axis=0, tiled=True),
        preferred_element_type=jnp.float32,
    )
    query_update = lifted + balance * gradient
    query_renewed = query_master - STEP_RATE * query_update
    query_copy = query_renewed.astype(jnp.bfloat16)
    gating_average = BETA_ONE * gating_mean + (1.0 - BETA_ONE) * forget_gradient
    gating_energy = BETA_TWO * gating_square + (1.0 - BETA_TWO) * forget_gradient * forget_gradient
    gating_update = gating_average / (jnp.sqrt(gating_energy) + EPSILON)
    return (
        query_update,
        query_renewed,
        query_copy,
        mean_after,
        square_after,
        gating_update,
        gating_average,
        gating_energy,
    )


def fused_kernel(
    nf, nr, nt,
    x_hbm, c_hbm, gc_hbm, gt_hbm, pj_hbm, lm_hbm, ls_hbm,
    g_all, h_all, balance_ref, projected_ref, rd_all,
    x_ref, c_ref, c_twin, gc_ref, gt_ref, lm_ref, ls_ref, p_all,
    a_send, a_recv, a_own, a_keep, m_send, m_recv, b_send, b_recv, v_send, v_recv,
    xp_ref, d_send, d_recv, e_all, f_send, f_recv,
    ra_send, ra_recv, rb_all,
    send_sem, recv_sem, load_sem,
):
    f, r, t = lax.axis_index("fs"), lax.axis_index("rep"), lax.axis_index("tp")
    tokens, width = x_ref.shape
    cols = c_ref.shape[1]
    piece = cols // PIECES
    thin = width // (nf * nr)
    half = thin // 2
    rank_rows = lm_ref.shape[0]
    rank_half = p_all.shape[2]
    norming = 1.0 / (tokens * nf * nr) ** 0.5
    fl, bf = jnp.float32, jnp.bfloat16
    side, line = lax.rem(r, 2), r // 2
    square = [r, line * 2 + (1 - side), (1 - line) * 2 + side, (1 - line) * 2 + (1 - side)]
    fss, squares = list(range(1, nf)), [1, 2, 3]

    def columns(owner, j):
        return pl.ds(pl.multiple_of((j * nr + owner) * thin, thin), thin)

    def load(slot, src, dst):
        pltpu.make_async_copy(src, dst, load_sem.at[slot]).start()

    def settle(sem, ref):
        pltpu.make_async_copy(ref, ref, sem).wait()

    mine = pl.ds(pl.multiple_of(t * rank_half, rank_half), rank_half)
    load(nr + 1, pj_hbm.at[:, mine], p_all.at[f])
    load(nr, c_hbm, c_ref)
    for k in [3, 1, 2, 0]:
        for j in range(nf):
            where = columns(square[k], j)
            load(k, x_hbm.at[:, where], x_ref.at[:, where])
    for i, v in enumerate(((gc_hbm, gc_ref), (gt_hbm, gt_ref), (lm_hbm, lm_ref), (ls_hbm, ls_ref))):
        load(nr + 2 + i, *v)

    groups, arrivals, totals_sent = {}, {}, {}

    def send(group, key, src, dst, where):
        copy = pltpu.make_async_remote_copy(
            src_ref=src, dst_ref=dst,
            send_sem=send_sem.at[groups.setdefault(group, len(groups))],
            recv_sem=recv_sem.at[arrivals.setdefault(key, len(arrivals))],
            device_id=where, device_id_type=MESH,
        )
        copy.start()

    def arrive(key, ref):
        settle(recv_sem.at[arrivals[key]], ref)

    def rep(k):
        return (f, square[k], t)

    def place(n):
        up = jnp.where(f <= n, n + 1, n)
        down = jnp.where(f <= nf - 2 - n, nf - 1 - n, nf - 2 - n)
        return jnp.where(2 * f < nf, up, down)

    def spread(group, key, src, dst):
        for n in reversed(range(nf - 1)):
            send(group, key, src, dst, (place(n), r, t))

    spots = [(f, square[k], lax.rem(t + dt, nt)) for k in range(4) for dt in range(nt) if k or dt]
    peers = [(place(n), r, t) for n in range(nf - 1)] + spots
    barrier = pltpu.get_barrier_semaphore()
    for peer in peers:
        pl.semaphore_signal(barrier, inc=1, device_id=peer, device_id_type=MESH)

    def cut(p):
        return slice(p * piece, (p + 1) * piece)

    def fill(k, j):
        value = lax.dot_general(
            x_ref[:, columns(square[k], j)], c_ref[...], CONTRACT, preferred_element_type=fl
        )
        upper, lower = value[:half], value[half:]
        if k == 0:
            a_own[j] = value
        if k == 1:
            a_keep[1, j] = lower
        if k == 2:
            a_keep[0, j] = upper
        for h, part, slot in ((0, upper, {3: 0, 1: 1}), (1, lower, {3: 0, 2: 1})):
            if k in slot:
                small = part.astype(bf)
                for p in range(PIECES):
                    a_send[p, h, slot[k], j] = small[:, cut(p)]

    def ready(k):
        settle(load_sem.at[k], x_ref.at[:, : nf * thin])

    def send_open(h, o):
        send("first", ("open", o), a_send.at[0, h, o], a_recv.at[0, h, o], rep(1 + h))

    def send_first(p):
        for h in range(2):
            send("first", ("first", p), a_send.at[p, h], a_recv.at[p, h], rep(1 + h))

    def send_second(p):
        if p == 0:
            arrive(("open", 0), a_recv.at[0, :, 0])
        else:
            arrive(("first", p), a_recv.at[p])
        for h in range(2):
            for j in range(nf):
                value = a_keep[h, j, :, cut(p)] + a_recv[p, h, 0, j].astype(fl)
                m_send[p, h, j] = value.astype(bf)
            send("second", ("second", p), m_send.at[p, h], m_recv.at[p, h], rep(2 - h))

    mate = f + 1 - 2 * lax.rem(f, 2)
    over = lax.rem(f + nf // 2, nf)
    mate_over = lax.rem(mate + nf // 2, nf)

    def summed(p, h, j):
        rows = slice(h * half, (h + 1) * half)
        return (
            a_own[j, rows, cut(p)] + a_recv[p, h, 1, j].astype(fl) + m_recv[p, h, j].astype(fl)
        )

    def send_third(p):
        if p == 0:
            arrive(("open", 1), a_recv.at[0, :, 1])
        arrive(("second", p), m_recv.at[p])
        for o, j in enumerate((mate_over, mate)):
            for h in range(2):
                b_send[p, o, h] = summed(p, h, j).astype(bf)
        if p < PIECES - 1:
            send("third", ("third", p), b_send.at[p], b_recv.at[p], (mate, r, t))
            return
        for h in range(2):
            v_send[p, h] = summed(p, h, over).astype(bf)
        send("third", ("third", p), b_send.at[p, 0], b_recv.at[p, 0], (mate_over, r, t))
        send("cross", ("cross", p), v_send.at[p], v_recv.at[p], (over, r, t))
        send("third", ("third", p), b_send.at[p, 1], b_recv.at[p, 1], (mate, r, t))

    def send_cross(p):
        arrive(("third", p), b_recv.at[p])
        for h in range(2):
            v_send[p, h] = (summed(p, h, over) + b_recv[p, 0, h].astype(fl)).astype(bf)
        send("cross", ("cross", p), v_send.at[p], v_recv.at[p], (over, r, t))

    def send_fourth(p):
        arrive(("cross", p), v_recv.at[p])
        if p == PIECES - 1:
            arrive(("third", p), b_recv.at[p])
        for h in range(2):
            total = summed(p, h, f) + b_recv[p, 1, h].astype(fl) + v_recv[p, h].astype(fl)
            if p == PIECES - 1:
                total = total + b_recv[p, 0, h].astype(fl)
            g_all[r, h * half : (h + 1) * half, cut(p)] = (total * norming).astype(bf)
        where = g_all.at[r, :, cut(p)]
        for k in (3, 1, 2):
            send("fourth", "fourth", where, where, rep(k))

    settle(load_sem.at[nr + 1], p_all.at[0])
    pl.semaphore_wait(barrier, len(peers))
    inner = f * (nf - 1 - f) > 0
    cast_sem = 4 * PIECES + 11
    deep = p_all.shape[1] // LEAVES

    def leaf(q, i):
        return p_all.at[q, i * deep : (i + 1) * deep]

    def cast_arrive(q, i):
        settle(recv_sem.at[cast_sem + LEAVES * q + i], leaf(0, i))

    def cast_send(group, q, i, where):
        pltpu.make_async_remote_copy(
            src_ref=leaf(q, i), dst_ref=leaf(q, i),
            send_sem=send_sem.at[groups.setdefault(group, len(groups))],
            recv_sem=recv_sem.at[cast_sem + LEAVES * q + i],
            device_id=(where, r, t), device_id_type=MESH,
        ).start()

    def relay(hop, leaves):
        @pl.when(inner)
        def _():
            for i in leaves:
                relay_leaf(hop, i)

    def relay_leaf(hop, i):
        if hop == 1:
            cast_arrive(f - 1, i)
            cast_send("cast", f - 1, i, f + 1)
            cast_arrive(f + 1, i)
            cast_send("cast", f + 1, i, f - 1)
        else:
            cast_arrive(over, i)
            cast_send("cast2", over, i, (nf - 1) * (f - 1))

    @pl.when(inner)
    def _():
        for i in range(LEAVES):
            cast_send("cast", f, i, f - 1)
            cast_send("cast", f, i, f + 1)

    @pl.when(jnp.logical_not(inner))
    def _():
        for i in range(LEAVES):
            cast_send("cast", f, i, place(0))

    settle(load_sem.at[nr], c_ref)
    send("twin", "twin", c_ref, c_twin, (f, r, 1 - t))
    ready(3)
    for j in range(nf):
        fill(3, j)
    send_open(0, 0)
    send_open(1, 0)
    for k in (1, 2):
        ready(k)
        for j in range(nf):
            fill(k, j)
        send_open(k - 1, 1)
    send_first(1)
    ready(0)
    for j in range(nf):
        fill(0, j)
    relay(1, range(LEAVES))
    send_second(0)

    def cast(q):
        where = pl.ds(pl.multiple_of(q * nr * thin, nr * thin), nr * thin)
        return jnp.dot(x_ref[:, where], p_all[q], preferred_element_type=fl)

    xp_ref[...] = cast(f)
    relay(2, range(LEAVES))

    for i, ref in enumerate((gc_ref, gt_ref, lm_ref, ls_ref)):
        settle(load_sem.at[nr + 2 + i], ref)
    lanes = 128
    lower = lax.broadcasted_iota(jnp.int32, (lanes, lanes), 0)
    upper = lax.broadcasted_iota(jnp.int32, (lanes, lanes), 1)
    later = (lower >= upper).astype(fl)
    carry = jnp.zeros((gc_ref.shape[0], 1), fl)
    signals = []
    totals = gt_ref[...]
    opens = lax.broadcasted_iota(jnp.int32, totals.shape, 1) == 0
    gate_logarithm = totals - jnp.where(opens, 0.0, pltpu.roll(totals, 1, 1))
    for i in reversed(range(tokens // lanes)):
        window = slice(i * lanes, (i + 1) * lanes)
        own = gc_ref[:, window]
        trailing = carry + jnp.dot(
            own, later, precision=lax.Precision.HIGHEST, preferred_element_type=fl
        )
        carry = carry + jnp.sum(own, axis=1, keepdims=True)
        signals.append(trailing)
    trailing = jnp.concatenate(signals[::-1], axis=1)
    series = jnp.ones_like(gate_logarithm)
    for i in range(8, 1, -1):
        series = 1.0 + gate_logarithm * series / i
    opening = jnp.where(
        gate_logarithm > -0.25, -gate_logarithm * series, 1.0 - jnp.exp(gate_logarithm)
    )
    gate_signal = (trailing * opening).astype(bf)
    gate_partial = jnp.dot(gate_signal, x_ref[...], preferred_element_type=fl)
    for i in range(nr):
        for j in range(nf):
            start = (i * nf + j) * thin
            ra_send[i, j] = gate_partial[:, start : start + thin]

    def arrive_cast(n):
        @pl.when(jnp.logical_not(inner))
        def _():
            for i in range(LEAVES):
                cast_arrive(place(n), i)
        return cast(place(n))

    for k in (3, 1, 2):
        send("ra", "ra", ra_send.at[square[k]], ra_recv.at[k - 1], rep(k))
    xp_ref[...] += arrive_cast(0)
    xp_ref[...] += arrive_cast(1)
    send_second(1)
    send_first(2)
    cast_all = xp_ref[...] + arrive_cast(2)
    high = cast_all.astype(bf)
    low = (cast_all - high.astype(fl)).astype(bf)
    terms = jnp.concatenate([high, low], axis=1)
    arrive("twin", c_twin)
    crossed = lax.rem(line + t, 2)
    short = rank_rows // 2

    def send_d(u, i):
        core = lax.rem(t + u, nt)
        near = (f, (1 - crossed) * square[0] + crossed * square[2], core)
        far = (f, (1 - crossed) * square[1] + crossed * square[3], core)
        own = slice(i * short, (i + 1) * short)
        send("d", ("d", i), d_send.at[1, u, own], d_recv.at[i, 1 + 2 * crossed], far)
        if u == 1:
            send("d", ("d", i), d_send.at[0, u, own], d_recv.at[i, 2 * crossed], near)
        else:
            @pl.when(crossed == 0)
            def _():
                d_recv[i, 0] = d_send[0, 0, own]

            @pl.when(crossed == 1)
            def _():
                send("d1", ("d", i), d_send.at[0, 0, own], d_recv.at[i, 2], rep(2))

    for u, ref in ((1, c_twin), (0, c_ref)):
        partial = lax.dot_general(terms, ref[...], CONTRACT, preferred_element_type=fl)
        partial = ((partial[:rank_half] + partial[rank_half:]) * norming).astype(bf)
        straight, across = partial[:rank_rows], partial[rank_rows:]
        d_send[0, u] = jnp.where(side == 0, straight, across)
        d_send[1, u] = jnp.where(side == 0, across, straight)
        send_d(u, 0)
    for u in (1, 0):
        send_d(u, 1)

    send_third(0)
    arrive("ra", ra_recv)
    gate_rows = ra_send[r]
    for k in squares:
        gate_rows = gate_rows + ra_recv[k - 1]
    rb_all[f] = gate_rows
    spread("rb", "rb", rb_all.at[f], rb_all.at[f])
    send_third(1)
    send_second(2)
    send_first(3)
    send_cross(0)
    send_cross(1)

    for i in range(2):
        @pl.when(crossed == 0)
        def _():
            arrive(("d", i), d_recv.at[i, : nr - 1])

        @pl.when(crossed == 1)
        def _():
            arrive(("d", i), d_recv.at[i])

        total = d_recv[i, 0].astype(fl)
        for k in squares:
            total = total + d_recv[i, k].astype(fl)
        own = slice(i * short, (i + 1) * short)
        e_all[f, own] = total.astype(bf)
        spread("e", "e", e_all.at[f, own], e_all.at[f, own])
    send_fourth(0)
    send_third(2)
    send_second(3)
    send_fourth(1)
    send_cross(2)

    arrive("e", e_all.at[: nf - 1])
    projected = e_all[0].astype(fl)
    for j in fss:
        projected = projected + e_all[j].astype(fl)
    mean_after = BETA_ONE * lm_ref[...] + (1.0 - BETA_ONE) * projected
    square_after = BETA_TWO * ls_ref[...] + (1.0 - BETA_TWO) * projected * projected
    direction = mean_after / (jnp.sqrt(square_after) + EPSILON)
    top = lax.broadcasted_iota(jnp.int32, f_send.shape, 0) == 0
    f_send[...] = jnp.where(top, jnp.sum(direction * direction), jnp.sum(projected * projected))
    for i, spot in enumerate(spots):
        send("f", "f", f_send, f_recv.at[i], spot)
    projected_ref[...] = projected
    send_third(3)
    arrive("rb", rb_all.at[: nf - 1])
    gate_block = rb_all[0]
    for j in fss:
        gate_block = gate_block + rb_all[j]
    rd_all[r] = gate_block * norming
    for k in (3, 1, 2):
        send("rd", "rd", rd_all.at[r], rd_all.at[r], rep(k))
    send_fourth(2)
    arrive("f", f_recv)
    sums = f_send[...]
    for i in range(len(spots)):
        sums = sums + f_recv[i]
    balance = jnp.sqrt(sums[:1, :1] / (sums[1:2, :1] + NORM_FLOOR))
    balance_ref[...] = jnp.broadcast_to(balance, balance_ref.shape)
    h_all[r] = (direction - balance * projected).astype(bf)
    for k in (3, 1, 2):
        send("h", "h", h_all.at[r], h_all.at[r], rep(k))

    send_fourth(3)
    arrive("rd", rd_all.at[: nr - 1])
    arrive("h", h_all.at[: nr - 1])
    arrive("fourth", g_all.at[: nr - 1])
    sent = {
        "first": a_send, "twin": c_ref, "second": m_send,
        "third": b_send, "cross": v_send, "fourth": g_all.at[: nr - 1], "d": e_all.at[: nf - 1],
        "e": e_all.at[: nf - 1], "f": f_recv, "h": h_all.at[: nr - 1], "ra": ra_recv,
        "rb": rb_all.at[: nf - 1], "rd": rd_all.at[: nr - 1],
    }
    for group, ref in sent.items():
        settle(send_sem.at[groups[group]], ref)

    @pl.when(inner)
    def _():
        settle(send_sem.at[groups["cast"]], p_all)
        settle(send_sem.at[groups["cast2"]], p_all.at[0])

    @pl.when(jnp.logical_not(inner))
    def _():
        settle(send_sem.at[groups["cast"]], p_all.at[0])

    @pl.when(crossed == 1)
    def _():
        settle(send_sem.at[groups["d1"]], d_send.at[0, 0])


def closing_kernel(
    g_ref, h_ref, balance_ref, projected_ref, gate_ref, pj_ref, qm_ref, lm_ref, ls_ref, gm_ref, gq_ref,
    *rest,
):
    outs, staged, out_sem = rest[:8], rest[8:16], rest[16]
    qu_ref, qr_ref, qc_ref, ma_ref, sa_ref, gu_ref, ga_ref, ge_ref = staged
    copies = []

    def flush(i, where=slice(None)):
        copy = pltpu.make_async_copy(
            staged[i].at[where], outs[i].at[where], out_sem.at[len(copies)]
        )
        copy.start()
        copies.append(copy)

    factor = h_ref[...].reshape(pj_ref.shape[1], qm_ref.shape[1])
    balance = balance_ref[:1, :1]
    thin = g_ref.shape[1]
    for i in range(g_ref.shape[0]):
        rows = slice(i * thin, (i + 1) * thin)
        lifted = jnp.dot(pj_ref[rows], factor, preferred_element_type=jnp.float32)
        query_update = lifted + balance * g_ref[i].astype(jnp.float32)
        query_renewed = qm_ref[rows] - STEP_RATE * query_update
        qu_ref[rows] = query_update
        flush(0, rows)
        qr_ref[rows] = query_renewed
        flush(1, rows)
        qc_ref[rows] = query_renewed.astype(jnp.bfloat16)
        flush(2, rows)
    projected = projected_ref[...]
    ma_ref[...] = BETA_ONE * lm_ref[...] + (1.0 - BETA_ONE) * projected
    flush(3)
    sa_ref[...] = BETA_TWO * ls_ref[...] + (1.0 - BETA_TWO) * projected * projected
    flush(4)
    nr, nf, _, thin = gate_ref.shape
    for i in range(nr):
        for j in range(nf):
            window = slice((i * nf + j) * thin, (i * nf + j + 1) * thin)
            forget_gradient = gate_ref[i, j]
            average = BETA_ONE * gm_ref[:, window] + (1.0 - BETA_ONE) * forget_gradient
            energy = (
                BETA_TWO * gq_ref[:, window]
                + (1.0 - BETA_TWO) * forget_gradient * forget_gradient
            )
            ga_ref[:, window] = average
            ge_ref[:, window] = energy
            gu_ref[:, window] = average / (jnp.sqrt(energy) + EPSILON)
    for i in (5, 6, 7):
        flush(i)
    for copy in copies:
        copy.wait()


def per_device(nf, nr, nt, *args):
    x, c, gc, gt, pj, qm, lm, ls, gm, gq = args
    width, cols, rank_rows, heads = x.shape[1], c.shape[1], lm.shape[0], gc.shape[0]
    rank_all = pj.shape[1]
    thin = width // (nf * nr)
    fits = (
        width % (nf * nr * 128) == 0 and rank_rows % 32 == 0
        and cols % (PIECES * 128) == 0 and heads % 8 == 0 and nf == 4 and nr == 4 and nr * thin % (LEAVES * 16) == 0 and nt == 2
        and x.shape[0] % 128 == 0 and rank_all % (nt * 128) == 0
    )
    if not fits:
        return collective_form(*args)
    piece, half, bf, fl = cols // PIECES, thin // 2, jnp.bfloat16, jnp.float32
    scratch = [
        (x.shape, bf), (c.shape, bf), (c.shape, bf), (gc.shape, fl), (gt.shape, fl),
        (lm.shape, fl), (ls.shape, fl), ((nf, nr * thin, rank_all // nt), bf),
        ((PIECES, 2, 2, nf, half, piece), bf), ((PIECES, 2, 2, nf, half, piece), bf),
        ((nf, thin, cols), fl), ((2, nf, half, cols), fl),
        ((PIECES, 2, nf, half, piece), bf), ((PIECES, 2, nf, half, piece), bf),
        ((PIECES, 2, 2, half, piece), bf), ((PIECES, 2, 2, half, piece), bf),
        ((PIECES, 2, half, piece), bf), ((PIECES, 2, half, piece), bf),
        ((x.shape[0], rank_all // nt), fl),
        ((2, nt, rank_rows, cols), bf), ((2, nr, rank_rows // 2, cols), bf),
        ((nf, rank_rows, cols), bf), ((8, 128), fl), ((nr * nt - 1, 8, 128), fl),
        ((nr, nf, heads, thin), fl), ((nr - 1, nf, heads, thin), fl),
        ((nf, nf, heads, thin), fl),
    ]
    outs = [
        (qm.shape, fl), (qm.shape, fl), (qm.shape, bf), (lm.shape, fl), (lm.shape, fl),
        (gm.shape, fl), (gm.shape, fl), (gm.shape, fl),
    ]
    between = [
        ((nr, thin, cols), bf), ((nr, rank_rows, cols), bf), ((8, 128), fl), (lm.shape, fl),
        ((nr, nf, heads, thin), fl),
    ]
    vmem = pl.BlockSpec(memory_space=pltpu.VMEM)
    hbm = pl.BlockSpec(memory_space=pltpu.HBM)
    semaphores = (16, 4 * PIECES + 11 + LEAVES * nf, nr + 6)
    passed = pl.pallas_call(
        functools.partial(fused_kernel, nf, nr, nt),
        out_shape=tuple(jax.ShapeDtypeStruct(*o) for o in between),
        in_specs=[hbm] * 7,
        out_specs=(vmem,) * len(between),
        scratch_shapes=[pltpu.VMEM(*v) for v in scratch]
        + [pltpu.SemaphoreType.DMA((n,)) for n in semaphores],
        compiler_params=pltpu.CompilerParams(
            collective_id=0, has_side_effects=True, vmem_limit_bytes=VMEM_GRANT
        ),
    )(*(pltpu.with_memory_space_constraint(v, pltpu.HBM) for v in (x, c, gc, gt, pj, lm, ls)))

    return pl.pallas_call(
        closing_kernel,
        out_shape=tuple(jax.ShapeDtypeStruct(*o) for o in outs),
        in_specs=[vmem] * (len(between) + 6),
        out_specs=(hbm,) * len(outs),
        scratch_shapes=[pltpu.VMEM(*o) for o in outs]
        + [pltpu.SemaphoreType.DMA((3 * nr + 5,))],
        compiler_params=pltpu.CompilerParams(vmem_limit_bytes=VMEM_GRANT // 2),
    )(*passed, pj, qm, lm, ls, gm, gq)


def solution(mesh):
    in_specs = (
        P(("fs", "rep"), None),
        P(("fs", "rep"), "tp"),
        P("tp", ("fs", "rep")),
        P("tp", ("fs", "rep")),
        P("fs", None),
        P("fs", "tp"),
        P("rep", "tp"),
        P("rep", "tp"),
        P("tp", None),
        P("tp", None),
    )
    out_specs = (
        P("fs", "tp"),
        P("fs", "tp"),
        P("fs", "tp"),
        P("rep", "tp"),
        P("rep", "tp"),
        P("tp", None),
        P("tp", None),
        P("tp", None),
    )
    return jax.shard_map(
        functools.partial(per_device, mesh.shape["fs"], mesh.shape["rep"], mesh.shape["tp"]),
        mesh=mesh, in_specs=in_specs, out_specs=out_specs, check_vma=False
    )
```
